256 devices in a mesh: grp: 2 (over y), st: 32 (over z, core), tp: 4 (over x).
Axes of the slice: x: 4, y: 2, z: 16, core: 2. Of those that a mesh axis runs over, the one named last changes fastest.
The devices are a block of a 4x16x16 slice.
Arguments:
- pass_ids: int32 [512, 4], P(('grp', 'st')), parts along dimension 0, may hold values from 0 to 511, as said below
- store: bfloat16 [512, 64, 2048], P('st', None, 'tp'), may hold values from -6 to 6
- queries: bfloat16 [65536, 1024], P(('grp', 'st'), 'tp'), parts along dimension 0, may hold values from -40 to 40
- gate_pre: bfloat16 [65536, 1024], P(('grp', 'st'), 'tp'), parts along dimension 0, may hold values from -6 to 6
- w_query: bfloat16 [2048, 1024], P(None, 'tp'), may hold values from -0.125 to 0.125
- w_gate: bfloat16 [2048, 1024], P(None, 'tp'), may hold values from -0.125 to 0.125
- w_key: bfloat16 [2048, 1024], P(None, 'tp'), may hold values from -0.125 to 0.125
- w_value: bfloat16 [2048, 1024], P(None, 'tp'), may hold values from -0.125 to 0.125
- d_mem: bfloat16 [65536, 1024], P(('grp', 'st'), 'tp'), parts along dimension 0, may hold values from -6 to 6
Outputs:
- d_tokens: bfloat16 [65536, 2048], P(('grp', 'st', 'tp')), parts along dimension 0
- d_store: bfloat16 [1024, 64, 2048], P(('grp', 'st', 'tp')), parts along dimension 0
- d_wkey: float32 [4096, 1024], P(('grp', 'st'), 'tp'), parts along dimension 0
The draws below stay inside these ranges and needn't reach their ends.
There are 2 independent parts, one for each index of `grp`. The reference program is written for one: setup_inputs(seed, part) draws one part's arguments, and reference() takes and returns one part's arrays. A program takes and returns all parts, laid end to end along the dimension named above; an argument that names none is the same for every part. Nothing has to cross between parts.
Inputs may be any that keep to these rules, and one draw needn't show every extreme that they name: `pass_ids`: the 8 blocks of one index of st name at most 2 passages (counted with repetition) held by any one index of st o, that is passages o * 16 to o * 16 + 15. Every index of st takes exactly 2 passages from each of 16 indices of st and none from the others, so the bound 2 is reached by every index.
All inputs are finite; a program needn't handle non-finite values.
Results may differ from the reference program's by a relative error of at most 0.02.
Values may be sent and summed in bfloat16 or wider, within the bound.
A program may use at most 128 MiB of HBM per device.

```python
import jax
import jax.numpy as jnp
from jax import lax

D = 2048
HD = 256
MH = 4
BLK = 128
PB = 4
PL = 64
PASS_DEV = 16
MW = 1024
NBLK_DEV = 8
NBLK = 256
TOKENS = 32768
NPASS = 512
MOST = 2
N_ST = 32
N_TP = 4


def draw_pass_ids(key, part):
    folded = jax.random.fold_in(key, 17)
    key_hot, key_rank, key_order, key_pick, key_shift = jax.random.split(folded, 5)
    total_req = NBLK_DEV * PB
    used_owners = total_req // MOST
    device = jnp.arange(N_ST, dtype=jnp.int32)[:, None]
    owner_row = jnp.arange(N_ST, dtype=jnp.int32)[None, :]
    hottest = jax.random.randint(key_hot, (), 0, N_ST)
    levels = jnp.where(owner_row == hottest, 3, jnp.where(owner_row == (device - 1) % N_ST, 2, jnp.where(owner_row == (device + N_ST // 2) % N_ST, 1, 0)))
    jitter = jax.random.randint(key_rank, (N_ST, N_ST), 0, 1000)
    scores = levels * (1000 * N_ST) + jitter * N_ST + owner_row
    chosen = lax.top_k(scores, used_owners)[1].astype(jnp.int32)
    owners = jnp.repeat(chosen, MOST, axis=1)
    order_keys = jax.random.randint(key_order, (N_ST, total_req), 0, 1000) * total_req + jnp.arange(total_req, dtype=jnp.int32)[None, :]
    ordering = jnp.argsort(order_keys, axis=1)
    owners = jnp.take_along_axis(owners, ordering, axis=1)
    samples = jax.random.randint(key_pick, (3, N_ST, total_req), 0, PASS_DEV)
    popular = jnp.min(samples, axis=0)
    offsets = jax.random.randint(key_shift, (N_ST,), 0, PASS_DEV)
    within = (popular + offsets[owners]) % PASS_DEV
    passage_ids = owners * PASS_DEV + within
    return passage_ids.reshape(N_ST * NBLK_DEV, PB).astype(jnp.int32)


def draw_queries(key, part):
    folded = jax.random.fold_in(key, 23)
    key_base = jax.random.fold_in(folded, 0)
    base = jnp.clip(jax.random.normal(key_base, (TOKENS, MW), jnp.float32), -6.0, 6.0)
    return base.astype(jnp.bfloat16)


def level_of(own_key, dims, cuts, least, high):
    def one(dim, shards_of):
        steps = jax.random.uniform(jax.random.fold_in(jax.random.fold_in(own_key, 6), dim), (shards_of,), jnp.float32, least / len(cuts), high / len(cuts))
        return jnp.repeat(jnp.exp(steps), dims[dim] // shards_of).reshape((-1,) + (1,) * (len(dims) - dim - 1))

    loudness = one(*cuts[0])
    for cut in cuts[1:]:
        loudness = loudness * one(*cut)
    return loudness


def bell_draw(key, shape, deviation, reach, cuts=(), kind=jnp.bfloat16):
    array = jax.random.normal(key, shape, jnp.float32) * deviation
    if len(cuts) > 0:
        array = level_of(key, shape, cuts, -0.22, 0.18) * array
    return jnp.clip(array, min=-reach, max=reach).astype(kind)


def setup_inputs(seed: int = 0, part: int = 0) -> dict:
    keys = jax.random.split(jax.random.key(seed), 10)
    part_keys = jax.random.split(jax.random.fold_in(keys[9], part), 10)
    return {
        "pass_ids": draw_pass_ids(jax.random.fold_in(jax.random.fold_in(keys[9], part), 71), part),
        "store": bell_draw(keys[1], (NPASS, PL, D), 1.0, 6.0, ((0, 32), (2, 4))),
        "queries": draw_queries(jax.random.fold_in(jax.random.fold_in(keys[9], part), 71), part),
        "gate_pre": bell_draw(part_keys[3], (TOKENS, MW), 1.5, 6.0, ((0, 32), (1, 4))),
        "w_query": bell_draw(keys[4], (D, MW), D ** -0.5, 0.125, ((1, 4),)),
        "w_gate": bell_draw(keys[5], (D, MW), D ** -0.5, 0.125, ((1, 4),)),
        "w_key": bell_draw(keys[6], (D, MW), D ** -0.5, 0.125, ((1, 4),)),
        "w_value": bell_draw(keys[7], (D, MW), D ** -0.5, 0.125, ((1, 4),)),
        "d_mem": bell_draw(part_keys[8], (TOKENS, MW), 1.0, 6.0, ((0, 32), (1, 4))),
    }


def rounded_copy(values):
    return lax.optimization_barrier(values.astype(jnp.bfloat16)).astype(jnp.float32)


def reference(pass_ids, store, queries, gate_pre, w_query, w_gate, w_key, w_value, d_mem):
    flat_rows = store.reshape(NPASS * PL, D)
    keys_all = jnp.dot(flat_rows, w_key, preferred_element_type=jnp.float32).astype(jnp.bfloat16).reshape(NPASS, PL, MW)
    values_all = jnp.dot(flat_rows, w_value, preferred_element_type=jnp.float32).astype(jnp.bfloat16).reshape(NPASS, PL, MW)
    request_ids = pass_ids.reshape(-1).astype(jnp.int32)
    key_rows = keys_all[request_ids].reshape(NBLK, PB * PL, MH, HD).astype(jnp.float32)
    value_rows = values_all[request_ids].reshape(NBLK, PB * PL, MH, HD).astype(jnp.float32)
    query_rows = queries.reshape(NBLK, BLK, MH, HD).astype(jnp.float32)
    score_scale = HD ** -0.5
    scores = jnp.einsum('nqhd,nkhd->nhqk', query_rows, key_rows) * score_scale
    shifted = jnp.exp(scores - jnp.max(scores, axis=-1, keepdims=True))
    prob_rows = shifted / jnp.sum(shifted, axis=-1, keepdims=True)
    probs_low = rounded_copy(prob_rows)
    attended = jnp.einsum('nhqk,nkhd->nqhd', probs_low, value_rows).reshape(TOKENS, MW)
    gate_vals = gate_pre.astype(jnp.float32)
    sigmoid_vals = jax.nn.sigmoid(gate_vals)
    mem_grad = d_mem.astype(jnp.float32)
    attended_grad = rounded_copy(gate_vals * sigmoid_vals * mem_grad)
    gate_grad = rounded_copy(mem_grad * attended * sigmoid_vals * (1.0 + gate_vals * (1.0 - sigmoid_vals)))
    attended_four = attended_grad.reshape(NBLK, BLK, MH, HD)
    prob_grad = jnp.einsum('nqhd,nkhd->nhqk', attended_four, value_rows)
    score_grad = rounded_copy(score_scale * prob_rows * (prob_grad - jnp.sum(prob_rows * prob_grad, axis=-1, keepdims=True)))
    query_grad = rounded_copy(jnp.einsum('nhqk,nkhd->nqhd', score_grad, key_rows).reshape(TOKENS, MW))
    key_grad = rounded_copy(jnp.einsum('nhqk,nqhd->nkhd', score_grad, query_rows)).reshape(NBLK * PB, PL, MW)
    value_grad = rounded_copy(jnp.einsum('nhqk,nqhd->nkhd', probs_low, attended_four)).reshape(NBLK * PB, PL, MW)
    key_sums = jax.ops.segment_sum(key_grad, request_ids, NPASS).astype(jnp.bfloat16).reshape(NPASS * PL, MW)
    value_sums = jax.ops.segment_sum(value_grad, request_ids, NPASS).astype(jnp.bfloat16).reshape(NPASS * PL, MW)
    d_wkey = jnp.dot(flat_rows.T, key_sums, preferred_element_type=jnp.float32)
    group_width = MW // N_TP
    query_low = query_grad.astype(jnp.bfloat16)
    gate_low = gate_grad.astype(jnp.bfloat16)
    store_total = jnp.zeros((NPASS * PL, D), jnp.float32)
    token_total = jnp.zeros((TOKENS, D), jnp.float32)
    for group_index in range(N_TP):
        col_low = group_index * group_width
        col_high = col_low + group_width
        store_part = jnp.dot(key_sums[:, col_low:col_high], w_key[:, col_low:col_high].T, preferred_element_type=jnp.float32)
        store_part = store_part + jnp.dot(value_sums[:, col_low:col_high], w_value[:, col_low:col_high].T, preferred_element_type=jnp.float32)
        store_total = store_total + rounded_copy(store_part)
        token_part = jnp.dot(query_low[:, col_low:col_high], w_query[:, col_low:col_high].T, preferred_element_type=jnp.float32)
        token_part = token_part + jnp.dot(gate_low[:, col_low:col_high], w_gate[:, col_low:col_high].T, preferred_element_type=jnp.float32)
        token_total = token_total + rounded_copy(token_part)
    d_store = store_total.astype(jnp.bfloat16).reshape(NPASS, PL, D)
    d_tokens = token_total.astype(jnp.bfloat16)
    return (d_tokens, d_store, d_wkey)
```

```python
import functools

import jax
import jax.numpy as jnp
from jax import lax
from jax.experimental import pallas as pl
from jax.experimental.pallas import tpu as pltpu
from jax.sharding import Mesh
from jax.sharding import PartitionSpec as P

HD = 256
BLK = 128
PB = 4
MOST = 2
CHUNK = 4
ST = ("st_0", "st_1")
GRP_ST = ("grp", "st_0", "st_1")
GRP_ST_TP = ("grp", "st_0", "st_1", "tp")
MESH_ID = pl.DeviceIdType.MESH
VMEM_SPEC = pl.BlockSpec(memory_space=pltpu.VMEM)
SMEM_SPEC = pl.BlockSpec(memory_space=pltpu.SMEM)
ANY_SPEC = pl.BlockSpec(memory_space=pl.ANY)


class Plan:
    def __init__(self, ring, passages):
        self.ring = ring
        self.passages = passages
        self.reach = (ring // 2, (ring - 1) // 2)
        self.sizes = [
            {t: min(passages, 2 * MOST * (reach - t + 1)) for t in range(1, reach + 1)}
            for reach in self.reach
        ]
        self.base = [{}, {}]
        at = passages
        for d in range(2):
            for t in range(1, self.reach[d] + 1):
                self.base[d][t] = at
                at += self.sizes[d][t]
        self.slots = at

    def steps(self, down=False):
        order = range(1, max(self.reach) + 1)
        for t in reversed(order) if down else order:
            for first in range(0, self.passages, CHUNK):
                for d in range(2):
                    if t <= self.reach[d] and first < self.sizes[d][t]:
                        yield d, t, first, min(CHUNK, self.sizes[d][t] - first)


def places():
    z, k = lax.axis_index("st_0"), lax.axis_index("st_1")
    ring = lax.axis_size("st_0")
    g, x = lax.axis_index("grp"), lax.axis_index("tp")
    turn = 1 - 2 * k
    ahead = lax.rem(z + turn + ring, ring)
    behind = lax.rem(z - turn + ring, ring)
    return (g, ahead, k, x), (g, behind, k, x), (g, z, 1 - k, x)


def greet(*devices):
    barrier = pltpu.get_barrier_semaphore()
    for device in devices:
        pl.semaphore_signal(barrier, inc=1, device_id=device, device_id_type=MESH_ID)
    pl.semaphore_wait(barrier, len(devices))


def cast_kernel(
    plan, order_ref, where_ref, kv_ref, out_ref, buf, first_buf, send_sem, recv_sem, give_sem, take_sem
):
    ahead, behind, twin = places()
    count = plan.passages

    @pl.loop(0, count)
    def _(j):
        buf[j] = kv_ref[j]
        first_buf[j] = kv_ref[order_ref[j]]
        first_buf[count + j] = kv_ref[order_ref[count + j]]

    greet(ahead, behind, twin)
    copies = {}
    gifts = []

    def give(n, src, at, size):
        gift = pltpu.make_async_remote_copy(
            src_ref=src,
            dst_ref=buf.at[pl.ds(plan.slots + at, size)],
            send_sem=give_sem.at[n],
            recv_sem=take_sem.at[n],
            device_id=twin,
            device_id_type=MESH_ID,
        )
        gift.start()
        gifts.append(gift)

    def send(n, d, t, first, size):
        if t == 1:
            src = first_buf.at[pl.ds(d * count + first, size)]
        else:
            src = buf.at[pl.ds(plan.base[d][t - 1] + first, size)]
        copy = pltpu.make_async_remote_copy(
            src_ref=src,
            dst_ref=buf.at[pl.ds(plan.base[d][t] + first, size)],
            send_sem=send_sem.at[n],
            recv_sem=recv_sem.at[n],
            device_id=(ahead, behind)[d],
            device_id_type=MESH_ID,
        )
        copy.start()
        copies[d, t, first] = copy

    steps = list(plan.steps())
    number = {(d, t, first): n for n, (d, t, first, _) in enumerate(steps)}
    extent = {(d, t, first): size for d, t, first, size in steps}
    for d, t, first, size in steps:
        if t == 1:
            send(number[d, t, first], d, t, first, size)
    give(len(steps), kv_ref, 0, count)
    for n, (d, t, first, size) in enumerate(steps):
        copies[d, t, first].wait_recv()
        if (d, t + 1, first) in number:
            send(number[d, t + 1, first], d, t + 1, first, extent[d, t + 1, first])
        at = plan.base[d][t] + first
        give(n, buf.at[pl.ds(at, size)], at, size)
    for gift in gifts:
        gift.wait_recv()

    @pl.loop(0, out_ref.shape[0])
    def _(r):
        out_ref[r] = buf[where_ref[r]]

    for gift in gifts:
        gift.wait_send()
    for copy in copies.values():
        copy.wait_send()


def cast_rows(plan, order, where, kv):
    count, rows, cols = kv.shape
    steps = len(list(plan.steps()))
    return pl.pallas_call(
        functools.partial(cast_kernel, plan),
        out_shape=jax.ShapeDtypeStruct((where.shape[0], rows, cols), kv.dtype),
        in_specs=[SMEM_SPEC, SMEM_SPEC, VMEM_SPEC],
        out_specs=VMEM_SPEC,
        scratch_shapes=[
            pltpu.VMEM((2 * plan.slots, rows, cols), kv.dtype),
            pltpu.VMEM((2 * count, rows, cols), kv.dtype),
            pltpu.SemaphoreType.DMA((steps,)),
            pltpu.SemaphoreType.DMA((steps,)),
            pltpu.SemaphoreType.DMA((steps + 1,)),
            pltpu.SemaphoreType.DMA((steps + 1,)),
        ],
        compiler_params=pltpu.CompilerParams(
            collective_id=0, has_side_effects=True, vmem_limit_bytes=60 * 1024 * 1024
        ),
        name="cast_rows",
    )(order, where, kv)


def fold_kernel(
    plan,
    table_ref,
    rank_ref,
    grads_ref,
    out_ref,
    held,
    here,
    sums,
    send_sem,
    recv_sem,
    give_sem,
    take_sem,
    load_sem,
):
    ahead, behind, twin = places()
    count = plan.passages
    own = grads_ref.shape[0]
    readers = 2 * MOST

    load = pltpu.make_async_copy(grads_ref, held.at[pl.ds(0, own)], load_sem)
    load.start()
    held[2 * own] = jnp.zeros_like(held[2 * own])
    greet(ahead, behind, twin)
    gift = pltpu.make_async_remote_copy(
        src_ref=grads_ref,
        dst_ref=held.at[pl.ds(own, own)],
        send_sem=give_sem,
        recv_sem=take_sem,
        device_id=twin,
        device_id_type=MESH_ID,
    )
    gift.start()
    load.wait()
    gift.wait_recv()

    def readers_sum(slot):
        total = held[table_ref[slot * readers]].astype(jnp.float32)
        for q in range(1, readers):
            total += held[table_ref[slot * readers + q]].astype(jnp.float32)
        return total

    copies = {}
    steps = list(plan.steps(down=True))
    number = {(d, t, first): n for n, (d, t, first, _) in enumerate(steps)}
    for n, (d, t, first, size) in enumerate(steps):
        more = (d, t + 1, first) in number
        at = plan.base[d][t] + first
        if more:
            copies[d, t + 1, first].wait_recv()
            far_at = plan.base[d][t + 1] + first
            far_size = plan.sizes[d][t + 1] - first

            @pl.loop(0, min(far_size, size))
            def _(j):
                total = readers_sum(at + j) + here[far_at - count + j].astype(jnp.float32)
                sums[at - count + j] = total.astype(sums.dtype)

            begin = min(far_size, size)
        else:
            begin = 0
        if begin < size:

            @pl.loop(begin, size)
            def _(j):
                sums[at - count + j] = readers_sum(at + j).astype(sums.dtype)

        copy = pltpu.make_async_remote_copy(
            src_ref=sums.at[pl.ds(at - count, size)],
            dst_ref=here.at[pl.ds(at - count, size)],
            send_sem=send_sem.at[n],
            recv_sem=recv_sem.at[n],
            device_id=(behind, ahead)[d],
            device_id_type=MESH_ID,
        )
        copy.start()
        copies[d, t, first] = copy
    for (d, t, first), copy in copies.items():
        if t == 1:
            copy.wait_recv()

    @pl.loop(0, count)
    def _(p):
        total = readers_sum(p)
        for d in range(2):
            total += here[plan.base[d][1] - count + rank_ref[d * count + p]].astype(jnp.float32)
        out_ref[p] = total.astype(out_ref.dtype)

    gift.wait_send()
    for copy in copies.values():
        copy.wait_send()


def fold_rows(plan, table, rank, grads):
    own, rows, cols = grads.shape
    steps = len(list(plan.steps()))
    count = plan.passages
    return pl.pallas_call(
        functools.partial(fold_kernel, plan),
        out_shape=jax.ShapeDtypeStruct((count, rows, cols), grads.dtype),
        in_specs=[SMEM_SPEC, SMEM_SPEC, ANY_SPEC],
        out_specs=VMEM_SPEC,
        scratch_shapes=[
            pltpu.VMEM((2 * own + 1, rows, cols), grads.dtype),
            pltpu.VMEM((plan.slots - count, rows, cols), grads.dtype),
            pltpu.VMEM((plan.slots - count, rows, cols), grads.dtype),
            pltpu.SemaphoreType.DMA((steps,)),
            pltpu.SemaphoreType.DMA((steps,)),
            pltpu.SemaphoreType.DMA,
            pltpu.SemaphoreType.DMA,
            pltpu.SemaphoreType.DMA,
        ],
        compiler_params=pltpu.CompilerParams(
            collective_id=1, has_side_effects=True, vmem_limit_bytes=60 * 1024 * 1024
        ),
        name="fold_rows",
    )(table, rank, grads)


def by_value(plan, d, step):
    total = jnp.zeros_like(step)
    for t, at in plan.base[d].items():
        total = total + jnp.where(step == t, at, 0)
    return total


def routes(plan, pass_ids):
    count, ring = plan.passages, plan.ring
    me_z, me_k = lax.axis_index("st_0"), lax.axis_index("st_1")
    ids = lax.all_gather(pass_ids.reshape(-1), ST, axis=0, tiled=False)
    devices, requests = ids.shape
    total = devices * count
    every = jnp.arange(total, dtype=jnp.int32)
    owner = ids // count
    owner_z, owner_k = owner // 2, owner % 2
    reader_z = (jnp.arange(devices, dtype=jnp.int32) // 2)[:, None]
    away = jnp.mod((1 - 2 * owner_k) * (reader_z - owner_z), ring)
    reach = plan.reach[0]
    steps = (
        jnp.where((away >= 1) & (away <= reach), away, 0),
        jnp.where(away > reach, ring - away, 0),
    )
    hot = ids.reshape(-1)[:, None] == every[None, :]
    ranks = []
    slots = (every % count,)
    for d in range(2):
        far = jnp.max(jnp.where(hot, steps[d].reshape(-1)[:, None], 0), axis=0)
        far = far.reshape(devices, count)
        place = jnp.arange(count, dtype=jnp.int32)
        before = (far[:, None, :] > far[:, :, None]) | (
            (far[:, None, :] == far[:, :, None]) & (place[None, None, :] < place[None, :, None])
        )
        ranks.append(jnp.sum(before.astype(jnp.int32), axis=2))

    def of_chip(array):
        return lax.dynamic_slice_in_dim(array, me_z * 2, 2, axis=0)

    mine = lax.dynamic_slice_in_dim
    me = me_z * 2 + me_k
    rank_me = jnp.concatenate([mine(r, me, 1, axis=0).reshape(-1) for r in ranks])
    order = jnp.concatenate(
        [
            jnp.sum(
                jnp.where(
                    mine(r, me, 1, axis=0).reshape(-1)[None, :] == jnp.arange(count, dtype=jnp.int32)[:, None],
                    jnp.arange(count, dtype=jnp.int32)[None, :],
                    0,
                ),
                axis=1,
            )
            for r in ranks
        ]
    ).astype(jnp.int32)
    chip_ids = of_chip(ids).reshape(-1)
    chip_steps = [of_chip(s).reshape(-1) for s in steps]
    chip_k = of_chip(owner_k).reshape(-1)
    chip_hot = chip_ids[:, None] == every[None, :]
    slot = chip_ids % count
    for d in range(2):
        rank = jnp.sum(jnp.where(chip_hot, ranks[d].reshape(-1)[None, :], 0), axis=1)
        slot = jnp.where(chip_steps[d] > 0, by_value(plan, d, chip_steps[d]) + rank, slot)
    where = slot + jnp.where(chip_k == me_k, 0, plan.slots)
    where = mine(where, me_k * requests, requests, axis=0)
    first = jnp.where(chip_k == me_k, slot, -1).reshape(2, requests)
    first = jnp.where(me_k == 0, first, first[::-1]).reshape(-1)
    at_slot = first[:, None] == jnp.arange(plan.slots, dtype=jnp.int32)[None, :]
    turn = jnp.cumsum(at_slot.astype(jnp.int32), axis=0)
    number = jnp.arange(2 * requests, dtype=jnp.int32)[:, None]
    table = jnp.stack(
        [
            jnp.min(jnp.where(at_slot & (turn == q + 1), number, 2 * requests), axis=0)
            for q in range(2 * MOST)
        ],
        axis=1,
    ).reshape(-1)
    return order, rank_me.astype(jnp.int32), where.astype(jnp.int32), table.astype(jnp.int32)


def sum_in_order(tiles, axes, order):
    dims = [lax.axis_size(a) for a in axes]
    tiles = tiles.reshape(*dims, *tiles.shape[1:])
    tiles = tiles.transpose(*order, *range(len(axes), tiles.ndim))
    tiles = tiles.reshape(-1, *tiles.shape[len(axes) :])
    for k in order:
        tiles = lax.psum_scatter(tiles, axes[k], scatter_dimension=0, tiled=True)
    return tiles[0]


def in_blocks(array, dim, devices):
    before, after = (array.shape[:dim], array.shape[dim + 1 :])
    return jnp.moveaxis(array.reshape(*before, devices, -1, *after), dim, 0)


def summed_rows_2(array, axes, order, dim):
    devices = lax.axis_size(axes)
    return sum_in_order(in_blocks(array, dim, devices), axes, order)


def summed_on_arrival(array, axis, dim):
    devices = lax.axis_size(axis)
    tiles = lax.all_to_all(in_blocks(array, dim, devices), axis, 0, 0, tiled=True)
    return jnp.sum(tiles.astype(jnp.float32), axis=0)


def local(pass_ids, store, queries, gate_pre, w_query, w_gate, w_key, w_value, d_mem):
    tp_count = lax.axis_size("tp")
    tok_rows, head_cols = queries.shape
    head_count = head_cols // HD
    blocks = tok_rows // BLK
    passages = store.shape[0]
    pass_len = store.shape[1]
    model_width = w_key.shape[0]
    requests = blocks * PB
    pair_cols = 2 * head_cols
    plan = Plan(lax.axis_size("st_0"), passages)
    order, rank_me, where, table = routes(plan, pass_ids)
    weight_kv = jnp.concatenate([w_key, w_value], axis=1)
    gathered = lax.all_gather(store, "tp", axis=2, tiled=True)
    flat_rows = gathered.reshape(passages * pass_len, model_width)
    kv_pass = jnp.dot(flat_rows, weight_kv, preferred_element_type=jnp.float32)
    kv_low = kv_pass.astype(jnp.bfloat16).reshape(passages, pass_len, pair_cols)
    request_kv = cast_rows(plan, order, where, kv_low)
    block_kv = request_kv.reshape(blocks, PB * pass_len, pair_cols)
    key_rows = block_kv[:, :, :head_cols].reshape(blocks, PB * pass_len, head_count, HD)
    value_rows = block_kv[:, :, head_cols:].reshape(blocks, PB * pass_len, head_count, HD)
    query_rows = queries.reshape(blocks, BLK, head_count, HD)
    score_scale = HD ** (-0.5)
    scores = (
        jnp.einsum("nqhd,nkhd->nhqk", query_rows, key_rows, preferred_element_type=jnp.float32)
        * score_scale
    )
    shifted = jnp.exp(scores - jnp.max(scores, axis=-1, keepdims=True))
    prob_rows = shifted / jnp.sum(shifted, axis=-1, keepdims=True)
    probs_low = prob_rows.astype(jnp.bfloat16)
    attended = jnp.einsum(
        "nhqk,nkhd->nqhd", probs_low, value_rows, preferred_element_type=jnp.float32
    ).reshape(tok_rows, head_cols)
    gate_vals = gate_pre.astype(jnp.float32)
    sigmoid_vals = jax.nn.sigmoid(gate_vals)
    mem_grad = d_mem.astype(jnp.float32)
    attended_grad = (gate_vals * sigmoid_vals * mem_grad).astype(jnp.bfloat16)
    gate_grad = (
        mem_grad * attended * sigmoid_vals * (1.0 + gate_vals * (1.0 - sigmoid_vals))
    ).astype(jnp.bfloat16)
    attended_four = attended_grad.reshape(blocks, BLK, head_count, HD)
    prob_grad = jnp.einsum(
        "nqhd,nkhd->nhqk", attended_four, value_rows, preferred_element_type=jnp.float32
    )
    score_grad = (
        score_scale
        * prob_rows
        * (prob_grad - jnp.sum(prob_rows * prob_grad, axis=-1, keepdims=True))
    ).astype(jnp.bfloat16)
    query_grad = (
        jnp.einsum("nhqk,nkhd->nqhd", score_grad, key_rows, preferred_element_type=jnp.float32)
        .astype(jnp.bfloat16)
        .reshape(tok_rows, head_cols)
    )
    key_grad = jnp.einsum(
        "nhqk,nqhd->nkhd", score_grad, query_rows, preferred_element_type=jnp.float32
    )
    value_grad = jnp.einsum(
        "nhqk,nqhd->nkhd", probs_low, attended_four, preferred_element_type=jnp.float32
    )
    request_grads = jnp.concatenate(
        [
            key_grad.reshape(blocks, PB * pass_len, head_cols),
            value_grad.reshape(blocks, PB * pass_len, head_cols),
        ],
        axis=2,
    )
    request_grads = request_grads.astype(jnp.bfloat16).reshape(requests, pass_len, pair_cols)
    pass_low = fold_rows(plan, table, rank_me, request_grads)
    key_sums = pass_low[:, :, :head_cols].reshape(passages * pass_len, head_cols)
    d_wkey = summed_rows_2(
        jnp.einsum("rc,rh->ch", flat_rows, key_sums, preferred_element_type=jnp.float32),
        ST,
        (1, 0),
        0,
    )
    partial_value = pass_low.reshape(
        passages // tp_count * lax.axis_size("tp") * pass_len, pair_cols
    )
    d_store = summed_on_arrival(
        jnp.einsum("rc,dc->rd", partial_value, weight_kv, preferred_element_type=jnp.float32)
        .reshape(passages // tp_count * lax.axis_size("tp"), pass_len, model_width)
        .astype(jnp.bfloat16),
        "tp",
        0,
    ).astype(jnp.bfloat16)
    grad_both = jnp.concatenate([query_grad, gate_grad], axis=1)
    weight_both = jnp.concatenate([w_query, w_gate], axis=1)
    partial_value = grad_both
    d_tokens = summed_on_arrival(
        jnp.einsum(
            "rc,dc->rd", partial_value, weight_both, preferred_element_type=jnp.float32
        ).astype(jnp.bfloat16),
        "tp",
        0,
    ).astype(jnp.bfloat16)
    return (d_tokens, d_store, d_wkey)


def solution(mesh):
    finer = Mesh(
        mesh.devices.reshape(mesh.shape["grp"], -1, 2, mesh.shape["tp"]),
        ("grp", "st_0", "st_1", "tp"),
    )
    in_specs = (
        P(GRP_ST, None),
        P(ST, None, "tp"),
        P(GRP_ST, "tp"),
        P(GRP_ST, "tp"),
        P(None, "tp"),
        P(None, "tp"),
        P(None, "tp"),
        P(None, "tp"),
        P(GRP_ST, "tp"),
    )
    out_specs = (P(GRP_ST_TP, None), P(GRP_ST_TP, None, None), P(GRP_ST, "tp"))
    return jax.shard_map(local, mesh=finer, in_specs=in_specs, out_specs=out_specs, check_vma=False)
```

```python
import functools

import jax
import jax.numpy as jnp
from jax import lax
from jax.experimental import pallas as pl
from jax.experimental.pallas import tpu as pltpu
from jax.sharding import Mesh
from jax.sharding import PartitionSpec as P

HD = 256
BLK = 128
PB = 4
MOST = 2
CHUNK = 4
LIGHT = (24, 22, 22, 20, 18, 16, 12, 4)
VMEM_LIMIT = 62 * 1024 * 1024
ST = ("st_0", "st_1")
GRP_ST = ("grp", "st_0", "st_1")
GRP_ST_TP = ("grp", "st_0", "st_1", "tp")
MESH_ID = pl.DeviceIdType.MESH
VMEM_SPEC = pl.BlockSpec(memory_space=pltpu.VMEM)
SMEM_SPEC = pl.BlockSpec(memory_space=pltpu.SMEM)
ANY_SPEC = pl.BlockSpec(memory_space=pl.ANY)
F32 = jnp.float32


class Plan:
    def __init__(self, ring, passages, light=False):
        self.ring = ring
        self.passages = passages
        self.reach = ring // 2
        self.steps_of = range(1, self.reach + 1)
        per_owner = 2 * MOST
        self.layout = {
            t: min(passages, per_owner * (self.reach - t + 1))
            + min(passages, per_owner * (self.reach - t))
            for t in self.steps_of
        }
        self.sizes = dict(self.layout)
        if light:
            self.sizes = {t: min(n, LIGHT[t - 1]) for t, n in self.layout.items()}
        self.base = [{}, {}]
        at = passages
        for d in range(2):
            for t in self.steps_of:
                self.base[d][t] = at
                at += -(-self.layout[t] // 2)
        self.slots = at

    def half(self, t):
        return -(-self.sizes[t] // 2) if t <= self.reach else 0

    def steps(self, down=False):
        for t in reversed(self.steps_of) if down else self.steps_of:
            for first in range(0, self.half(t), CHUNK):
                for d in range(2):
                    yield d, t, first, min(CHUNK, self.half(t) - first)


class Place:
    def __init__(self):
        self.g, self.z, self.k, self.x = (lax.axis_index(a) for a in GRP_ST_TP)
        self.ring = lax.axis_size("st_0")
        self.tp = lax.axis_size("tp")
        self.twin = (self.g, self.z, 1 - self.k, self.x)

    def along_z(self, step):
        return (self.g, lax.rem(self.z + step + self.ring, self.ring), self.k, self.x)

    def along_x(self, step):
        return (self.g, self.z, self.k, lax.rem(self.x + step + self.tp, self.tp))


def greet(*devices):
    barrier = pltpu.get_barrier_semaphore()
    for device in devices:
        pl.semaphore_signal(barrier, inc=1, device_id=device, device_id_type=MESH_ID)
    pl.semaphore_wait(barrier, len(devices))


class Copies:
    def __init__(self, send_sem, recv_sem):
        self.send_sem, self.recv_sem = send_sem, recv_sem
        self.all = []

    def start(self, src, dst, device):
        n = len(self.all)
        copy = pltpu.make_async_remote_copy(
            src_ref=src,
            dst_ref=dst,
            send_sem=self.send_sem.at[n],
            recv_sem=self.recv_sem.at[n],
            device_id=device,
            device_id_type=MESH_ID,
        )
        copy.start()
        self.all.append(copy)
        return copy

    def wait_sends(self):
        for copy in self.all:
            copy.wait_send()


def copy_sems(count):
    return [pltpu.SemaphoreType.DMA((count,)), pltpu.SemaphoreType.DMA((count,))]


def cast_kernel(plan, weights, order_ref, where_ref, kv_ref, *refs):
    w_refs, refs = refs[:weights], refs[weights:]
    out_ref, w_outs, refs = refs[0], refs[1 : 1 + weights], refs[1 + weights :]
    buf, first_buf, home, *sems = refs
    ring_copies, gifts, w_copies = (Copies(*sems[2 * i : 2 * i + 2]) for i in range(3))
    place = Place()
    count, slots = plan.passages, plan.slots
    top = plan.half(1)

    greet(place.along_z(1), place.along_z(-1), place.along_x(1), place.along_x(-1), place.twin)
    own_gift = gifts.start(kv_ref, home.at[pl.ds(count, count)], place.twin)

    @pl.loop(0, count)
    def _(j):
        home[j] = kv_ref[j]
        buf[j] = kv_ref[j]

    own_gift.wait_recv()

    @pl.loop(0, top)
    def _(j):
        for d in range(2):
            first_buf[d * top + j] = home[order_ref[d * count + j]]

    copies = {}
    steps = list(plan.steps())
    extent = {(d, t, first): size for d, t, first, size in steps}

    def send(d, t, first):
        size = extent[d, t, first]
        if t == 1:
            src = first_buf.at[pl.ds(d * top + first, size)]
        else:
            src = buf.at[pl.ds(plan.base[d][t - 1] + first, size)]
        dst = buf.at[pl.ds(plan.base[d][t] + first, size)]
        copies[d, t, first] = ring_copies.start(src, dst, place.along_z(1 - 2 * d))

    for d, t, first, _ in steps:
        if t == 1:
            send(d, t, first)
    rows = w_refs[0].shape[0] // 2
    half = pl.ds(place.k * rows, rows)
    arrive = [[], []]
    for w_ref, w_out in zip(w_refs, w_outs):
        arrive[0].append(
            w_copies.start(w_ref.at[half], w_out.at[2, half], place.along_x(1))
        )
        arrive[1].append(
            w_copies.start(w_ref.at[half], w_out.at[0, half], place.along_x(-1))
        )
    w_gifts = []
    middle = []

    def forward_weights():
        for copy in arrive[0] + arrive[1]:
            copy.wait_recv()
        for w_out in w_outs:
            middle.append(
                w_copies.start(
                    w_out.at[2 * place.k, half],
                    w_out.at[1, half],
                    place.along_x(2 * place.k - 1),
                )
            )
            for rel in (0, 2):
                part = w_out.at[rel, half]
                w_gifts.append(w_copies.start(part, part, place.twin))

    last = None
    for d, t, first, size in steps:
        if t != last and t == plan.reach // 2 + 1:
            forward_weights()
        last = t
        copies[d, t, first].wait_recv()
        if (d, t + 1, first) in extent:
            send(d, t + 1, first)
        at = plan.base[d][t] + first
        gifts.start(buf.at[pl.ds(at, size)], buf.at[pl.ds(slots + at, size)], place.twin)
    for copy, w_out in zip(middle, w_outs):
        copy.wait_recv()
        part = w_out.at[1, half]
        w_gifts.append(w_copies.start(part, part, place.twin))
    for gift in gifts.all[1:]:
        gift.wait_recv()

    @pl.loop(0, count)
    def _(j):
        buf[slots + j] = home[count + j]

    @pl.loop(0, out_ref.shape[0])
    def _(r):
        out_ref[r] = buf[where_ref[r]]

    for gift in w_gifts:
        gift.wait_recv()
    for group in (gifts, ring_copies, w_copies):
        group.wait_sends()


def cast_rows(plan, ident, order, where, kv, weights):
    count, rows, cols = kv.shape
    steps = len(list(plan.steps()))
    others = lax.axis_size("tp") - 1
    return pl.pallas_call(
        functools.partial(cast_kernel, plan, len(weights)),
        out_shape=[jax.ShapeDtypeStruct((where.shape[0], rows, cols), kv.dtype)]
        + [jax.ShapeDtypeStruct((others, *w.shape), w.dtype) for w in weights],
        in_specs=[SMEM_SPEC, SMEM_SPEC, VMEM_SPEC] + [ANY_SPEC] * len(weights),
        out_specs=[VMEM_SPEC] + [ANY_SPEC] * len(weights),
        scratch_shapes=[
            pltpu.VMEM((2 * plan.slots, rows, cols), kv.dtype),
            pltpu.VMEM((2 * plan.half(1), rows, cols), kv.dtype),
            pltpu.VMEM((2 * count, rows, cols), kv.dtype),
        ]
        + copy_sems(steps)
        + copy_sems(steps + 1)
        + copy_sems(6 * len(weights)),
        compiler_params=pltpu.CompilerParams(
            collective_id=ident, has_side_effects=True, vmem_limit_bytes=VMEM_LIMIT
        ),
        name="cast_rows",
    )(order, where, kv, *weights)


def fold_kernel(
    plan,
    table_ref,
    final_ref,
    grads_ref,
    tokens_ref,
    out_ref,
    tokens_out,
    held,
    here,
    sums,
    load_sem,
    *sems,
):
    ring_copies, gifts, exchange = (Copies(*sems[2 * i : 2 * i + 2]) for i in range(3))
    place = Place()
    count, top = plan.passages, plan.half(1)
    own = grads_ref.shape[0]
    readers = 2 * MOST
    twin_at = plan.slots - count
    zero_at = twin_at + plan.layout[1]
    peers = [place.along_x(rel) for rel in range(1, place.tp)]

    load = pltpu.make_async_copy(grads_ref, held.at[pl.ds(0, own)], load_sem)
    load.start()
    held[2 * own] = jnp.zeros_like(held[2 * own])
    here[zero_at] = jnp.zeros_like(here[zero_at])
    greet(place.along_z(1), place.along_z(-1), place.twin, *peers)
    own_gift = gifts.start(grads_ref, held.at[pl.ds(own, own)], place.twin)
    block = tokens_out.shape[1]
    for rel, peer in enumerate(peers, 1):
        exchange.start(
            tokens_ref.at[pl.ds(peer[3] * block, block)],
            tokens_out.at[place.tp - 1 - rel],
            peer,
        )
    load.wait()
    own_gift.wait_recv()

    def readers_sum(slot):
        total = held[table_ref[slot * readers]].astype(F32)
        for q in range(1, readers):
            total += held[table_ref[slot * readers + q]].astype(F32)
        return total

    copies = {}
    steps = list(plan.steps(down=True))
    extent = {(d, t, first): size for d, t, first, size in steps}
    for d, t, first, size in steps:
        at = plan.base[d][t] + first
        begin = extent.get((d, t + 1, first), 0)
        if begin:
            copies[d, t + 1, first].wait_recv()
            far_at = plan.base[d][t + 1] + first

            @pl.loop(0, begin)
            def _(j):
                total = readers_sum(at + j) + here[far_at - count + j].astype(F32)
                sums[at - count + j] = total.astype(sums.dtype)

        if begin < size:

            @pl.loop(begin, size)
            def _(j):
                sums[at - count + j] = readers_sum(at + j).astype(sums.dtype)

        part = pl.ds(at - count, size)
        copies[d, t, first] = ring_copies.start(
            sums.at[part], here.at[part], place.along_z(2 * d - 1)
        )
    for d, t, first, size in steps:
        if t == 1:
            copies[d, t, first].wait_recv()
            src = here.at[pl.ds(plan.base[d][1] - count + first, size)]
            dst = here.at[pl.ds(twin_at + d * (plan.layout[1] // 2) + first, size)]
            gifts.start(src, dst, place.twin)
    for gift in gifts.all[1:]:
        gift.wait_recv()

    @pl.loop(0, count)
    def _(p):
        total = readers_sum(p)
        for d in range(2):
            total += here[final_ref[d * count + p]].astype(F32)
        out_ref[p] = total.astype(out_ref.dtype)

    for copy in exchange.all:
        copy.wait_recv()
    for group in (gifts, ring_copies, exchange):
        group.wait_sends()


def fold_rows(plan, ident, table, final, grads, tokens):
    own, rows, cols = grads.shape
    steps = list(plan.steps())
    ends = sum(1 for _, t, _, _ in steps if t == 1)
    count = plan.passages
    tp = lax.axis_size("tp")
    return pl.pallas_call(
        functools.partial(fold_kernel, plan),
        out_shape=[
            jax.ShapeDtypeStruct((count, rows, cols), grads.dtype),
            jax.ShapeDtypeStruct((tp - 1, tokens.shape[0] // tp, tokens.shape[1]), tokens.dtype),
        ],
        in_specs=[SMEM_SPEC, SMEM_SPEC, ANY_SPEC, ANY_SPEC],
        out_specs=[VMEM_SPEC, ANY_SPEC],
        scratch_shapes=[
            pltpu.VMEM((2 * own + 1, rows, cols), grads.dtype),
            pltpu.VMEM((plan.slots - count + plan.layout[1] + 1, rows, cols), grads.dtype),
            pltpu.VMEM((plan.slots - count, rows, cols), grads.dtype),
            pltpu.SemaphoreType.DMA,
        ]
        + copy_sems(len(steps))
        + copy_sems(1 + ends)
        + copy_sems(tp - 1),
        compiler_params=pltpu.CompilerParams(
            collective_id=ident, has_side_effects=True, vmem_limit_bytes=VMEM_LIMIT
        ),
        name="fold_rows",
    )(table, final, grads, tokens)


def project(rows_list, weight_list, out_ref, tile):
    @pl.loop(0, out_ref.shape[1] // tile)
    def _(n):
        cols = pl.ds(pl.multiple_of(n * tile, tile), tile)
        total = None
        for rows, weight in zip(rows_list, weight_list):
            term = lax.dot_general(
                rows[...], weight[cols, :], (((1,), (1,)), ((), ())), preferred_element_type=F32
            )
            total = term if total is None else total + term
        out_ref[:, cols] = total.astype(out_ref.dtype)


def tail_kernel(
    sums_ref,
    partial_ref,
    tokens_ref,
    tokens_in,
    *refs,
):
    weights, refs = refs[:8], refs[8:]
    d_tokens_ref, d_store_ref, d_wkey_ref = refs[:3]
    wbuf_t, wbuf_s, own_t, in_t, own_s, in_s, twin_buf, chip_buf, ring_buf = refs[3:12]
    load_sem, *sems = refs[12:]
    exchange, gifts, ring_copies = (Copies(*sems[2 * i : 2 * i + 2]) for i in range(3))
    place = Place()
    tp, ring = place.tp, place.ring
    peers = [place.along_x(rel) for rel in range(1, tp)]
    far = [place.along_z(rel) for rel in range(1, ring)]
    loads = []

    def load(src, dst):
        copy = pltpu.make_async_copy(src, dst, load_sem.at[len(loads)])
        copy.start()
        loads.append(copy)

    greet(place.twin, *peers, *far)
    gift = gifts.start(partial_ref.at[:, pl.ds(1 - place.k, 1)], twin_buf, place.twin)
    share = sums_ref.shape[0] // tp
    for rel, peer in enumerate(peers, 1):
        exchange.start(
            sums_ref.at[pl.ds(peer[3] * share, share)], in_s.at[tp - 1 - rel], peer
        )
    block = own_t.shape[0]
    load(tokens_ref.at[pl.ds(place.x * block, block)], own_t)
    load(tokens_in, in_t)
    load(sums_ref.at[pl.ds(place.x * share, share)], own_s)
    for wbuf, (wa, wb, wa_far, wb_far) in ((wbuf_t, weights[:4]), (wbuf_s, weights[4:])):
        load(wa, wbuf.at[0])
        load(wb, wbuf.at[1])
        load(wa_far, wbuf.at[pl.ds(2, tp - 1)])
        load(wb_far, wbuf.at[pl.ds(2 + tp - 1, tp - 1)])
    gift.wait_recv()

    @pl.loop(0, ring)
    def _(i):
        total = partial_ref[i, place.k] + twin_buf[i, 0]
        chip_buf[i] = total.astype(chip_buf.dtype)

    for rel, device in enumerate(far, 1):
        ring_copies.start(chip_buf.at[device[1]], ring_buf.at[ring - rel], device)
    for copy in loads:
        copy.wait()

    def operands(own, far_rows, wbuf):
        cols = own.shape[-1] // 2
        rows_list, weight_list = [], []
        for c in range(2):
            rows_list.append(own.at[:, pl.ds(c * cols, cols)])
            weight_list.append(wbuf.at[c])
        for rel in range(tp - 1):
            for c in range(2):
                rows_list.append(far_rows.at[rel, :, pl.ds(c * cols, cols)])
                weight_list.append(wbuf.at[2 + c * (tp - 1) + rel])
        return rows_list, weight_list

    project(*operands(own_t, in_t, wbuf_t), d_tokens_ref, 512)
    for copy in exchange.all:
        copy.wait_recv()
    rows = share * sums_ref.shape[1]
    cols = sums_ref.shape[2]
    project(
        *operands(own_s.reshape(rows, cols), in_s.reshape(tp - 1, rows, cols), wbuf_s),
        d_store_ref,
        512,
    )
    ring_copies_done = [copy.wait_recv() for copy in ring_copies.all]
    del ring_copies_done
    total = partial_ref[place.z, place.k] + twin_buf[place.z, 0]
    for rel in range(1, ring):
        total += ring_buf[rel].astype(F32)
    d_wkey_ref[...] = total
    for group in (exchange, gifts, ring_copies):
        group.wait_sends()


def tail(ident, sums, partial, tokens, tokens_in, weights):
    tp = lax.axis_size("tp")
    ring, cores, rows, cols = partial.shape
    model = weights[0].shape[0]
    head_cols = weights[0].shape[1]
    share = sums.shape[0] // tp
    low = sums.dtype
    return pl.pallas_call(
        tail_kernel,
        out_shape=[
            jax.ShapeDtypeStruct((tokens.shape[0] // tp, model), low),
            jax.ShapeDtypeStruct((share * sums.shape[1], model), low),
            jax.ShapeDtypeStruct((rows, cols), F32),
        ],
        in_specs=[ANY_SPEC, VMEM_SPEC] + [ANY_SPEC] * (2 + len(weights)),
        out_specs=[VMEM_SPEC] * 3,
        scratch_shapes=[
            pltpu.VMEM((2 * tp, model, head_cols), low),
            pltpu.VMEM((2 * tp, model, head_cols), low),
            pltpu.VMEM((tokens.shape[0] // tp, tokens.shape[1]), low),
            pltpu.VMEM(tokens_in.shape, low),
            pltpu.VMEM((share, *sums.shape[1:]), low),
            pltpu.VMEM((tp - 1, share, *sums.shape[1:]), low),
            pltpu.VMEM((ring, 1, rows, cols), F32),
            pltpu.VMEM((ring, rows, cols), low),
            pltpu.VMEM((ring, rows, cols), low),
            pltpu.SemaphoreType.DMA((3 + len(weights),)),
        ]
        + copy_sems(tp - 1)
        + copy_sems(1)
        + copy_sems(ring - 1),
        compiler_params=pltpu.CompilerParams(
            collective_id=ident, has_side_effects=True, vmem_limit_bytes=VMEM_LIMIT
        ),
        name="tail",
    )(sums, partial, tokens, tokens_in, *weights)


def first_slot(plan, d, step):
    total = jnp.zeros_like(step)
    for t, at in plan.base[d].items():
        total = total + jnp.where(step == t, at, 0)
    return total


def routes(plan, light, pass_ids):
    count, ring, slots = plan.passages, plan.ring, plan.slots
    me_z, me_k = lax.axis_index("st_0"), lax.axis_index("st_1")
    ids = lax.all_gather(pass_ids.reshape(-1), ST, axis=0, tiled=False)
    devices, requests = ids.shape
    pair = 2 * count
    every = jnp.arange(devices * count, dtype=jnp.int32)
    owner = ids // count
    owner_z, owner_k = owner // 2, owner % 2
    reader_z = (jnp.arange(devices, dtype=jnp.int32) // 2)[:, None]
    away = jnp.mod(reader_z - owner_z, ring)
    up = (2 * away < ring) | ((2 * away == ring) & (owner_k == 0))
    steps = (jnp.where(up, away, 0), jnp.where(up, 0, ring - away))
    hot = ids.reshape(-1)[:, None] == every[None, :]
    place = jnp.arange(pair, dtype=jnp.int32)
    ranks, fars = [], []
    fits = jnp.bool_(True)
    for d in range(2):
        far = jnp.max(jnp.where(hot, steps[d].reshape(-1)[:, None], 0), axis=0)
        far = far.reshape(ring, pair)
        before = (far[:, None, :] > far[:, :, None]) | (
            (far[:, None, :] == far[:, :, None]) & (place[None, None, :] < place[None, :, None])
        )
        ranks.append(jnp.sum(before.astype(jnp.int32), axis=2))
        fars.append(far)
        bounds = jnp.array([light.sizes[t] for t in light.steps_of], jnp.int32)
        dist = jnp.arange(1, plan.reach + 1, dtype=jnp.int32)
        sent = jnp.sum((far[:, None, :] >= dist[None, :, None]).astype(jnp.int32), axis=2)
        fits &= jnp.all(sent <= bounds[None, :])

    def chip(array):
        return lax.dynamic_slice_in_dim(array, me_z, 1, axis=0)[0]

    def readers(array):
        return lax.dynamic_slice_in_dim(array, me_z * 2, 2, axis=0).reshape(-1)

    at_home = place % count + jnp.where(place // count == me_k, 0, count)
    want = 2 * jnp.arange(count, dtype=jnp.int32) + me_k
    order, final = [], []
    for d in range(2):
        rank, far = chip(ranks[d]), chip(fars[d])
        order.append(jnp.sum(jnp.where(rank[None, :] == want[:, None], at_home[None, :], 0), axis=1))
        twin_at = plan.slots - count
        near = plan.base[d][1] - count
        aside = twin_at + d * (plan.layout[1] // 2)
        index = jnp.where(rank % 2 == me_k, near, aside) + rank // 2
        index = jnp.where(far > 0, index, twin_at + plan.layout[1])
        final.append(lax.dynamic_slice_in_dim(index, me_k * count, count, axis=0))
    chip_ids = readers(ids)
    chip_hot = chip_ids[:, None] == every[None, :]
    slot, core = chip_ids % count, readers(owner_k)
    for d in range(2):
        rank = jnp.sum(jnp.where(chip_hot, ranks[d].reshape(-1)[None, :], 0), axis=1)
        step = readers(steps[d] * (away > 0))
        slot = jnp.where(step > 0, first_slot(plan, d, step) + rank // 2, slot)
        core = jnp.where(step > 0, rank % 2, core)
    where = slot + jnp.where(core == me_k, 0, slots)
    where = lax.dynamic_slice_in_dim(where, me_k * requests, requests, axis=0)
    mine = jnp.where(core == me_k, slot, -1).reshape(2, requests)
    mine = jnp.where(me_k == 0, mine, mine[::-1]).reshape(-1)
    at_slot = mine[:, None] == jnp.arange(slots, dtype=jnp.int32)[None, :]
    turn = jnp.cumsum(at_slot.astype(jnp.int32), axis=0)
    number = jnp.arange(2 * requests, dtype=jnp.int32)[:, None]
    table = jnp.stack(
        [
            jnp.min(jnp.where(at_slot & (turn == q + 1), number, 2 * requests), axis=0)
            for q in range(2 * MOST)
        ],
        axis=1,
    ).reshape(-1)
    tables = (jnp.concatenate(order), where, table, jnp.concatenate(final))
    return fits, *(t.astype(jnp.int32) for t in tables)


def local(pass_ids, store, queries, gate_pre, w_query, w_gate, w_key, w_value, d_mem):
    tp_count = lax.axis_size("tp")
    ring = lax.axis_size("st_0")
    tok_rows, head_cols = queries.shape
    head_count = head_cols // HD
    blocks = tok_rows // BLK
    passages = store.shape[0]
    pass_len = store.shape[1]
    model_width = w_key.shape[0]
    requests = blocks * PB
    pair_cols = 2 * head_cols
    plan = Plan(ring, passages)
    light = Plan(ring, passages, light=True)
    fits, order, where, table, final = routes(plan, light, pass_ids)
    weight_kv = jnp.concatenate([w_key, w_value], axis=1)
    gathered = lax.all_gather(store, "tp", axis=2, tiled=True)
    flat_rows = gathered.reshape(passages * pass_len, model_width)
    kv_pass = jnp.dot(flat_rows, weight_kv, preferred_element_type=jnp.float32)
    kv_low = kv_pass.astype(jnp.bfloat16).reshape(passages, pass_len, pair_cols)
    weights = (w_query, w_gate, w_key, w_value)
    request_kv, wq_far, wg_far, wk_far, wv_far = lax.cond(
        fits,
        functools.partial(cast_rows, light, 0),
        functools.partial(cast_rows, plan, 1),
        order,
        where,
        kv_low,
        weights,
    )
    block_kv = request_kv.reshape(blocks, PB * pass_len, pair_cols)
    key_rows = block_kv[:, :, :head_cols].reshape(blocks, PB * pass_len, head_count, HD)
    value_rows = block_kv[:, :, head_cols:].reshape(blocks, PB * pass_len, head_count, HD)
    query_rows = queries.reshape(blocks, BLK, head_count, HD)
    score_scale = HD ** (-0.5)
    scores = (
        jnp.einsum("nqhd,nkhd->nhqk", query_rows, key_rows, preferred_element_type=jnp.float32)
        * score_scale
    )
    shifted = jnp.exp(scores - jnp.max(scores, axis=-1, keepdims=True))
    prob_rows = shifted / jnp.sum(shifted, axis=-1, keepdims=True)
    probs_low = prob_rows.astype(jnp.bfloat16)
    attended = jnp.einsum(
        "nhqk,nkhd->nqhd", probs_low, value_rows, preferred_element_type=jnp.float32
    ).reshape(tok_rows, head_cols)
    gate_vals = gate_pre.astype(jnp.float32)
    sigmoid_vals = jax.nn.sigmoid(gate_vals)
    mem_grad = d_mem.astype(jnp.float32)
    attended_grad = (gate_vals * sigmoid_vals * mem_grad).astype(jnp.bfloat16)
    gate_grad = (
        mem_grad * attended * sigmoid_vals * (1.0 + gate_vals * (1.0 - sigmoid_vals))
    ).astype(jnp.bfloat16)
    attended_four = attended_grad.reshape(blocks, BLK, head_count, HD)
    prob_grad = jnp.einsum(
        "nqhd,nkhd->nhqk", attended_four, value_rows, preferred_element_type=jnp.float32
    )
    score_grad = (
        score_scale
        * prob_rows
        * (prob_grad - jnp.sum(prob_rows * prob_grad, axis=-1, keepdims=True))
    ).astype(jnp.bfloat16)
    query_grad = (
        jnp.einsum("nhqk,nkhd->nqhd", score_grad, key_rows, preferred_element_type=jnp.float32)
        .astype(jnp.bfloat16)
        .reshape(tok_rows, head_cols)
    )
    key_grad = jnp.einsum(
        "nhqk,nqhd->nkhd", score_grad, query_rows, preferred_element_type=jnp.float32
    )
    value_grad = jnp.einsum(
        "nhqk,nqhd->nkhd", probs_low, attended_four, preferred_element_type=jnp.float32
    )
    request_grads = jnp.concatenate(
        [
            key_grad.reshape(blocks, PB * pass_len, head_cols),
            value_grad.reshape(blocks, PB * pass_len, head_cols),
        ],
        axis=2,
    )
    request_grads = request_grads.astype(jnp.bfloat16).reshape(requests, pass_len, pair_cols)
    token_grads = jnp.concatenate([query_grad, gate_grad], axis=1)
    pass_low, tokens_in = lax.cond(
        fits,
        functools.partial(fold_rows, light, 2),
        functools.partial(fold_rows, plan, 3),
        table,
        final,
        request_grads,
        token_grads,
    )
    key_sums = pass_low[:, :, :head_cols].reshape(passages * pass_len, head_cols)
    partial = jnp.einsum("rc,rh->ch", flat_rows, key_sums, preferred_element_type=jnp.float32)
    partial = partial.reshape(ring, 2, model_width // (2 * ring), head_cols)
    d_tokens, d_store, d_wkey = tail(
        4,
        pass_low,
        partial,
        token_grads,
        tokens_in,
        (w_query, w_gate, wq_far, wg_far, w_key, w_value, wk_far, wv_far),
    )
    return d_tokens, d_store.reshape(passages // tp_count, pass_len, model_width), d_wkey


def solution(mesh):
    finer = Mesh(
        mesh.devices.reshape(mesh.shape["grp"], -1, 2, mesh.shape["tp"]),
        ("grp", "st_0", "st_1", "tp"),
    )
    in_specs = (
        P(GRP_ST, None),
        P(ST, None, "tp"),
        P(GRP_ST, "tp"),
        P(GRP_ST, "tp"),
        P(None, "tp"),
        P(None, "tp"),
        P(None, "tp"),
        P(None, "tp"),
        P(GRP_ST, "tp"),
    )
    out_specs = (P(GRP_ST_TP, None), P(GRP_ST_TP, None, None), P(GRP_ST, "tp"))
    return jax.shard_map(local, mesh=finer, in_specs=in_specs, out_specs=out_specs, check_vma=False)
```

```python
import functools

import jax
import jax.numpy as jnp
from jax import lax
from jax.experimental import pallas as pl
from jax.experimental.pallas import tpu as pltpu
from jax.sharding import Mesh
from jax.sharding import PartitionSpec as P

HD = 256
BLK = 128
PB = 4
MOST = 2
CHUNK = 4
LIGHT = (24, 22, 22, 20, 18, 16, 12, 4)
VMEM_LIMIT = 62 * 1024 * 1024
ST = ("st_0", "st_1")
GRP_ST = ("grp", "st_0", "st_1")
GRP_ST_TP = ("grp", "st_0", "st_1", "tp")
MESH_ID = pl.DeviceIdType.MESH
VMEM_SPEC = pl.BlockSpec(memory_space=pltpu.VMEM)
SMEM_SPEC = pl.BlockSpec(memory_space=pltpu.SMEM)
ANY_SPEC = pl.BlockSpec(memory_space=pl.ANY)
F32 = jnp.float32


class Plan:
    def __init__(self, ring, passages, light=False):
        self.ring = ring
        self.passages = passages
        self.reach = ring // 2
        self.steps_of = range(1, self.reach + 1)
        per_owner = 2 * MOST
        self.layout = {
            t: min(passages, per_owner * (self.reach - t + 1))
            + min(passages, per_owner * (self.reach - t))
            for t in self.steps_of
        }
        self.sizes = dict(self.layout)
        if light:
            self.sizes = {t: min(n, LIGHT[t - 1]) for t, n in self.layout.items()}
        self.base = [{}, {}]
        at = passages
        for d in range(2):
            for t in self.steps_of:
                self.base[d][t] = at
                at += -(-self.layout[t] // 2)
        self.slots = at

    def half(self, t):
        return -(-self.sizes[t] // 2) if t <= self.reach else 0

    def steps(self, down=False):
        for t in reversed(self.steps_of) if down else self.steps_of:
            for first in range(0, self.half(t), CHUNK):
                for d in range(2):
                    yield d, t, first, min(CHUNK, self.half(t) - first)


class Place:
    def __init__(self):
        self.g, self.z, self.k, self.x = (lax.axis_index(a) for a in GRP_ST_TP)
        self.ring = lax.axis_size("st_0")
        self.tp = lax.axis_size("tp")
        self.twin = (self.g, self.z, 1 - self.k, self.x)

    def along_z(self, step):
        return (self.g, lax.rem(self.z + step + self.ring, self.ring), self.k, self.x)

    def along_x(self, step):
        return (self.g, self.z, self.k, lax.rem(self.x + step + self.tp, self.tp))


def greet(*devices):
    barrier = pltpu.get_barrier_semaphore()
    for device in devices:
        pl.semaphore_signal(barrier, inc=1, device_id=device, device_id_type=MESH_ID)
    pl.semaphore_wait(barrier, len(devices))


class Copies:
    def __init__(self, send_sem, recv_sem):
        self.send_sem, self.recv_sem = send_sem, recv_sem
        self.all = []

    def start(self, src, dst, device):
        n = len(self.all)
        copy = pltpu.make_async_remote_copy(
            src_ref=src,
            dst_ref=dst,
            send_sem=self.send_sem.at[n],
            recv_sem=self.recv_sem.at[n],
            device_id=device,
            device_id_type=MESH_ID,
        )
        copy.start()
        self.all.append(copy)
        return copy

    def wait_sends(self):
        for copy in self.all:
            copy.wait_send()


def copy_sems(count):
    return [pltpu.SemaphoreType.DMA((count,)), pltpu.SemaphoreType.DMA((count,))]


def front_kernel(ids_ref, store_ref, wk_ref, wv_ref, ids_out, all_out, kv_out, total, *sems):
    gifts, ring_copies, x_copies = (Copies(*sems[2 * i : 2 * i + 2]) for i in range(3))
    place = Place()
    count = store_ref.shape[0]
    half = count // 2
    reach = place.ring // 2
    greet(place.along_z(1), place.along_z(-1), place.along_x(1), place.along_x(-1), place.twin)
    halves = (pl.ds(0, half), pl.ds(half, half))
    near = {}
    for d, step in ((0, 1), (1, -1)):
        for h in (d, 1 - d):
            near[d, h] = x_copies.start(
                store_ref.at[halves[h]], all_out.at[place.x, halves[h]], place.along_x(step)
            )
    gift = gifts.start(ids_ref, ids_out.at[place.z, place.k], place.twin)
    ids_out[place.z, place.k] = ids_ref[...]
    all_out[place.x] = store_ref[...]
    gift.wait_recv()
    hops = {}

    def hop(d, t):
        source = lax.rem(place.z + (t - 1) * (2 * d - 1) + place.ring, place.ring)
        part = ids_out.at[source]
        hops[d, t] = ring_copies.start(part, part, place.along_z(1 - 2 * d))

    def hops_until(first, last):
        for t in range(first, last):
            for d in range(2):
                if t > 1 and t <= reach - d:
                    hops[d, t - 1].wait_recv()
                if t <= reach - d:
                    hop(d, t)

    def add(source, start):
        rows = total.shape[0]
        depth = store_ref.shape[2]
        cols = wk_ref.shape[1]
        part = all_out[source].reshape(rows, depth)
        w_rows = pl.ds(pl.multiple_of(source * depth, depth), depth)
        for c, w_ref in enumerate((wk_ref, wv_ref)):
            at = slice(c * cols, (c + 1) * cols)
            term = jnp.dot(part, w_ref[w_rows, :], preferred_element_type=F32)
            total[:, at] = term if start else total[:, at] + term

    hops_until(1, 4)
    add(place.x, True)
    hops_until(4, 6)
    far = []
    for d, step in ((0, 1), (1, -1)):
        near[d, d].wait_recv()
        source = lax.rem(place.x - step + place.tp, place.tp)
        part = all_out.at[source, halves[d]]
        far.append(x_copies.start(part, part, place.along_x(step)))
    hops_until(6, reach + 1)
    for d, step in ((0, 1), (1, -1)):
        near[d, 1 - d].wait_recv()
        add(lax.rem(place.x - step + place.tp, place.tp), False)
    for d in range(2):
        hops[d, reach - d].wait_recv()
    for copy in far:
        copy.wait_recv()
    add(lax.rem(place.x + 2, place.tp), False)
    kv_out[...] = total[...].reshape(kv_out.shape).astype(kv_out.dtype)
    for group in (gifts, ring_copies, x_copies):
        group.wait_sends()


def front(ident, ids, store, w_key, w_value):
    count, rows, cols = store.shape
    ring, tp = lax.axis_size("st_0"), lax.axis_size("tp")
    pair = 2 * w_key.shape[1]
    return pl.pallas_call(
        front_kernel,
        out_shape=[
            jax.ShapeDtypeStruct((ring, 2, *ids.shape), ids.dtype),
            jax.ShapeDtypeStruct((tp, *store.shape), store.dtype),
            jax.ShapeDtypeStruct((count, rows, pair), store.dtype),
        ],
        in_specs=[VMEM_SPEC] * 4,
        out_specs=[VMEM_SPEC] * 3,
        scratch_shapes=[pltpu.VMEM((count * rows, pair), F32)]
        + copy_sems(1)
        + copy_sems(ring - 1)
        + copy_sems(6),
        compiler_params=pltpu.CompilerParams(
            collective_id=ident, has_side_effects=True, vmem_limit_bytes=VMEM_LIMIT
        ),
        name="front",
    )(ids, store, w_key, w_value)


def attend_kernel(scale, q_ref, gate_ref, mem_ref, kv_ref, grads_ref, tokens_ref):
    blocks = q_ref.shape[0] // BLK
    cols = q_ref.shape[1]
    pass_len = kv_ref.shape[1]
    low = q_ref.dtype

    def dot(a, b, ca, cb):
        return lax.dot_general(a, b, (((ca,), (cb,)), ((), ())), preferred_element_type=F32)

    for b in range(blocks):
        toks = pl.ds(b * BLK, BLK)
        kv = kv_ref[pl.ds(b * PB, PB)].reshape(PB * pass_len, 2 * cols)
        for h in range(cols // HD):
            k_at = slice(h * HD, (h + 1) * HD)
            v_at = slice(cols + h * HD, cols + (h + 1) * HD)
            q, keys, values = q_ref[toks, k_at], kv[:, k_at], kv[:, v_at]
            scores = dot(q, keys, 1, 1) * scale
            shifted = jnp.exp(scores - jnp.max(scores, axis=-1, keepdims=True))
            probs = shifted / jnp.sum(shifted, axis=-1, keepdims=True)
            probs_low = probs.astype(low)
            attended = dot(probs_low, values, 1, 0)
            gate = gate_ref[toks, k_at].astype(F32)
            mem = mem_ref[toks, k_at].astype(F32)
            sig = jax.nn.sigmoid(gate)
            attended_grad = (gate * sig * mem).astype(low)
            gate_grad = mem * attended * sig * (1.0 + gate * (1.0 - sig))
            prob_grad = dot(attended_grad, values, 1, 1)
            inner = jnp.sum(probs * prob_grad, axis=-1, keepdims=True)
            score_grad = (scale * probs * (prob_grad - inner)).astype(low)
            tokens_ref[toks, k_at] = dot(score_grad, keys, 1, 0).astype(low)
            tokens_ref[toks, v_at] = gate_grad.astype(low)
            key_grad = dot(score_grad, q, 0, 0).astype(low)
            value_grad = dot(probs_low, attended_grad, 0, 0).astype(low)
            passes = pl.ds(b * PB, PB)
            grads_ref[passes, :, k_at] = key_grad.reshape(PB, pass_len, HD)
            grads_ref[passes, :, v_at] = value_grad.reshape(PB, pass_len, HD)


def attend(queries, gate_pre, d_mem, request_kv):
    toks, cols = queries.shape
    _, pass_len, pair = request_kv.shape
    step = 2
    grid = toks // BLK // step
    tok_spec = pl.BlockSpec((step * BLK, cols), lambda i: (i, 0))
    kv_spec = pl.BlockSpec((step * PB, pass_len, pair), lambda i: (i, 0, 0))
    return pl.pallas_call(
        functools.partial(attend_kernel, HD**-0.5),
        grid=(grid,),
        out_shape=[
            jax.ShapeDtypeStruct(request_kv.shape, request_kv.dtype),
            jax.ShapeDtypeStruct((toks, pair), queries.dtype),
        ],
        in_specs=[tok_spec, tok_spec, tok_spec, kv_spec],
        out_specs=[kv_spec, pl.BlockSpec((step * BLK, pair), lambda i: (i, 0))],
        name="attend",
    )(queries, gate_pre, d_mem, request_kv)


def cast_kernel(plan, weights, order_ref, where_ref, kv_ref, *refs):
    w_refs, refs = refs[:weights], refs[weights:]
    out_ref, w_outs, refs = refs[0], refs[1 : 1 + weights], refs[1 + weights :]
    buf, first_buf, home, *sems = refs
    ring_copies, gifts, w_copies = (Copies(*sems[2 * i : 2 * i + 2]) for i in range(3))
    place = Place()
    count, slots = plan.passages, plan.slots
    top = plan.half(1)

    greet(place.along_z(1), place.along_z(-1), place.along_x(1), place.along_x(-1), place.twin)
    own_gift = gifts.start(kv_ref, home.at[pl.ds(count, count)], place.twin)

    @pl.loop(0, count)
    def _(j):
        home[j] = kv_ref[j]
        buf[j] = kv_ref[j]

    own_gift.wait_recv()

    @pl.loop(0, top)
    def _(j):
        for d in range(2):
            first_buf[d * top + j] = home[order_ref[d * count + j]]

    copies = {}
    steps = list(plan.steps())
    extent = {(d, t, first): size for d, t, first, size in steps}

    def send(d, t, first):
        size = extent[d, t, first]
        if t == 1:
            src = first_buf.at[pl.ds(d * top + first, size)]
        else:
            src = buf.at[pl.ds(plan.base[d][t - 1] + first, size)]
        dst = buf.at[pl.ds(plan.base[d][t] + first, size)]
        copies[d, t, first] = ring_copies.start(src, dst, place.along_z(1 - 2 * d))

    for d, t, first, _ in steps:
        if t == 1:
            send(d, t, first)
    rows = w_refs[0].shape[0] // 2
    half = pl.ds(place.k * rows, rows)
    arrive = [[], []]
    for w_ref, w_out in zip(w_refs, w_outs):
        arrive[0].append(
            w_copies.start(w_ref.at[half], w_out.at[2, half], place.along_x(1))
        )
        arrive[1].append(
            w_copies.start(w_ref.at[half], w_out.at[0, half], place.along_x(-1))
        )
    w_gifts = []
    middle = []

    def forward_weights():
        for copy in arrive[0] + arrive[1]:
            copy.wait_recv()
        for w_out in w_outs:
            middle.append(
                w_copies.start(
                    w_out.at[2 * place.k, half],
                    w_out.at[1, half],
                    place.along_x(2 * place.k - 1),
                )
            )
            for rel in (0, 2):
                part = w_out.at[rel, half]
                w_gifts.append(w_copies.start(part, part, place.twin))

    last = None
    for d, t, first, size in steps:
        if t != last and t == plan.reach // 2 + 1:
            forward_weights()
        last = t
        copies[d, t, first].wait_recv()
        if (d, t + 1, first) in extent:
            send(d, t + 1, first)
        at = plan.base[d][t] + first
        gifts.start(buf.at[pl.ds(at, size)], buf.at[pl.ds(slots + at, size)], place.twin)
    for copy, w_out in zip(middle, w_outs):
        copy.wait_recv()
        part = w_out.at[1, half]
        w_gifts.append(w_copies.start(part, part, place.twin))
    for gift in gifts.all[1:]:
        gift.wait_recv()

    @pl.loop(0, count)
    def _(j):
        buf[slots + j] = home[count + j]

    @pl.loop(0, out_ref.shape[0])
    def _(r):
        out_ref[r] = buf[where_ref[r]]

    for gift in w_gifts:
        gift.wait_recv()
    for group in (gifts, ring_copies, w_copies):
        group.wait_sends()


def cast_rows(plan, ident, order, where, kv, weights):
    count, rows, cols = kv.shape
    steps = len(list(plan.steps()))
    others = lax.axis_size("tp") - 1
    return pl.pallas_call(
        functools.partial(cast_kernel, plan, len(weights)),
        out_shape=[jax.ShapeDtypeStruct((where.shape[0], rows, cols), kv.dtype)]
        + [jax.ShapeDtypeStruct((others, *w.shape), w.dtype) for w in weights],
        in_specs=[SMEM_SPEC, SMEM_SPEC, VMEM_SPEC] + [ANY_SPEC] * len(weights),
        out_specs=[VMEM_SPEC] + [ANY_SPEC] * len(weights),
        scratch_shapes=[
            pltpu.VMEM((2 * plan.slots, rows, cols), kv.dtype),
            pltpu.VMEM((2 * plan.half(1), rows, cols), kv.dtype),
            pltpu.VMEM((2 * count, rows, cols), kv.dtype),
        ]
        + copy_sems(steps)
        + copy_sems(steps + 1)
        + copy_sems(6 * len(weights)),
        compiler_params=pltpu.CompilerParams(
            collective_id=ident, has_side_effects=True, vmem_limit_bytes=VMEM_LIMIT
        ),
        name="cast_rows",
    )(order, where, kv, *weights)


def fold_kernel(
    plan,
    table_ref,
    final_ref,
    grads_ref,
    tokens_ref,
    out_ref,
    tokens_out,
    held,
    here,
    sums,
    load_sem,
    *sems,
):
    ring_copies, gifts, exchange = (Copies(*sems[2 * i : 2 * i + 2]) for i in range(3))
    place = Place()
    count, top = plan.passages, plan.half(1)
    own = grads_ref.shape[0]
    readers = 2 * MOST
    twin_at = plan.slots - count
    zero_at = twin_at + plan.layout[1]
    peers = [place.along_x(rel) for rel in range(1, place.tp)]

    load = pltpu.make_async_copy(grads_ref, held.at[pl.ds(0, own)], load_sem)
    load.start()
    held[2 * own] = jnp.zeros_like(held[2 * own])
    here[zero_at] = jnp.zeros_like(here[zero_at])
    greet(place.along_z(1), place.along_z(-1), place.twin, *peers)
    own_gift = gifts.start(grads_ref, held.at[pl.ds(own, own)], place.twin)
    block = tokens_out.shape[1]
    for rel, peer in enumerate(peers, 1):
        exchange.start(
            tokens_ref.at[pl.ds(peer[3] * block, block)],
            tokens_out.at[place.tp - 1 - rel],
            peer,
        )
    load.wait()
    own_gift.wait_recv()

    def readers_sum(slot):
        total = held[table_ref[slot * readers]].astype(F32)
        for q in range(1, readers):
            total += held[table_ref[slot * readers + q]].astype(F32)
        return total

    copies = {}
    steps = list(plan.steps(down=True))
    extent = {(d, t, first): size for d, t, first, size in steps}
    for d, t, first, size in steps:
        at = plan.base[d][t] + first
        begin = extent.get((d, t + 1, first), 0)
        if begin:
            copies[d, t + 1, first].wait_recv()
            far_at = plan.base[d][t + 1] + first

            @pl.loop(0, begin)
            def _(j):
                total = readers_sum(at + j) + here[far_at - count + j].astype(F32)
                sums[at - count + j] = total.astype(sums.dtype)

        if begin < size:

            @pl.loop(begin, size)
            def _(j):
                sums[at - count + j] = readers_sum(at + j).astype(sums.dtype)

        part = pl.ds(at - count, size)
        copies[d, t, first] = ring_copies.start(
            sums.at[part], here.at[part], place.along_z(2 * d - 1)
        )
    for d, t, first, size in steps:
        if t == 1:
            copies[d, t, first].wait_recv()
            src = here.at[pl.ds(plan.base[d][1] - count + first, size)]
            dst = here.at[pl.ds(twin_at + d * (plan.layout[1] // 2) + first, size)]
            gifts.start(src, dst, place.twin)
    for gift in gifts.all[1:]:
        gift.wait_recv()

    @pl.loop(0, count)
    def _(p):
        total = readers_sum(p)
        for d in range(2):
            total += here[final_ref[d * count + p]].astype(F32)
        out_ref[p] = total.astype(out_ref.dtype)

    for copy in exchange.all:
        copy.wait_recv()
    for group in (gifts, ring_copies, exchange):
        group.wait_sends()


def fold_rows(plan, ident, table, final, grads, tokens):
    own, rows, cols = grads.shape
    steps = list(plan.steps())
    ends = sum(1 for _, t, _, _ in steps if t == 1)
    count = plan.passages
    tp = lax.axis_size("tp")
    return pl.pallas_call(
        functools.partial(fold_kernel, plan),
        out_shape=[
            jax.ShapeDtypeStruct((count, rows, cols), grads.dtype),
            jax.ShapeDtypeStruct((tp - 1, tokens.shape[0] // tp, tokens.shape[1]), tokens.dtype),
        ],
        in_specs=[SMEM_SPEC, SMEM_SPEC, ANY_SPEC, ANY_SPEC],
        out_specs=[VMEM_SPEC, ANY_SPEC],
        scratch_shapes=[
            pltpu.VMEM((2 * own + 1, rows, cols), grads.dtype),
            pltpu.VMEM((plan.slots - count + plan.layout[1] + 1, rows, cols), grads.dtype),
            pltpu.VMEM((plan.slots - count, rows, cols), grads.dtype),
            pltpu.SemaphoreType.DMA,
        ]
        + copy_sems(len(steps))
        + copy_sems(1 + ends)
        + copy_sems(tp - 1),
        compiler_params=pltpu.CompilerParams(
            collective_id=ident, has_side_effects=True, vmem_limit_bytes=VMEM_LIMIT
        ),
        name="fold_rows",
    )(table, final, grads, tokens)


def project(rows_list, weight_list, out_ref, n, tile):
    cols = pl.ds(n * tile, tile)
    total = None
    for rows, weight in zip(rows_list, weight_list):
        term = lax.dot_general(
            rows[...], weight[cols, :], (((1,), (1,)), ((), ())), preferred_element_type=F32
        )
        total = term if total is None else total + term
    out_ref[:, cols] = total.astype(out_ref.dtype)


def tail_kernel(sums_ref, all_ref, tokens_ref, tokens_in, *refs):
    weights, refs = refs[:8], refs[8:]
    d_tokens_ref, d_store_ref, d_wkey_ref = refs[:3]
    wbuf_t, wbuf_s, own_t, in_t, own_s, in_s, refs = *refs[3:9], refs[9:]
    keys, keys_turned, all_buf, terms, twin_terms, sent, come, last, last_in, refs = *refs[:9], refs[9:]
    load_sem, *sems = refs
    exchange, gifts, ring_copies = (Copies(*sems[2 * i : 2 * i + 2]) for i in range(3))
    place = Place()
    tp, ring = place.tp, place.ring
    reach = ring // 2
    peers = [place.along_x(rel) for rel in range(1, tp)]
    loads = []

    def load(src, dst):
        copy = pltpu.make_async_copy(src, dst, load_sem.at[len(loads)])
        copy.start()
        loads.append(copy)

    load(sums_ref, keys)
    for n in range(tp):
        load(all_ref.at[n], all_buf.at[n])
    greet(place.twin, place.along_z(1), place.along_z(-1), *peers)
    share = sums_ref.shape[0] // tp
    for rel, peer in enumerate(peers, 1):
        exchange.start(
            sums_ref.at[pl.ds(peer[3] * share, share)], in_s.at[tp - 1 - rel], peer
        )
    block = own_t.shape[0]
    load(tokens_ref.at[pl.ds(place.x * block, block)], own_t)
    load(tokens_in, in_t)
    load(sums_ref.at[pl.ds(place.x * share, share)], own_s)
    for wbuf, (wa, wb, wa_far, wb_far) in ((wbuf_t, weights[:4]), (wbuf_s, weights[4:])):
        load(wa, wbuf.at[0])
        load(wb, wbuf.at[1])
        load(wa_far, wbuf.at[pl.ds(2, tp - 1)])
        load(wb_far, wbuf.at[pl.ds(2 + tp - 1, tp - 1)])
    count, pass_len, pair = sums_ref.shape
    rows, cols = count * pass_len, pair // 2
    depth = all_ref.shape[3]
    width = terms.shape[3]
    loads[0].wait()
    keys_turned[...] = keys[:, :, :cols].reshape(rows, cols).T
    for n in range(tp):
        loads[1 + n].wait()
        term = jnp.dot(
            keys_turned[...], all_buf[n].reshape(rows, depth), preferred_element_type=F32
        )
        for c in range(depth // width):
            for h in range(2):
                terms[h, n * (depth // width) + c] = term[
                    h * (cols // 2) : (h + 1) * (cols // 2), c * width : (c + 1) * width
                ]
    gift = gifts.start(terms.at[1 - place.k], twin_terms, place.twin)
    for copy in loads[1 + tp :]:
        copy.wait()

    def operands(own, far_rows, wbuf):
        n_cols = own.shape[-1] // 2
        rows_list, weight_list = [], []
        for c in range(2):
            rows_list.append(own.at[:, pl.ds(c * n_cols, n_cols)])
            weight_list.append(wbuf.at[c])
        for rel in range(tp - 1):
            for c in range(2):
                rows_list.append(far_rows.at[rel, :, pl.ds(c * n_cols, n_cols)])
                weight_list.append(wbuf.at[2 + c * (tp - 1) + rel])
        return rows_list, weight_list

    part_rows = share * pass_len
    tile = 512
    tiles = d_tokens_ref.shape[1] // tile
    for_tokens = operands(own_t, in_t, wbuf_t)
    for_store = operands(
        own_s.reshape(part_rows, pair), in_s.reshape(tp - 1, part_rows, pair), wbuf_s
    )
    gift.wait_recv()
    hops = {}

    def mine(dest):
        return terms[place.k, dest] + twin_terms[dest]

    done = 0
    for s in range(1, reach + 1):
        for d in range(2):
            to_go = reach - d + 1 - s
            if to_go < 1:
                continue
            turn = 1 - 2 * d
            total = mine(lax.rem(place.z + turn * to_go + ring, ring))
            n = d * reach + s - 1
            if s > 1:
                hops[d, s - 1].wait_recv()
                total += come[n - 1].astype(F32)
            sent[n] = total.astype(sent.dtype)
            hops[d, s] = ring_copies.start(sent.at[n], come.at[n], place.along_z(turn))
        if s == reach // 2:
            for copy in exchange.all:
                copy.wait_recv()
        if s <= reach // 2:
            for _ in range(-(-tiles // (reach // 2))):
                if done < tiles:
                    project(*for_tokens, d_tokens_ref, done, tile)
                    done += 1
        elif s < reach:
            for _ in range(-(-tiles // (reach // 2 - 1))):
                if done < 2 * tiles:
                    project(*for_store, d_store_ref, done - tiles, tile)
                    done += 1
    total = mine(place.z)
    for d in range(2):
        hops[d, reach - d].wait_recv()
        total += come[d * reach + reach - d - 1].astype(F32)
    turned = total.T
    out_rows = turned.shape[0] // 2
    for c in range(2):
        last[c] = turned[c * out_rows : (c + 1) * out_rows]
    end = gifts.start(last.at[1 - place.k], last_in, place.twin)
    half = cols // 2
    d_wkey_ref[:, pl.ds(pl.multiple_of(place.k * half, half), half)] = last[place.k]
    end.wait_recv()
    d_wkey_ref[:, pl.ds(pl.multiple_of((1 - place.k) * half, half), half)] = last_in[...]
    for group in (exchange, gifts, ring_copies):
        group.wait_sends()


def tail(ident, sums, all_rows, tokens, tokens_in, weights):
    tp, ring = lax.axis_size("tp"), lax.axis_size("st_0")
    model, head_cols = weights[0].shape
    count, pass_len, pair = sums.shape
    share = count // tp
    width = model // ring
    low = sums.dtype
    return pl.pallas_call(
        tail_kernel,
        out_shape=[
            jax.ShapeDtypeStruct((tokens.shape[0] // tp, model), low),
            jax.ShapeDtypeStruct((share * pass_len, model), low),
            jax.ShapeDtypeStruct((width // 2, head_cols), F32),
        ],
        in_specs=[ANY_SPEC] * (4 + len(weights)),
        out_specs=[VMEM_SPEC] * 3,
        scratch_shapes=[
            pltpu.VMEM((2 * tp, model, head_cols), low),
            pltpu.VMEM((2 * tp, model, head_cols), low),
            pltpu.VMEM((tokens.shape[0] // tp, tokens.shape[1]), low),
            pltpu.VMEM(tokens_in.shape, low),
            pltpu.VMEM((share, pass_len, pair), low),
            pltpu.VMEM((tp - 1, share, pass_len, pair), low),
            pltpu.VMEM(sums.shape, low),
            pltpu.VMEM((head_cols, count * pass_len), low),
            pltpu.VMEM(all_rows.shape, low),
            pltpu.VMEM((2, ring, head_cols // 2, width), F32),
            pltpu.VMEM((ring, head_cols // 2, width), F32),
            pltpu.VMEM((ring, head_cols // 2, width), low),
            pltpu.VMEM((ring, head_cols // 2, width), low),
            pltpu.VMEM((2, width // 2, head_cols // 2), F32),
            pltpu.VMEM((width // 2, head_cols // 2), F32),
            pltpu.SemaphoreType.DMA((4 + tp + len(weights),)),
        ]
        + copy_sems(tp - 1)
        + copy_sems(2)
        + copy_sems(ring - 1),
        compiler_params=pltpu.CompilerParams(
            collective_id=ident, has_side_effects=True, vmem_limit_bytes=VMEM_LIMIT
        ),
        name="tail",
    )(sums, all_rows, tokens, tokens_in, *weights)


def first_slot(plan, d, step):
    total = jnp.zeros_like(step)
    for t, at in plan.base[d].items():
        total = total + jnp.where(step == t, at, 0)
    return total


def routes(plan, light, ids):
    count, ring, slots = plan.passages, plan.ring, plan.slots
    me_z, me_k = lax.axis_index("st_0"), lax.axis_index("st_1")
    devices, requests = ids.shape
    pair = 2 * count
    every = jnp.arange(devices * count, dtype=jnp.int32)
    owner = ids // count
    owner_z, owner_k = owner // 2, owner % 2
    reader_z = (jnp.arange(devices, dtype=jnp.int32) // 2)[:, None]
    away = jnp.mod(reader_z - owner_z, ring)
    up = (2 * away < ring) | ((2 * away == ring) & (owner_k == 0))
    steps = (jnp.where(up, away, 0), jnp.where(up, 0, ring - away))
    hot = ids.reshape(-1)[:, None] == every[None, :]
    place = jnp.arange(pair, dtype=jnp.int32)
    ranks, fars = [], []
    fits = jnp.bool_(True)
    for d in range(2):
        far = jnp.max(jnp.where(hot, steps[d].reshape(-1)[:, None], 0), axis=0)
        far = far.reshape(ring, pair)
        before = (far[:, None, :] > far[:, :, None]) | (
            (far[:, None, :] == far[:, :, None]) & (place[None, None, :] < place[None, :, None])
        )
        ranks.append(jnp.sum(before.astype(jnp.int32), axis=2))
        fars.append(far)
        bounds = jnp.array([light.sizes[t] for t in light.steps_of], jnp.int32)
        dist = jnp.arange(1, plan.reach + 1, dtype=jnp.int32)
        sent = jnp.sum((far[:, None, :] >= dist[None, :, None]).astype(jnp.int32), axis=2)
        fits &= jnp.all(sent <= bounds[None, :])

    def chip(array):
        return lax.dynamic_slice_in_dim(array, me_z, 1, axis=0)[0]

    def readers(array):
        return lax.dynamic_slice_in_dim(array, me_z * 2, 2, axis=0).reshape(-1)

    at_home = place % count + jnp.where(place // count == me_k, 0, count)
    want = 2 * jnp.arange(count, dtype=jnp.int32) + me_k
    order, final = [], []
    for d in range(2):
        rank, far = chip(ranks[d]), chip(fars[d])
        order.append(jnp.sum(jnp.where(rank[None, :] == want[:, None], at_home[None, :], 0), axis=1))
        twin_at = plan.slots - count
        near = plan.base[d][1] - count
        aside = twin_at + d * (plan.layout[1] // 2)
        index = jnp.where(rank % 2 == me_k, near, aside) + rank // 2
        index = jnp.where(far > 0, index, twin_at + plan.layout[1])
        final.append(lax.dynamic_slice_in_dim(index, me_k * count, count, axis=0))
    chip_ids = readers(ids)
    chip_hot = chip_ids[:, None] == every[None, :]
    slot, core = chip_ids % count, readers(owner_k)
    for d in range(2):
        rank = jnp.sum(jnp.where(chip_hot, ranks[d].reshape(-1)[None, :], 0), axis=1)
        step = readers(steps[d] * (away > 0))
        slot = jnp.where(step > 0, first_slot(plan, d, step) + rank // 2, slot)
        core = jnp.where(step > 0, rank % 2, core)
    where = slot + jnp.where(core == me_k, 0, slots)
    where = lax.dynamic_slice_in_dim(where, me_k * requests, requests, axis=0)
    mine = jnp.where(core == me_k, slot, -1).reshape(2, requests)
    mine = jnp.where(me_k == 0, mine, mine[::-1]).reshape(-1)
    at_slot = mine[:, None] == jnp.arange(slots, dtype=jnp.int32)[None, :]
    turn = jnp.cumsum(at_slot.astype(jnp.int32), axis=0)
    number = jnp.arange(2 * requests, dtype=jnp.int32)[:, None]
    table = jnp.stack(
        [
            jnp.min(jnp.where(at_slot & (turn == q + 1), number, 2 * requests), axis=0)
            for q in range(2 * MOST)
        ],
        axis=1,
    ).reshape(-1)
    tables = (jnp.concatenate(order), where, table, jnp.concatenate(final))
    return fits, *(t.astype(jnp.int32) for t in tables)


def local(pass_ids, store, queries, gate_pre, w_query, w_gate, w_key, w_value, d_mem):
    tp_count = lax.axis_size("tp")
    ring = lax.axis_size("st_0")
    passages, pass_len, _ = store.shape
    model_width = w_key.shape[0]
    requests = pass_ids.size
    plan = Plan(ring, passages)
    light = Plan(ring, passages, light=True)
    ids = jnp.zeros((8, 128), jnp.int32).at[0, :requests].set(pass_ids.reshape(-1))
    ids, all_rows, kv = front(5, ids, store, w_key, w_value)
    fits, order, where, table, final = routes(
        plan, light, ids[:, :, 0, :requests].reshape(2 * ring, requests)
    )
    weights = (w_query, w_gate, w_key, w_value)
    request_kv, wq_far, wg_far, wk_far, wv_far = lax.cond(
        fits,
        functools.partial(cast_rows, light, 0),
        functools.partial(cast_rows, plan, 1),
        order,
        where,
        kv,
        weights,
    )
    request_grads, token_grads = attend(queries, gate_pre, d_mem, request_kv)
    sums, tokens_in = lax.cond(
        fits,
        functools.partial(fold_rows, light, 2),
        functools.partial(fold_rows, plan, 3),
        table,
        final,
        request_grads,
        token_grads,
    )
    d_tokens, d_store, d_wkey = tail(
        4,
        sums,
        all_rows,
        token_grads,
        tokens_in,
        (w_query, w_gate, wq_far, wg_far, w_key, w_value, wk_far, wv_far),
    )
    return d_tokens, d_store.reshape(passages // tp_count, pass_len, model_width), d_wkey


def solution(mesh):
    finer = Mesh(
        mesh.devices.reshape(mesh.shape["grp"], -1, 2, mesh.shape["tp"]),
        ("grp", "st_0", "st_1", "tp"),
    )
    in_specs = (
        P(GRP_ST, None),
        P(ST, None, "tp"),
        P(GRP_ST, "tp"),
        P(GRP_ST, "tp"),
        P(None, "tp"),
        P(None, "tp"),
        P(None, "tp"),
        P(None, "tp"),
        P(GRP_ST, "tp"),
    )
    out_specs = (P(GRP_ST_TP, None), P(GRP_ST_TP, None, None), P(GRP_ST, "tp"))
    return jax.shard_map(local, mesh=finer, in_specs=in_specs, out_specs=out_specs, check_vma=False)
```

```python
import functools

import jax
import jax.numpy as jnp
from jax import lax
from jax.experimental import pallas as pl
from jax.experimental.pallas import tpu as pltpu
from jax.sharding import Mesh
from jax.sharding import PartitionSpec as P

HD = 256
BLK = 128
PB = 4
MOST = 2
CHUNK = 4
LENGTH = 54
STAGE = 2
LAG = 2 * STAGE
VMEM_LIMIT = 62 * 1024 * 1024
ST = ("st_0", "st_1")
GRP_ST = ("grp", "st_0", "st_1")
GRP_ST_TP = ("grp", "st_0", "st_1", "tp")
MESH_ID = pl.DeviceIdType.MESH
VMEM_SPEC = pl.BlockSpec(memory_space=pltpu.VMEM)
SMEM_SPEC = pl.BlockSpec(memory_space=pltpu.SMEM)
ANY_SPEC = pl.BlockSpec(memory_space=pl.ANY)
F32 = jnp.float32


class Plan:
    def __init__(self, ring, passages):
        self.ring = ring
        self.passages = passages
        self.reach = ring // 2
        self.steps_of = range(1, self.reach + 1)
        per_owner = 2 * MOST
        self.layout = {
            t: min(passages, per_owner * (self.reach - t + 1))
            + min(passages, per_owner * (self.reach - t))
            for t in self.steps_of
        }
        self.sizes = self.layout
        self.base = [{}, {}]
        at = passages
        for d in range(2):
            for t in self.steps_of:
                self.base[d][t] = at
                at += -(-self.layout[t] // 2)
        self.slots = at

    def half(self, t):
        return -(-self.sizes[t] // 2) if t <= self.reach else 0

    def steps(self, down=False):
        for t in reversed(self.steps_of) if down else self.steps_of:
            for first in range(0, self.half(t), CHUNK):
                for d in range(2):
                    yield d, t, first, min(CHUNK, self.half(t) - first)


class Place:
    def __init__(self):
        self.g, self.z, self.k, self.x = (lax.axis_index(a) for a in GRP_ST_TP)
        self.ring = lax.axis_size("st_0")
        self.tp = lax.axis_size("tp")
        self.twin = (self.g, self.z, 1 - self.k, self.x)

    def along_z(self, step):
        return (self.g, lax.rem(self.z + step + self.ring, self.ring), self.k, self.x)

    def along_x(self, step):
        return (self.g, self.z, self.k, lax.rem(self.x + step + self.tp, self.tp))


def greet(*devices):
    barrier = pltpu.get_barrier_semaphore()
    for device in devices:
        pl.semaphore_signal(barrier, inc=1, device_id=device, device_id_type=MESH_ID)
    pl.semaphore_wait(barrier, len(devices))


class Copies:
    def __init__(self, send_sem, recv_sem):
        self.send_sem, self.recv_sem = send_sem, recv_sem
        self.all = []

    def start(self, src, dst, device):
        n = len(self.all)
        copy = pltpu.make_async_remote_copy(
            src_ref=src,
            dst_ref=dst,
            send_sem=self.send_sem.at[n],
            recv_sem=self.recv_sem.at[n],
            device_id=device,
            device_id_type=MESH_ID,
        )
        copy.start()
        self.all.append(copy)
        return copy

    def wait_sends(self):
        for copy in self.all:
            copy.wait_send()


def copy_sems(count):
    return [pltpu.SemaphoreType.DMA((count,)), pltpu.SemaphoreType.DMA((count,))]


def front_kernel(ids_ref, store_ref, wk_ref, wv_ref, ids_out, all_out, kv_out, total, *sems):
    gifts, ring_copies, x_copies = (Copies(*sems[2 * i : 2 * i + 2]) for i in range(3))
    place = Place()
    count = store_ref.shape[0]
    half = count // 2
    reach = place.ring // 2
    greet(place.along_z(1), place.along_z(-1), place.along_x(1), place.along_x(-1), place.twin)
    halves = (pl.ds(0, half), pl.ds(half, half))
    near = {}
    for d, step in ((0, 1), (1, -1)):
        for h in (d, 1 - d):
            near[d, h] = x_copies.start(
                store_ref.at[halves[h]], all_out.at[place.x, halves[h]], place.along_x(step)
            )
    gift = gifts.start(ids_ref, ids_out.at[place.z, place.k], place.twin)
    ids_out[place.z, place.k] = ids_ref[...]
    all_out[place.x] = store_ref[...]
    gift.wait_recv()
    hops = {}

    def hop(d, t):
        source = lax.rem(place.z + (t - 1) * (2 * d - 1) + place.ring, place.ring)
        part = ids_out.at[source]
        hops[d, t] = ring_copies.start(part, part, place.along_z(1 - 2 * d))

    def hops_until(first, last):
        for t in range(first, last):
            for d in range(2):
                if t > 1 and t <= reach - d:
                    hops[d, t - 1].wait_recv()
                if t <= reach - d:
                    hop(d, t)

    def add(source, start):
        rows = total.shape[0]
        depth = store_ref.shape[2]
        cols = wk_ref.shape[1]
        part = all_out[source].reshape(rows, depth)
        w_rows = pl.ds(pl.multiple_of(source * depth, depth), depth)
        for c, w_ref in enumerate((wk_ref, wv_ref)):
            at = slice(c * cols, (c + 1) * cols)
            term = jnp.dot(part, w_ref[w_rows, :], preferred_element_type=F32)
            total[:, at] = term if start else total[:, at] + term

    hops_until(1, 4)
    add(place.x, True)
    hops_until(4, 6)
    far = []
    for d, step in ((0, 1), (1, -1)):
        near[d, d].wait_recv()
        source = lax.rem(place.x - step + place.tp, place.tp)
        part = all_out.at[source, halves[d]]
        far.append(x_copies.start(part, part, place.along_x(step)))
    hops_until(6, reach + 1)
    for d, step in ((0, 1), (1, -1)):
        near[d, 1 - d].wait_recv()
        add(lax.rem(place.x - step + place.tp, place.tp), False)
    for d in range(2):
        hops[d, reach - d].wait_recv()
    for copy in far:
        copy.wait_recv()
    add(lax.rem(place.x + 2, place.tp), False)
    kv_out[...] = total[...].reshape(kv_out.shape).astype(kv_out.dtype)
    for group in (gifts, ring_copies, x_copies):
        group.wait_sends()


def front(ident, ids, store, w_key, w_value):
    count, rows, cols = store.shape
    ring, tp = lax.axis_size("st_0"), lax.axis_size("tp")
    pair = 2 * w_key.shape[1]
    return pl.pallas_call(
        front_kernel,
        out_shape=[
            jax.ShapeDtypeStruct((ring, 2, *ids.shape), ids.dtype),
            jax.ShapeDtypeStruct((tp, *store.shape), store.dtype),
            jax.ShapeDtypeStruct((count, rows, pair), store.dtype),
        ],
        in_specs=[VMEM_SPEC] * 4,
        out_specs=[VMEM_SPEC] * 3,
        scratch_shapes=[pltpu.VMEM((count * rows, pair), F32)]
        + copy_sems(1)
        + copy_sems(ring - 1)
        + copy_sems(6),
        compiler_params=pltpu.CompilerParams(
            collective_id=ident, has_side_effects=True, vmem_limit_bytes=VMEM_LIMIT
        ),
        name="front",
    )(ids, store, w_key, w_value)


def attend_kernel(scale, q_ref, gate_ref, mem_ref, kv_ref, grads_ref, tokens_ref):
    blocks = q_ref.shape[0] // BLK
    cols = q_ref.shape[1]
    pass_len = kv_ref.shape[1]
    low = q_ref.dtype

    def dot(a, b, ca, cb):
        return lax.dot_general(a, b, (((ca,), (cb,)), ((), ())), preferred_element_type=F32)

    for b in range(blocks):
        toks = pl.ds(b * BLK, BLK)
        kv = kv_ref[pl.ds(b * PB, PB)].reshape(PB * pass_len, 2 * cols)
        for h in range(cols // HD):
            k_at = slice(h * HD, (h + 1) * HD)
            v_at = slice(cols + h * HD, cols + (h + 1) * HD)
            q, keys, values = q_ref[toks, k_at], kv[:, k_at], kv[:, v_at]
            scores = dot(q, keys, 1, 1) * scale
            shifted = jnp.exp(scores - jnp.max(scores, axis=-1, keepdims=True))
            probs = shifted / jnp.sum(shifted, axis=-1, keepdims=True)
            probs_low = probs.astype(low)
            attended = dot(probs_low, values, 1, 0)
            gate = gate_ref[toks, k_at].astype(F32)
            mem = mem_ref[toks, k_at].astype(F32)
            sig = jax.nn.sigmoid(gate)
            attended_grad = (gate * sig * mem).astype(low)
            gate_grad = mem * attended * sig * (1.0 + gate * (1.0 - sig))
            prob_grad = dot(attended_grad, values, 1, 1)
            inner = jnp.sum(probs * prob_grad, axis=-1, keepdims=True)
            score_grad = (scale * probs * (prob_grad - inner)).astype(low)
            tokens_ref[toks, k_at] = dot(score_grad, keys, 1, 0).astype(low)
            tokens_ref[toks, v_at] = gate_grad.astype(low)
            key_grad = dot(score_grad, q, 0, 0).astype(low)
            value_grad = dot(probs_low, attended_grad, 0, 0).astype(low)
            passes = pl.ds(b * PB, PB)
            grads_ref[passes, :, k_at] = key_grad.reshape(PB, pass_len, HD)
            grads_ref[passes, :, v_at] = value_grad.reshape(PB, pass_len, HD)


def attend(queries, gate_pre, d_mem, request_kv):
    toks, cols = queries.shape
    _, pass_len, pair = request_kv.shape
    step = 2
    grid = toks // BLK // step
    tok_spec = pl.BlockSpec((step * BLK, cols), lambda i: (i, 0))
    kv_spec = pl.BlockSpec((step * PB, pass_len, pair), lambda i: (i, 0, 0))
    return pl.pallas_call(
        functools.partial(attend_kernel, HD**-0.5),
        grid=(grid,),
        out_shape=[
            jax.ShapeDtypeStruct(request_kv.shape, request_kv.dtype),
            jax.ShapeDtypeStruct((toks, pair), queries.dtype),
        ],
        in_specs=[tok_spec, tok_spec, tok_spec, kv_spec],
        out_specs=[kv_spec, pl.BlockSpec((step * BLK, pair), lambda i: (i, 0))],
        name="attend",
    )(queries, gate_pre, d_mem, request_kv)


def cast_kernel(plan, weights, order_ref, where_ref, kv_ref, *refs):
    w_refs, refs = refs[:weights], refs[weights:]
    out_ref, w_outs, refs = refs[0], refs[1 : 1 + weights], refs[1 + weights :]
    buf, first_buf, home, *sems = refs
    ring_copies, gifts, w_copies = (Copies(*sems[2 * i : 2 * i + 2]) for i in range(3))
    place = Place()
    count, slots = plan.passages, plan.slots
    top = plan.half(1)

    greet(place.along_z(1), place.along_z(-1), place.along_x(1), place.along_x(-1), place.twin)
    own_gift = gifts.start(kv_ref, home.at[pl.ds(count, count)], place.twin)

    @pl.loop(0, count)
    def _(j):
        home[j] = kv_ref[j]
        buf[j] = kv_ref[j]

    own_gift.wait_recv()

    @pl.loop(0, top)
    def _(j):
        for d in range(2):
            first_buf[d * top + j] = home[order_ref[d * count + j]]

    copies = {}
    steps = list(plan.steps())
    extent = {(d, t, first): size for d, t, first, size in steps}

    def send(d, t, first):
        size = extent[d, t, first]
        if t == 1:
            src = first_buf.at[pl.ds(d * top + first, size)]
        else:
            src = buf.at[pl.ds(plan.base[d][t - 1] + first, size)]
        dst = buf.at[pl.ds(plan.base[d][t] + first, size)]
        copies[d, t, first] = ring_copies.start(src, dst, place.along_z(1 - 2 * d))

    for d, t, first, _ in steps:
        if t == 1:
            send(d, t, first)
    rows = w_refs[0].shape[0] // 2
    half = pl.ds(place.k * rows, rows)
    arrive = [[], []]
    for w_ref, w_out in zip(w_refs, w_outs):
        arrive[0].append(
            w_copies.start(w_ref.at[half], w_out.at[2, half], place.along_x(1))
        )
        arrive[1].append(
            w_copies.start(w_ref.at[half], w_out.at[0, half], place.along_x(-1))
        )
    w_gifts = []
    middle = []

    def forward_weights():
        for copy in arrive[0] + arrive[1]:
            copy.wait_recv()
        for w_out in w_outs:
            middle.append(
                w_copies.start(
                    w_out.at[2 * place.k, half],
                    w_out.at[1, half],
                    place.along_x(2 * place.k - 1),
                )
            )
            for rel in (0, 2):
                part = w_out.at[rel, half]
                w_gifts.append(w_copies.start(part, part, place.twin))

    last = None
    for d, t, first, size in steps:
        if t != last and t == plan.reach // 2 + 1:
            forward_weights()
        last = t
        copies[d, t, first].wait_recv()
        if (d, t + 1, first) in extent:
            send(d, t + 1, first)
        at = plan.base[d][t] + first
        gifts.start(buf.at[pl.ds(at, size)], buf.at[pl.ds(slots + at, size)], place.twin)
    for copy, w_out in zip(middle, w_outs):
        copy.wait_recv()
        part = w_out.at[1, half]
        w_gifts.append(w_copies.start(part, part, place.twin))
    for gift in gifts.all[1:]:
        gift.wait_recv()

    @pl.loop(0, count)
    def _(j):
        buf[slots + j] = home[count + j]

    @pl.loop(0, out_ref.shape[0])
    def _(r):
        out_ref[r] = buf[where_ref[r]]

    for gift in w_gifts:
        gift.wait_recv()
    for group in (gifts, ring_copies, w_copies):
        group.wait_sends()


def cast_rows(plan, ident, order, where, kv, weights):
    count, rows, cols = kv.shape
    steps = len(list(plan.steps()))
    others = lax.axis_size("tp") - 1
    return pl.pallas_call(
        functools.partial(cast_kernel, plan, len(weights)),
        out_shape=[jax.ShapeDtypeStruct((where.shape[0], rows, cols), kv.dtype)]
        + [jax.ShapeDtypeStruct((others, *w.shape), w.dtype) for w in weights],
        in_specs=[SMEM_SPEC, SMEM_SPEC, VMEM_SPEC] + [ANY_SPEC] * len(weights),
        out_specs=[VMEM_SPEC] + [ANY_SPEC] * len(weights),
        scratch_shapes=[
            pltpu.VMEM((2 * plan.slots, rows, cols), kv.dtype),
            pltpu.VMEM((2 * plan.half(1), rows, cols), kv.dtype),
            pltpu.VMEM((2 * count, rows, cols), kv.dtype),
        ]
        + copy_sems(steps)
        + copy_sems(steps + 1)
        + copy_sems(6 * len(weights)),
        compiler_params=pltpu.CompilerParams(
            collective_id=ident, has_side_effects=True, vmem_limit_bytes=VMEM_LIMIT
        ),
        name="cast_rows",
    )(order, where, kv, *weights)


def fold_kernel(
    plan,
    table_ref,
    final_ref,
    grads_ref,
    tokens_ref,
    out_ref,
    tokens_out,
    held,
    here,
    sums,
    load_sem,
    *sems,
):
    ring_copies, gifts, exchange = (Copies(*sems[2 * i : 2 * i + 2]) for i in range(3))
    place = Place()
    count, top = plan.passages, plan.half(1)
    own = grads_ref.shape[0]
    readers = 2 * MOST
    twin_at = plan.slots - count
    zero_at = twin_at + plan.layout[1]
    peers = [place.along_x(rel) for rel in range(1, place.tp)]

    load = pltpu.make_async_copy(grads_ref, held.at[pl.ds(0, own)], load_sem)
    load.start()
    held[2 * own] = jnp.zeros_like(held[2 * own])
    here[zero_at] = jnp.zeros_like(here[zero_at])
    greet(place.along_z(1), place.along_z(-1), place.twin, *peers)
    own_gift = gifts.start(grads_ref, held.at[pl.ds(own, own)], place.twin)
    block = tokens_out.shape[1]
    for rel, peer in enumerate(peers, 1):
        exchange.start(
            tokens_ref.at[pl.ds(peer[3] * block, block)],
            tokens_out.at[place.tp - 1 - rel],
            peer,
        )
    load.wait()
    own_gift.wait_recv()

    def readers_sum(slot):
        total = held[table_ref[slot * readers]].astype(F32)
        for q in range(1, readers):
            total += held[table_ref[slot * readers + q]].astype(F32)
        return total

    copies = {}
    steps = list(plan.steps(down=True))
    extent = {(d, t, first): size for d, t, first, size in steps}
    for d, t, first, size in steps:
        at = plan.base[d][t] + first
        begin = extent.get((d, t + 1, first), 0)
        if begin:
            copies[d, t + 1, first].wait_recv()
            far_at = plan.base[d][t + 1] + first

            @pl.loop(0, begin)
            def _(j):
                total = readers_sum(at + j) + here[far_at - count + j].astype(F32)
                sums[at - count + j] = total.astype(sums.dtype)

        if begin < size:

            @pl.loop(begin, size)
            def _(j):
                sums[at - count + j] = readers_sum(at + j).astype(sums.dtype)

        part = pl.ds(at - count, size)
        copies[d, t, first] = ring_copies.start(
            sums.at[part], here.at[part], place.along_z(2 * d - 1)
        )
    for d, t, first, size in steps:
        if t == 1:
            copies[d, t, first].wait_recv()
            src = here.at[pl.ds(plan.base[d][1] - count + first, size)]
            dst = here.at[pl.ds(twin_at + d * (plan.layout[1] // 2) + first, size)]
            gifts.start(src, dst, place.twin)
    for gift in gifts.all[1:]:
        gift.wait_recv()

    @pl.loop(0, count)
    def _(p):
        total = readers_sum(p)
        for d in range(2):
            total += here[final_ref[d * count + p]].astype(F32)
        out_ref[p] = total.astype(out_ref.dtype)

    for copy in exchange.all:
        copy.wait_recv()
    for group in (gifts, ring_copies, exchange):
        group.wait_sends()


def fold_rows(plan, ident, table, final, grads, tokens):
    own, rows, cols = grads.shape
    steps = list(plan.steps())
    ends = sum(1 for _, t, _, _ in steps if t == 1)
    count = plan.passages
    tp = lax.axis_size("tp")
    return pl.pallas_call(
        functools.partial(fold_kernel, plan),
        out_shape=[
            jax.ShapeDtypeStruct((count, rows, cols), grads.dtype),
            jax.ShapeDtypeStruct((tp - 1, tokens.shape[0] // tp, tokens.shape[1]), tokens.dtype),
        ],
        in_specs=[SMEM_SPEC, SMEM_SPEC, ANY_SPEC, ANY_SPEC],
        out_specs=[VMEM_SPEC, ANY_SPEC],
        scratch_shapes=[
            pltpu.VMEM((2 * own + 1, rows, cols), grads.dtype),
            pltpu.VMEM((plan.slots - count + plan.layout[1] + 1, rows, cols), grads.dtype),
            pltpu.VMEM((plan.slots - count, rows, cols), grads.dtype),
            pltpu.SemaphoreType.DMA,
        ]
        + copy_sems(len(steps))
        + copy_sems(1 + ends)
        + copy_sems(tp - 1),
        compiler_params=pltpu.CompilerParams(
            collective_id=ident, has_side_effects=True, vmem_limit_bytes=VMEM_LIMIT
        ),
        name="fold_rows",
    )(table, final, grads, tokens)


def copy_slots(src, src_at, dst, dst_at, size):
    @pl.loop(0, size)
    def _(j):
        dst[dst_at + j] = src[src_at + j]


class WeightShare:
    def __init__(self, place, copies, w_refs, w_outs):
        self.place, self.copies, self.outs = place, copies, w_outs
        rows = w_refs[0].shape[0] // 2
        self.half = pl.ds(place.k * rows, rows)
        self.near, self.middle, self.gifts = [], [], []
        for w_ref, w_out in zip(w_refs, w_outs):
            for slot, step in ((2, 1), (0, -1)):
                src, dst = w_ref.at[self.half], w_out.at[slot, self.half]
                self.near.append(copies.start(src, dst, place.along_x(step)))

    def forward(self):
        for copy in self.near:
            copy.wait_recv()
        for w_out in self.outs:
            src = w_out.at[2 * self.place.k, self.half]
            dst = w_out.at[1, self.half]
            device = self.place.along_x(2 * self.place.k - 1)
            self.middle.append(self.copies.start(src, dst, device))
            for slot in (0, 2):
                self.give(w_out.at[slot, self.half])

    def give(self, part):
        self.gifts.append(self.copies.start(part, part, self.place.twin))

    def finish(self):
        for copy, w_out in zip(self.middle, self.outs):
            copy.wait_recv()
            self.give(w_out.at[1, self.half])

    def wait(self):
        for gift in self.gifts:
            gift.wait_recv()


def stream_cast_kernel(weights, source_ref, where_ref, kv_ref, *refs):
    w_refs, refs = refs[:weights], refs[weights:]
    out_ref, w_outs, refs = refs[0], refs[1 : 1 + weights], refs[1 + weights :]
    kept, land, twin_land, leave, *sems = refs
    ring_copies, gifts, w_copies = (Copies(*sems[2 * i : 2 * i + 2]) for i in range(3))
    place = Place()
    count = kv_ref.shape[0]
    length = land.shape[0] // 2
    stages = length // STAGE
    home = 2 * count

    greet(place.along_z(1), place.along_z(-1), place.along_x(1), place.along_x(-1), place.twin)
    own_gift = gifts.start(kv_ref, kept.at[pl.ds(count, count)], place.twin)

    @pl.loop(0, count)
    def _(j):
        kept[j] = kv_ref[j]

    own_gift.wait_recv()
    sends, given = {}, {}
    share = None
    for i in range(stages + 4):
        for d in range(2):
            if 0 <= i - 2 < stages:
                at = d * length + (i - 2) * STAGE
                sends[d, i - 2].wait_recv()
                part = pl.ds(at, STAGE)
                given[d, i - 2] = gifts.start(land.at[part], twin_land.at[part], place.twin)
                copy_slots(land, at, kept, home + at, STAGE)
            if i < stages:
                at = d * length + i * STAGE

                @pl.loop(at, at + STAGE)
                def _(q):
                    leave[q] = kept[source_ref[q]]

            if 0 <= i - 4 < stages:
                at = d * length + (i - 4) * STAGE
                given[d, i - 4].wait_recv()
                copy_slots(twin_land, at, kept, home + 2 * length + at, STAGE)
        if i < stages:
            for d in range(2):
                part = pl.ds(d * length + i * STAGE, STAGE)
                sends[d, i] = ring_copies.start(
                    leave.at[part], land.at[part], place.along_z(1 - 2 * d)
                )
        if i == 1:
            share = WeightShare(place, w_copies, w_refs, w_outs)
        if i == 2 * stages // 3:
            share.forward()
    share.finish()

    @pl.loop(0, out_ref.shape[0])
    def _(r):
        out_ref[r] = kept[where_ref[r]]

    share.wait()
    for group in (gifts, ring_copies, w_copies):
        group.wait_sends()


def stream_cast(ident, source, where, kv, weights):
    count, rows, cols = kv.shape
    stages = LENGTH // STAGE
    others = lax.axis_size("tp") - 1
    return pl.pallas_call(
        functools.partial(stream_cast_kernel, len(weights)),
        out_shape=[jax.ShapeDtypeStruct((where.shape[0], rows, cols), kv.dtype)]
        + [jax.ShapeDtypeStruct((others, *w.shape), w.dtype) for w in weights],
        in_specs=[SMEM_SPEC, SMEM_SPEC, VMEM_SPEC] + [ANY_SPEC] * len(weights),
        out_specs=[VMEM_SPEC] + [ANY_SPEC] * len(weights),
        scratch_shapes=[
            pltpu.VMEM((2 * count + 4 * LENGTH, rows, cols), kv.dtype),
            pltpu.VMEM((2 * LENGTH, rows, cols), kv.dtype),
            pltpu.VMEM((2 * LENGTH, rows, cols), kv.dtype),
            pltpu.VMEM((2 * LENGTH, rows, cols), kv.dtype),
        ]
        + copy_sems(2 * stages)
        + copy_sems(2 * stages + 1)
        + copy_sems(6 * len(weights)),
        compiler_params=pltpu.CompilerParams(
            collective_id=ident, has_side_effects=True, vmem_limit_bytes=VMEM_LIMIT
        ),
        name="stream_cast",
    )(source, where, kv, *weights)


def stream_fold_kernel(
    table_ref, onward_ref, final_ref, grads_ref, tokens_ref, out_ref, tokens_out, held, kept, land,
    leave, twin_land, load_sem, *sems
):
    ring_copies, gifts, exchange = (Copies(*sems[2 * i : 2 * i + 2]) for i in range(3))
    place = Place()
    count = out_ref.shape[0]
    length = land.shape[0] // 2
    stages = length // STAGE
    own = grads_ref.shape[0]
    readers = 2 * MOST
    zero = 2 * length
    peers = [place.along_x(rel) for rel in range(1, place.tp)]

    load = pltpu.make_async_copy(grads_ref, held.at[pl.ds(0, own)], load_sem)
    load.start()
    blank = jnp.zeros_like(held[0])
    held[2 * own] = blank
    kept[zero] = blank
    twin_land[2 * count] = blank
    greet(place.along_z(1), place.along_z(-1), place.twin, *peers)
    own_gift = gifts.start(grads_ref, held.at[pl.ds(own, own)], place.twin)
    block = tokens_out.shape[1]
    for rel, peer in enumerate(peers, 1):
        exchange.start(
            tokens_ref.at[pl.ds(peer[3] * block, block)],
            tokens_out.at[place.tp - 1 - rel],
            peer,
        )
    load.wait()
    own_gift.wait_recv()

    def readers_sum(slot):
        total = held[table_ref[slot * readers]].astype(F32)
        for q in range(1, readers):
            total += held[table_ref[slot * readers + q]].astype(F32)
        return total

    sends = {}

    def arrive(i):
        for d in range(2):
            at = d * length + i * STAGE
            sends[d, i].wait_recv()
            if i * STAGE < count:
                src = land.at[pl.ds(at, STAGE)]
                dst = twin_land.at[pl.ds(d * count + i * STAGE, STAGE)]
                gifts.start(src, dst, place.twin)
            copy_slots(land, at, kept, at, STAGE)

    for i in reversed(range(stages)):
        if i + 2 < stages:
            arrive(i + 2)
        for d in range(2):
            at = d * length + i * STAGE

            @pl.loop(at, at + STAGE)
            def _(q):
                total = readers_sum(count + q) + kept[onward_ref[q]].astype(F32)
                leave[q] = total.astype(leave.dtype)

        for d in range(2):
            part = pl.ds(d * length + i * STAGE, STAGE)
            sends[d, i] = ring_copies.start(
                leave.at[part], land.at[part], place.along_z(2 * d - 1)
            )
    arrive(1)
    arrive(0)
    for gift in gifts.all[1:]:
        gift.wait_recv()

    @pl.loop(0, count)
    def _(p):
        total = readers_sum(p)
        for d in range(2):
            total += kept[final_ref[d * count + p]].astype(F32)
            total += twin_land[final_ref[(2 + d) * count + p]].astype(F32)
        out_ref[p] = total.astype(out_ref.dtype)

    for copy in exchange.all:
        copy.wait_recv()
    for group in (gifts, ring_copies, exchange):
        group.wait_sends()


def stream_fold(ident, count, table, onward, final, grads, tokens):
    own, rows, cols = grads.shape
    stages = LENGTH // STAGE
    tp = lax.axis_size("tp")
    return pl.pallas_call(
        stream_fold_kernel,
        out_shape=[
            jax.ShapeDtypeStruct((count, rows, cols), grads.dtype),
            jax.ShapeDtypeStruct((tp - 1, tokens.shape[0] // tp, tokens.shape[1]), tokens.dtype),
        ],
        in_specs=[SMEM_SPEC, SMEM_SPEC, SMEM_SPEC, ANY_SPEC, ANY_SPEC],
        out_specs=[VMEM_SPEC, ANY_SPEC],
        scratch_shapes=[
            pltpu.VMEM((2 * own + 1, rows, cols), grads.dtype),
            pltpu.VMEM((2 * LENGTH + 1, rows, cols), grads.dtype),
            pltpu.VMEM((2 * LENGTH, rows, cols), grads.dtype),
            pltpu.VMEM((2 * LENGTH, rows, cols), grads.dtype),
            pltpu.VMEM((2 * count + 1, rows, cols), grads.dtype),
            pltpu.SemaphoreType.DMA,
        ]
        + copy_sems(2 * stages)
        + copy_sems(1 + 2 * (-(-count // STAGE)))
        + copy_sems(tp - 1),
        compiler_params=pltpu.CompilerParams(
            collective_id=ident, has_side_effects=True, vmem_limit_bytes=VMEM_LIMIT
        ),
        name="stream_fold",
    )(table, onward, final, grads, tokens)


def summed(pairs, start):
    total = start
    for holds, value in pairs:
        total = total + jnp.where(holds, value, 0)
    return total


def readers_table(slot, slots, requests):
    at_slot = slot[:, None] == jnp.arange(slots, dtype=jnp.int32)[None, :]
    turn = jnp.cumsum(at_slot.astype(jnp.int32), axis=0)
    number = jnp.arange(requests, dtype=jnp.int32)[:, None]
    columns = [
        jnp.min(jnp.where(at_slot & (turn == q + 1), number, requests), axis=0)
        for q in range(2 * MOST)
    ]
    return jnp.stack(columns, axis=1).reshape(-1).astype(jnp.int32)


def needs(ring, count, ids):
    devices = ids.shape[0]
    pair = 2 * count
    every = jnp.arange(devices * count, dtype=jnp.int32)
    owner = ids // count
    owner_z, owner_k = owner // 2, owner % 2
    reader_z = (jnp.arange(devices, dtype=jnp.int32) // 2)[:, None]
    away = jnp.mod(reader_z - owner_z, ring)
    up = (2 * away < ring) | ((2 * away == ring) & (owner_k == 0))
    steps = (jnp.where(up, away, 0), jnp.where(up, 0, ring - away))
    hot = ids.reshape(-1)[:, None] == every[None, :]
    place = jnp.arange(pair, dtype=jnp.int32)
    ranks, fars = [], []
    for d in range(2):
        far = jnp.max(jnp.where(hot, steps[d].reshape(-1)[:, None], 0), axis=0)
        far = far.reshape(ring, pair)
        before = (far[:, None, :] > far[:, :, None]) | (
            (far[:, None, :] == far[:, :, None]) & (place[None, None, :] < place[None, :, None])
        )
        ranks.append(jnp.sum(before.astype(jnp.int32), axis=2))
        fars.append(far)
    return owner_k, steps, fars, ranks


def own_chip(array):
    return lax.dynamic_slice_in_dim(array, lax.axis_index("st_0"), 1, axis=0)[0]


def chip_requests(array):
    return lax.dynamic_slice_in_dim(array, 2 * lax.axis_index("st_0"), 2, axis=0).reshape(-1)


def stream_routes(ring, count, ids):
    me_k = lax.axis_index("st_1")
    requests = ids.shape[1]
    pair = 2 * count
    reach = ring // 2
    owner_k, steps, fars, ranks = needs(ring, count, ids)
    core = jnp.arange(2, dtype=jnp.int32)
    spot = jnp.arange(LENGTH, dtype=jnp.int32)
    place = jnp.arange(pair, dtype=jnp.int32)
    at_home = place % count + jnp.where(place // count == me_k, 0, count)
    want = 2 * jnp.arange(count, dtype=jnp.int32) + me_k
    chip_ids = chip_requests(ids)
    every = jnp.arange(ids.shape[0] * count, dtype=jnp.int32)
    chip_hot = chip_ids[:, None] == every[None, :]
    chip_owner = chip_requests(owner_k)
    within = chip_ids % count
    where = within + jnp.where(chip_owner == me_k, 0, count)
    slot = jnp.where(chip_owner == me_k, within, -1)
    fits = jnp.bool_(True)
    source, onward, near, aside = [], [], [], []
    for d in range(2):
        turn = 1 - 2 * d
        sizes, starts = [], []
        for t in range(1, reach + 1):
            whole = jnp.sum((fars[d] >= t).astype(jnp.int32), axis=1)[:, None]
            sizes.append((whole + 1 - core[None, :]) // 2)
            if t == 1:
                starts.append(jnp.zeros_like(sizes[0]))
            else:
                behind = jnp.roll(starts[-1] + sizes[-2], -turn, axis=0)
                starts.append(jnp.maximum(behind, starts[-1] + LAG))
            fits &= jnp.all(starts[-1] + sizes[-1] <= LENGTH)
        out_size = [own_chip(jnp.roll(a, turn * t, axis=0)) for t, a in enumerate(sizes)]
        out_at = [own_chip(jnp.roll(a, turn * t, axis=0)) for t, a in enumerate(starts)]
        in_size = [own_chip(jnp.roll(a, turn * (t + 1), axis=0)) for t, a in enumerate(sizes)]
        in_at = [own_chip(jnp.roll(a, turn * (t + 1), axis=0)) for t, a in enumerate(starts)]
        mine = [
            [jnp.where(me_k == 0, a[0], a[1]) for a in array]
            for array in (out_size, out_at, in_size, in_at)
        ]
        size_o, at_o, size_i, at_i = mine
        rank, far = own_chip(ranks[d]), own_chip(fars[d])
        order = jnp.sum(jnp.where(rank[None, :] == want[:, None], at_home[None, :], 0), axis=1)
        order = jnp.concatenate([order, jnp.zeros((LENGTH - count,), order.dtype)])
        base = pair + d * LENGTH
        source.append(
            summed(
                [
                    ((spot >= at_o[t]) & (spot < at_o[t] + size_o[t]), base + at_i[t - 1] + spot - at_o[t])
                    for t in range(1, reach)
                ],
                jnp.where(spot < size_o[0], order, 0),
            )
        )
        onward.append(
            summed(
                [
                    (
                        (spot >= at_i[t]) & (spot < at_i[t] + jnp.minimum(size_i[t], size_o[t + 1])),
                        d * LENGTH + at_o[t + 1] + spot - at_i[t] - 2 * LENGTH,
                    )
                    for t in range(reach - 1)
                ],
                jnp.full((LENGTH,), 2 * LENGTH, jnp.int32),
            )
        )
        index = lax.dynamic_slice_in_dim(rank, me_k * count, count)
        used = lax.dynamic_slice_in_dim(far, me_k * count, count) > 0
        same = index % 2 == me_k
        near.append(jnp.where(used & same, d * LENGTH + index // 2, 2 * LENGTH))
        aside.append(jnp.where(used & ~same, d * count + index // 2, 2 * count))
        step = chip_requests(steps[d])
        ranked = jnp.sum(jnp.where(chip_hot, ranks[d].reshape(-1)[None, :], 0), axis=1)
        at = summed(
            [
                ((step == t + 1) & (ranked % 2 == c), in_at[t][c])
                for t in range(reach)
                for c in range(2)
            ],
            ranked // 2,
        )
        by_me = ranked % 2 == me_k
        where = jnp.where(step > 0, base + at + jnp.where(by_me, 0, 2 * LENGTH), where)
        slot = jnp.where(step > 0, jnp.where(by_me, count + d * LENGTH + at, -1), slot)
    where = lax.dynamic_slice_in_dim(where, me_k * requests, requests)
    slot = slot.reshape(2, requests)
    slot = jnp.where(me_k == 0, slot, slot[::-1]).reshape(-1)
    table = readers_table(slot, count + 2 * LENGTH, 2 * requests)
    tables = (jnp.concatenate(source), where, jnp.concatenate(onward), jnp.concatenate(near + aside))
    source, where, onward, final = (t.astype(jnp.int32) for t in tables)
    return fits, source, where, table, onward, final


def project(rows_list, weight_list, out_ref, n, tile):
    cols = pl.ds(n * tile, tile)
    total = None
    for rows, weight in zip(rows_list, weight_list):
        term = lax.dot_general(
            rows[...], weight[cols, :], (((1,), (1,)), ((), ())), preferred_element_type=F32
        )
        total = term if total is None else total + term
    out_ref[:, cols] = total.astype(out_ref.dtype)


def tail_kernel(sums_ref, all_ref, tokens_ref, tokens_in, *refs):
    weights, refs = refs[:8], refs[8:]
    d_tokens_ref, d_store_ref, d_wkey_ref = refs[:3]
    wbuf_t, wbuf_s, own_t, in_t, own_s, in_s, refs = *refs[3:9], refs[9:]
    keys, keys_turned, all_buf, terms, twin_terms, sent, come, last, last_in, refs = *refs[:9], refs[9:]
    load_sem, *sems = refs
    exchange, gifts, ring_copies = (Copies(*sems[2 * i : 2 * i + 2]) for i in range(3))
    place = Place()
    tp, ring = place.tp, place.ring
    reach = ring // 2
    peers = [place.along_x(rel) for rel in range(1, tp)]
    loads = []

    def load(src, dst):
        copy = pltpu.make_async_copy(src, dst, load_sem.at[len(loads)])
        copy.start()
        loads.append(copy)

    load(sums_ref, keys)
    for n in range(tp):
        load(all_ref.at[n], all_buf.at[n])
    greet(place.twin, place.along_z(1), place.along_z(-1), *peers)
    share = sums_ref.shape[0] // tp
    for rel, peer in enumerate(peers, 1):
        exchange.start(
            sums_ref.at[pl.ds(peer[3] * share, share)], in_s.at[tp - 1 - rel], peer
        )
    block = own_t.shape[0]
    load(tokens_ref.at[pl.ds(place.x * block, block)], own_t)
    load(tokens_in, in_t)
    load(sums_ref.at[pl.ds(place.x * share, share)], own_s)
    for wbuf, (wa, wb, wa_far, wb_far) in ((wbuf_t, weights[:4]), (wbuf_s, weights[4:])):
        load(wa, wbuf.at[0])
        load(wb, wbuf.at[1])
        load(wa_far, wbuf.at[pl.ds(2, tp - 1)])
        load(wb_far, wbuf.at[pl.ds(2 + tp - 1, tp - 1)])
    count, pass_len, pair = sums_ref.shape
    rows, cols = count * pass_len, pair // 2
    depth = all_ref.shape[3]
    width = terms.shape[3]
    loads[0].wait()
    keys_turned[...] = keys[:, :, :cols].reshape(rows, cols).T
    for n in range(tp):
        loads[1 + n].wait()
        term = jnp.dot(
            keys_turned[...], all_buf[n].reshape(rows, depth), preferred_element_type=F32
        )
        for c in range(depth // width):
            for h in range(2):
                terms[h, n * (depth // width) + c] = term[
                    h * (cols // 2) : (h + 1) * (cols // 2), c * width : (c + 1) * width
                ]
    gift = gifts.start(terms.at[1 - place.k], twin_terms, place.twin)
    for copy in loads[1 + tp :]:
        copy.wait()

    def operands(own, far_rows, wbuf):
        n_cols = own.shape[-1] // 2
        rows_list, weight_list = [], []
        for c in range(2):
            rows_list.append(own.at[:, pl.ds(c * n_cols, n_cols)])
            weight_list.append(wbuf.at[c])
        for rel in range(tp - 1):
            for c in range(2):
                rows_list.append(far_rows.at[rel, :, pl.ds(c * n_cols, n_cols)])
                weight_list.append(wbuf.at[2 + c * (tp - 1) + rel])
        return rows_list, weight_list

    part_rows = share * pass_len
    tile = 512
    tiles = d_tokens_ref.shape[1] // tile
    for_tokens = operands(own_t, in_t, wbuf_t)
    for_store = operands(
        own_s.reshape(part_rows, pair), in_s.reshape(tp - 1, part_rows, pair), wbuf_s
    )
    gift.wait_recv()
    hops = {}

    def mine(dest):
        return terms[place.k, dest] + twin_terms[dest]

    done = 0
    for s in range(1, reach + 1):
        for d in range(2):
            to_go = reach - d + 1 - s
            if to_go < 1:
                continue
            turn = 1 - 2 * d
            total = mine(lax.rem(place.z + turn * to_go + ring, ring))
            n = d * reach + s - 1
            if s > 1:
                hops[d, s - 1].wait_recv()
                total += come[n - 1].astype(F32)
            sent[n] = total.astype(sent.dtype)
            hops[d, s] = ring_copies.start(sent.at[n], come.at[n], place.along_z(turn))
        if s == reach // 2:
            for copy in exchange.all:
                copy.wait_recv()
        if s <= reach // 2:
            for _ in range(-(-tiles // (reach // 2))):
                if done < tiles:
                    project(*for_tokens, d_tokens_ref, done, tile)
                    done += 1
        elif s < reach:
            for _ in range(-(-tiles // (reach // 2 - 1))):
                if done < 2 * tiles:
                    project(*for_store, d_store_ref, done - tiles, tile)
                    done += 1
    total = mine(place.z)
    for d in range(2):
        hops[d, reach - d].wait_recv()
        total += come[d * reach + reach - d - 1].astype(F32)
    turned = total.T
    out_rows = turned.shape[0] // 2
    for c in range(2):
        last[c] = turned[c * out_rows : (c + 1) * out_rows]
    end = gifts.start(last.at[1 - place.k], last_in, place.twin)
    half = cols // 2
    d_wkey_ref[:, pl.ds(pl.multiple_of(place.k * half, half), half)] = last[place.k]
    end.wait_recv()
    d_wkey_ref[:, pl.ds(pl.multiple_of((1 - place.k) * half, half), half)] = last_in[...]
    for group in (exchange, gifts, ring_copies):
        group.wait_sends()


def tail(ident, sums, all_rows, tokens, tokens_in, weights):
    tp, ring = lax.axis_size("tp"), lax.axis_size("st_0")
    model, head_cols = weights[0].shape
    count, pass_len, pair = sums.shape
    share = count // tp
    width = model // ring
    low = sums.dtype
    return pl.pallas_call(
        tail_kernel,
        out_shape=[
            jax.ShapeDtypeStruct((tokens.shape[0] // tp, model), low),
            jax.ShapeDtypeStruct((share * pass_len, model), low),
            jax.ShapeDtypeStruct((width // 2, head_cols), F32),
        ],
        in_specs=[ANY_SPEC] * (4 + len(weights)),
        out_specs=[VMEM_SPEC] * 3,
        scratch_shapes=[
            pltpu.VMEM((2 * tp, model, head_cols), low),
            pltpu.VMEM((2 * tp, model, head_cols), low),
            pltpu.VMEM((tokens.shape[0] // tp, tokens.shape[1]), low),
            pltpu.VMEM(tokens_in.shape, low),
            pltpu.VMEM((share, pass_len, pair), low),
            pltpu.VMEM((tp - 1, share, pass_len, pair), low),
            pltpu.VMEM(sums.shape, low),
            pltpu.VMEM((head_cols, count * pass_len), low),
            pltpu.VMEM(all_rows.shape, low),
            pltpu.VMEM((2, ring, head_cols // 2, width), F32),
            pltpu.VMEM((ring, head_cols // 2, width), F32),
            pltpu.VMEM((ring, head_cols // 2, width), low),
            pltpu.VMEM((ring, head_cols // 2, width), low),
            pltpu.VMEM((2, width // 2, head_cols // 2), F32),
            pltpu.VMEM((width // 2, head_cols // 2), F32),
            pltpu.SemaphoreType.DMA((4 + tp + len(weights),)),
        ]
        + copy_sems(tp - 1)
        + copy_sems(2)
        + copy_sems(ring - 1),
        compiler_params=pltpu.CompilerParams(
            collective_id=ident, has_side_effects=True, vmem_limit_bytes=VMEM_LIMIT
        ),
        name="tail",
    )(sums, all_rows, tokens, tokens_in, *weights)


def first_slot(plan, d, step):
    total = jnp.zeros_like(step)
    for t, at in plan.base[d].items():
        total = total + jnp.where(step == t, at, 0)
    return total


def routes(plan, ids):
    count, slots = plan.passages, plan.slots
    me_k = lax.axis_index("st_1")
    requests = ids.shape[1]
    every = jnp.arange(ids.shape[0] * count, dtype=jnp.int32)
    owner_k, steps, fars, ranks = needs(plan.ring, count, ids)
    place = jnp.arange(2 * count, dtype=jnp.int32)
    at_home = place % count + jnp.where(place // count == me_k, 0, count)
    want = 2 * jnp.arange(count, dtype=jnp.int32) + me_k
    order, final = [], []
    for d in range(2):
        rank, far = own_chip(ranks[d]), own_chip(fars[d])
        order.append(jnp.sum(jnp.where(rank[None, :] == want[:, None], at_home[None, :], 0), axis=1))
        twin_at = plan.slots - count
        near = plan.base[d][1] - count
        aside = twin_at + d * (plan.layout[1] // 2)
        index = jnp.where(rank % 2 == me_k, near, aside) + rank // 2
        index = jnp.where(far > 0, index, twin_at + plan.layout[1])
        final.append(lax.dynamic_slice_in_dim(index, me_k * count, count))
    chip_ids = chip_requests(ids)
    chip_hot = chip_ids[:, None] == every[None, :]
    slot, core = chip_ids % count, chip_requests(owner_k)
    for d in range(2):
        rank = jnp.sum(jnp.where(chip_hot, ranks[d].reshape(-1)[None, :], 0), axis=1)
        step = chip_requests(steps[d])
        slot = jnp.where(step > 0, first_slot(plan, d, step) + rank // 2, slot)
        core = jnp.where(step > 0, rank % 2, core)
    where = slot + jnp.where(core == me_k, 0, slots)
    where = lax.dynamic_slice_in_dim(where, me_k * requests, requests)
    mine = jnp.where(core == me_k, slot, -1).reshape(2, requests)
    mine = jnp.where(me_k == 0, mine, mine[::-1]).reshape(-1)
    table = readers_table(mine, slots, 2 * requests)
    tables = (jnp.concatenate(order), where, jnp.concatenate(final))
    order, where, final = (t.astype(jnp.int32) for t in tables)
    return order, where, table, final


def local(pass_ids, store, queries, gate_pre, w_query, w_gate, w_key, w_value, d_mem):
    tp_count = lax.axis_size("tp")
    ring = lax.axis_size("st_0")
    passages, pass_len, _ = store.shape
    model_width = w_key.shape[0]
    requests = pass_ids.size
    plan = Plan(ring, passages)
    ids = jnp.zeros((8, 128), jnp.int32).at[0, :requests].set(pass_ids.reshape(-1))
    ids, all_rows, kv = front(5, ids, store, w_key, w_value)
    ids = ids[:, :, 0, :requests].reshape(2 * ring, requests)
    fits, source, where, table, onward, final = stream_routes(ring, passages, ids)

    def cast_short(ids, source, where, kv, weights):
        return stream_cast(0, source, where, kv, weights)

    def cast_any(ids, source, where, kv, weights):
        order, where, _, _ = routes(plan, ids)
        return cast_rows(plan, 1, order, where, kv, weights)

    def fold_short(ids, table, onward, final, grads, tokens):
        return stream_fold(2, passages, table, onward, final, grads, tokens)

    def fold_any(ids, table, onward, final, grads, tokens):
        _, _, table, final = routes(plan, ids)
        return fold_rows(plan, 3, table, final, grads, tokens)

    weights = (w_query, w_gate, w_key, w_value)
    request_kv, wq_far, wg_far, wk_far, wv_far = lax.cond(
        fits, cast_short, cast_any, ids, source, where, kv, weights
    )
    request_grads, token_grads = attend(queries, gate_pre, d_mem, request_kv)
    sums, tokens_in = lax.cond(
        fits, fold_short, fold_any, ids, table, onward, final, request_grads, token_grads
    )
    d_tokens, d_store, d_wkey = tail(
        4,
        sums,
        all_rows,
        token_grads,
        tokens_in,
        (w_query, w_gate, wq_far, wg_far, w_key, w_value, wk_far, wv_far),
    )
    return d_tokens, d_store.reshape(passages // tp_count, pass_len, model_width), d_wkey


def solution(mesh):
    finer = Mesh(
        mesh.devices.reshape(mesh.shape["grp"], -1, 2, mesh.shape["tp"]),
        ("grp", "st_0", "st_1", "tp"),
    )
    in_specs = (
        P(GRP_ST, None),
        P(ST, None, "tp"),
        P(GRP_ST, "tp"),
        P(GRP_ST, "tp"),
        P(None, "tp"),
        P(None, "tp"),
        P(None, "tp"),
        P(None, "tp"),
        P(GRP_ST, "tp"),
    )
    out_specs = (P(GRP_ST_TP, None), P(GRP_ST_TP, None, None), P(GRP_ST, "tp"))
    return jax.shard_map(local, mesh=finer, in_specs=in_specs, out_specs=out_specs, check_vma=False)
```

```python
import functools

import jax
import jax.numpy as jnp
from jax import lax
from jax.experimental import pallas as pl
from jax.experimental.pallas import tpu as pltpu
from jax.sharding import Mesh
from jax.sharding import PartitionSpec as P

HD = 256
BLK = 128
PB = 4
MOST = 2
CHUNK = 4
LENGTH = 54
STAGE = 2
LAG = 2 * STAGE
VMEM_LIMIT = 62 * 1024 * 1024
ST = ("st_0", "st_1")
GRP_ST = ("grp", "st_0", "st_1")
GRP_ST_TP = ("grp", "st_0", "st_1", "tp")
MESH_ID = pl.DeviceIdType.MESH
VMEM_SPEC = pl.BlockSpec(memory_space=pltpu.VMEM)
SMEM_SPEC = pl.BlockSpec(memory_space=pltpu.SMEM)
ANY_SPEC = pl.BlockSpec(memory_space=pl.ANY)
F32 = jnp.float32


class Plan:
    def __init__(self, ring, passages):
        self.ring = ring
        self.passages = passages
        self.reach = ring // 2
        self.steps_of = range(1, self.reach + 1)
        per_owner = 2 * MOST
        self.layout = {
            t: min(passages, per_owner * (self.reach - t + 1))
            + min(passages, per_owner * (self.reach - t))
            for t in self.steps_of
        }
        self.sizes = self.layout
        self.base = [{}, {}]
        at = passages
        for d in range(2):
            for t in self.steps_of:
                self.base[d][t] = at
                at += -(-self.layout[t] // 2)
        self.slots = at

    def half(self, t):
        return -(-self.sizes[t] // 2) if t <= self.reach else 0

    def steps(self, down=False):
        for t in reversed(self.steps_of) if down else self.steps_of:
            for first in range(0, self.half(t), CHUNK):
                for d in range(2):
                    yield d, t, first, min(CHUNK, self.half(t) - first)


class Place:
    def __init__(self):
        self.g, self.z, self.k, self.x = (lax.axis_index(a) for a in GRP_ST_TP)
        self.ring = lax.axis_size("st_0")
        self.tp = lax.axis_size("tp")
        self.twin = (self.g, self.z, 1 - self.k, self.x)

    def along_z(self, step):
        return (self.g, lax.rem(self.z + step + self.ring, self.ring), self.k, self.x)

    def along_x(self, step):
        return (self.g, self.z, self.k, lax.rem(self.x + step + self.tp, self.tp))


def greet(*devices):
    barrier = pltpu.get_barrier_semaphore()
    for device in devices:
        pl.semaphore_signal(barrier, inc=1, device_id=device, device_id_type=MESH_ID)
    pl.semaphore_wait(barrier, len(devices))


class Copies:
    def __init__(self, send_sem, recv_sem):
        self.send_sem, self.recv_sem = send_sem, recv_sem
        self.all = []

    def start(self, src, dst, device):
        n = len(self.all)
        copy = pltpu.make_async_remote_copy(
            src_ref=src,
            dst_ref=dst,
            send_sem=self.send_sem.at[n],
            recv_sem=self.recv_sem.at[n],
            device_id=device,
            device_id_type=MESH_ID,
        )
        copy.start()
        self.all.append(copy)
        return copy

    def wait_sends(self):
        for copy in self.all:
            copy.wait_send()


def copy_sems(count):
    return [pltpu.SemaphoreType.DMA((count,)), pltpu.SemaphoreType.DMA((count,))]


def front_kernel(ids_ref, store_ref, wk_ref, wv_ref, ids_out, all_out, kv_out, total, *sems):
    gifts, ring_copies, x_copies = (Copies(*sems[2 * i : 2 * i + 2]) for i in range(3))
    place = Place()
    count = store_ref.shape[0]
    half = count // 2
    reach = place.ring // 2
    greet(place.along_z(1), place.along_z(-1), place.along_x(1), place.along_x(-1), place.twin)
    halves = (pl.ds(0, half), pl.ds(half, half))
    near = {}
    for d, step in ((0, 1), (1, -1)):
        for h in (d, 1 - d):
            near[d, h] = x_copies.start(
                store_ref.at[halves[h]], all_out.at[place.x, halves[h]], place.along_x(step)
            )
    gift = gifts.start(ids_ref, ids_out.at[place.z, place.k], place.twin)
    ids_out[place.z, place.k] = ids_ref[...]
    all_out[place.x] = store_ref[...]
    gift.wait_recv()
    hops = {}

    def hop(d, t):
        source = lax.rem(place.z + (t - 1) * (2 * d - 1) + place.ring, place.ring)
        part = ids_out.at[source]
        hops[d, t] = ring_copies.start(part, part, place.along_z(1 - 2 * d))

    def hops_until(first, last):
        for t in range(first, last):
            for d in range(2):
                if t > 1 and t <= reach - d:
                    hops[d, t - 1].wait_recv()
                if t <= reach - d:
                    hop(d, t)

    def add(source, start):
        rows = total.shape[0]
        depth = store_ref.shape[2]
        cols = wk_ref.shape[1]
        part = all_out[source].reshape(rows, depth)
        w_rows = pl.ds(pl.multiple_of(source * depth, depth), depth)
        for c, w_ref in enumerate((wk_ref, wv_ref)):
            at = slice(c * cols, (c + 1) * cols)
            term = jnp.dot(part, w_ref[w_rows, :], preferred_element_type=F32)
            total[:, at] = term if start else total[:, at] + term

    hops_until(1, 4)
    add(place.x, True)
    hops_until(4, 6)
    far = []
    for d, step in ((0, 1), (1, -1)):
        near[d, d].wait_recv()
        source = lax.rem(place.x - step + place.tp, place.tp)
        part = all_out.at[source, halves[d]]
        far.append(x_copies.start(part, part, place.along_x(step)))
    hops_until(6, reach + 1)
    for d, step in ((0, 1), (1, -1)):
        near[d, 1 - d].wait_recv()
        add(lax.rem(place.x - step + place.tp, place.tp), False)
    for d in range(2):
        hops[d, reach - d].wait_recv()
    for copy in far:
        copy.wait_recv()
    add(lax.rem(place.x + 2, place.tp), False)
    kv_out[...] = total[...].reshape(kv_out.shape).astype(kv_out.dtype)
    for group in (gifts, ring_copies, x_copies):
        group.wait_sends()


def front(ident, ids, store, w_key, w_value):
    count, rows, cols = store.shape
    ring, tp = lax.axis_size("st_0"), lax.axis_size("tp")
    pair = 2 * w_key.shape[1]
    return pl.pallas_call(
        front_kernel,
        out_shape=[
            jax.ShapeDtypeStruct((ring, 2, *ids.shape), ids.dtype),
            jax.ShapeDtypeStruct((tp, *store.shape), store.dtype),
            jax.ShapeDtypeStruct((count, rows, pair), store.dtype),
        ],
        in_specs=[VMEM_SPEC] * 4,
        out_specs=[VMEM_SPEC] * 3,
        scratch_shapes=[pltpu.VMEM((count * rows, pair), F32)]
        + copy_sems(1)
        + copy_sems(ring - 1)
        + copy_sems(6),
        compiler_params=pltpu.CompilerParams(
            collective_id=ident, has_side_effects=True, vmem_limit_bytes=VMEM_LIMIT
        ),
        name="front",
    )(ids, store, w_key, w_value)


def attend_kernel(scale, q_ref, gate_ref, mem_ref, kv_ref, grads_ref, tokens_ref):
    blocks = q_ref.shape[0] // BLK
    cols = q_ref.shape[1]
    pass_len = kv_ref.shape[1]
    low = q_ref.dtype

    def dot(a, b, ca, cb):
        return lax.dot_general(a, b, (((ca,), (cb,)), ((), ())), preferred_element_type=F32)

    for b in range(blocks):
        toks = pl.ds(b * BLK, BLK)
        kv = kv_ref[pl.ds(b * PB, PB)].reshape(PB * pass_len, 2 * cols)
        for h in range(cols // HD):
            k_at = slice(h * HD, (h + 1) * HD)
            v_at = slice(cols + h * HD, cols + (h + 1) * HD)
            q, keys, values = q_ref[toks, k_at], kv[:, k_at], kv[:, v_at]
            scores = dot(q, keys, 1, 1) * scale
            shifted = jnp.exp(scores - jnp.max(scores, axis=-1, keepdims=True))
            probs = shifted / jnp.sum(shifted, axis=-1, keepdims=True)
            probs_low = probs.astype(low)
            attended = dot(probs_low, values, 1, 0)
            gate = gate_ref[toks, k_at].astype(F32)
            mem = mem_ref[toks, k_at].astype(F32)
            sig = jax.nn.sigmoid(gate)
            attended_grad = (gate * sig * mem).astype(low)
            gate_grad = mem * attended * sig * (1.0 + gate * (1.0 - sig))
            prob_grad = dot(attended_grad, values, 1, 1)
            inner = jnp.sum(probs * prob_grad, axis=-1, keepdims=True)
            score_grad = (scale * probs * (prob_grad - inner)).astype(low)
            tokens_ref[toks, k_at] = dot(score_grad, keys, 1, 0).astype(low)
            tokens_ref[toks, v_at] = gate_grad.astype(low)
            key_grad = dot(score_grad, q, 0, 0).astype(low)
            value_grad = dot(probs_low, attended_grad, 0, 0).astype(low)
            passes = pl.ds(b * PB, PB)
            grads_ref[passes, :, k_at] = key_grad.reshape(PB, pass_len, HD)
            grads_ref[passes, :, v_at] = value_grad.reshape(PB, pass_len, HD)


def attend(queries, gate_pre, d_mem, request_kv):
    toks, cols = queries.shape
    _, pass_len, pair = request_kv.shape
    step = 2
    grid = toks // BLK // step
    tok_spec = pl.BlockSpec((step * BLK, cols), lambda i: (i, 0))
    kv_spec = pl.BlockSpec((step * PB, pass_len, pair), lambda i: (i, 0, 0))
    return pl.pallas_call(
        functools.partial(attend_kernel, HD**-0.5),
        grid=(grid,),
        out_shape=[
            jax.ShapeDtypeStruct(request_kv.shape, request_kv.dtype),
            jax.ShapeDtypeStruct((toks, pair), queries.dtype),
        ],
        in_specs=[tok_spec, tok_spec, tok_spec, kv_spec],
        out_specs=[kv_spec, pl.BlockSpec((step * BLK, pair), lambda i: (i, 0))],
        name="attend",
    )(queries, gate_pre, d_mem, request_kv)


def cast_kernel(plan, weights, order_ref, where_ref, kv_ref, *refs):
    w_refs, refs = refs[:weights], refs[weights:]
    out_ref, w_outs, refs = refs[0], refs[1 : 1 + weights], refs[1 + weights :]
    buf, first_buf, home, *sems = refs
    ring_copies, gifts, w_copies = (Copies(*sems[2 * i : 2 * i + 2]) for i in range(3))
    place = Place()
    count, slots = plan.passages, plan.slots
    top = plan.half(1)

    greet(place.along_z(1), place.along_z(-1), place.along_x(1), place.along_x(-1), place.twin)
    own_gift = gifts.start(kv_ref, home.at[pl.ds(count, count)], place.twin)

    @pl.loop(0, count)
    def _(j):
        home[j] = kv_ref[j]
        buf[j] = kv_ref[j]

    own_gift.wait_recv()

    @pl.loop(0, top)
    def _(j):
        for d in range(2):
            first_buf[d * top + j] = home[order_ref[d * count + j]]

    copies = {}
    steps = list(plan.steps())
    extent = {(d, t, first): size for d, t, first, size in steps}

    def send(d, t, first):
        size = extent[d, t, first]
        if t == 1:
            src = first_buf.at[pl.ds(d * top + first, size)]
        else:
            src = buf.at[pl.ds(plan.base[d][t - 1] + first, size)]
        dst = buf.at[pl.ds(plan.base[d][t] + first, size)]
        copies[d, t, first] = ring_copies.start(src, dst, place.along_z(1 - 2 * d))

    for d, t, first, _ in steps:
        if t == 1:
            send(d, t, first)
    rows = w_refs[0].shape[0] // 2
    half = pl.ds(place.k * rows, rows)
    arrive = [[], []]
    for w_ref, w_out in zip(w_refs, w_outs):
        arrive[0].append(
            w_copies.start(w_ref.at[half], w_out.at[2, half], place.along_x(1))
        )
        arrive[1].append(
            w_copies.start(w_ref.at[half], w_out.at[0, half], place.along_x(-1))
        )
    w_gifts = []
    middle = []

    def forward_weights():
        for copy in arrive[0] + arrive[1]:
            copy.wait_recv()
        for w_out in w_outs:
            middle.append(
                w_copies.start(
                    w_out.at[2 * place.k, half],
                    w_out.at[1, half],
                    place.along_x(2 * place.k - 1),
                )
            )
            for rel in (0, 2):
                part = w_out.at[rel, half]
                w_gifts.append(w_copies.start(part, part, place.twin))

    last = None
    for d, t, first, size in steps:
        if t != last and t == plan.reach // 2 + 1:
            forward_weights()
        last = t
        copies[d, t, first].wait_recv()
        if (d, t + 1, first) in extent:
            send(d, t + 1, first)
        at = plan.base[d][t] + first
        gifts.start(buf.at[pl.ds(at, size)], buf.at[pl.ds(slots + at, size)], place.twin)
    for copy, w_out in zip(middle, w_outs):
        copy.wait_recv()
        part = w_out.at[1, half]
        w_gifts.append(w_copies.start(part, part, place.twin))
    for gift in gifts.all[1:]:
        gift.wait_recv()

    @pl.loop(0, count)
    def _(j):
        buf[slots + j] = home[count + j]

    @pl.loop(0, out_ref.shape[0])
    def _(r):
        out_ref[r] = buf[where_ref[r]]

    for gift in w_gifts:
        gift.wait_recv()
    for group in (gifts, ring_copies, w_copies):
        group.wait_sends()


def cast_rows(plan, ident, order, where, kv, weights):
    count, rows, cols = kv.shape
    steps = len(list(plan.steps()))
    others = lax.axis_size("tp") - 1
    return pl.pallas_call(
        functools.partial(cast_kernel, plan, len(weights)),
        out_shape=[jax.ShapeDtypeStruct((where.shape[0], rows, cols), kv.dtype)]
        + [jax.ShapeDtypeStruct((others, *w.shape), w.dtype) for w in weights],
        in_specs=[SMEM_SPEC, SMEM_SPEC, VMEM_SPEC] + [ANY_SPEC] * len(weights),
        out_specs=[VMEM_SPEC] + [ANY_SPEC] * len(weights),
        scratch_shapes=[
            pltpu.VMEM((2 * plan.slots, rows, cols), kv.dtype),
            pltpu.VMEM((2 * plan.half(1), rows, cols), kv.dtype),
            pltpu.VMEM((2 * count, rows, cols), kv.dtype),
        ]
        + copy_sems(steps)
        + copy_sems(steps + 1)
        + copy_sems(6 * len(weights)),
        compiler_params=pltpu.CompilerParams(
            collective_id=ident, has_side_effects=True, vmem_limit_bytes=VMEM_LIMIT
        ),
        name="cast_rows",
    )(order, where, kv, *weights)


def fold_kernel(
    plan,
    table_ref,
    final_ref,
    grads_ref,
    tokens_ref,
    out_ref,
    tokens_out,
    held,
    here,
    sums,
    load_sem,
    *sems,
):
    ring_copies, gifts, exchange = (Copies(*sems[2 * i : 2 * i + 2]) for i in range(3))
    place = Place()
    count, top = plan.passages, plan.half(1)
    own = grads_ref.shape[0]
    readers = 2 * MOST
    twin_at = plan.slots - count
    zero_at = twin_at + plan.layout[1]
    peers = [place.along_x(rel) for rel in range(1, place.tp)]

    load = pltpu.make_async_copy(grads_ref, held.at[pl.ds(0, own)], load_sem)
    load.start()
    held[2 * own] = jnp.zeros_like(held[2 * own])
    here[zero_at] = jnp.zeros_like(here[zero_at])
    greet(place.along_z(1), place.along_z(-1), place.twin, *peers)
    own_gift = gifts.start(grads_ref, held.at[pl.ds(own, own)], place.twin)
    block = tokens_out.shape[1]
    for rel, peer in enumerate(peers, 1):
        exchange.start(
            tokens_ref.at[pl.ds(peer[3] * block, block)],
            tokens_out.at[place.tp - 1 - rel],
            peer,
        )
    load.wait()
    own_gift.wait_recv()

    def readers_sum(slot):
        total = held[table_ref[slot * readers]].astype(F32)
        for q in range(1, readers):
            total += held[table_ref[slot * readers + q]].astype(F32)
        return total

    copies = {}
    steps = list(plan.steps(down=True))
    extent = {(d, t, first): size for d, t, first, size in steps}
    for d, t, first, size in steps:
        at = plan.base[d][t] + first
        begin = extent.get((d, t + 1, first), 0)
        if begin:
            copies[d, t + 1, first].wait_recv()
            far_at = plan.base[d][t + 1] + first

            @pl.loop(0, begin)
            def _(j):
                total = readers_sum(at + j) + here[far_at - count + j].astype(F32)
                sums[at - count + j] = total.astype(sums.dtype)

        if begin < size:

            @pl.loop(begin, size)
            def _(j):
                sums[at - count + j] = readers_sum(at + j).astype(sums.dtype)

        part = pl.ds(at - count, size)
        copies[d, t, first] = ring_copies.start(
            sums.at[part], here.at[part], place.along_z(2 * d - 1)
        )
    for d, t, first, size in steps:
        if t == 1:
            copies[d, t, first].wait_recv()
            src = here.at[pl.ds(plan.base[d][1] - count + first, size)]
            dst = here.at[pl.ds(twin_at + d * (plan.layout[1] // 2) + first, size)]
            gifts.start(src, dst, place.twin)
    for gift in gifts.all[1:]:
        gift.wait_recv()

    @pl.loop(0, count)
    def _(p):
        total = readers_sum(p)
        for d in range(2):
            total += here[final_ref[d * count + p]].astype(F32)
        out_ref[p] = total.astype(out_ref.dtype)

    for copy in exchange.all:
        copy.wait_recv()
    for group in (gifts, ring_copies, exchange):
        group.wait_sends()


def fold_rows(plan, ident, table, final, grads, tokens):
    own, rows, cols = grads.shape
    steps = list(plan.steps())
    ends = sum(1 for _, t, _, _ in steps if t == 1)
    count = plan.passages
    tp = lax.axis_size("tp")
    return pl.pallas_call(
        functools.partial(fold_kernel, plan),
        out_shape=[
            jax.ShapeDtypeStruct((count, rows, cols), grads.dtype),
            jax.ShapeDtypeStruct((tp - 1, tokens.shape[0] // tp, tokens.shape[1]), tokens.dtype),
        ],
        in_specs=[SMEM_SPEC, SMEM_SPEC, ANY_SPEC, ANY_SPEC],
        out_specs=[VMEM_SPEC, ANY_SPEC],
        scratch_shapes=[
            pltpu.VMEM((2 * own + 1, rows, cols), grads.dtype),
            pltpu.VMEM((plan.slots - count + plan.layout[1] + 1, rows, cols), grads.dtype),
            pltpu.VMEM((plan.slots - count, rows, cols), grads.dtype),
            pltpu.SemaphoreType.DMA,
        ]
        + copy_sems(len(steps))
        + copy_sems(1 + ends)
        + copy_sems(tp - 1),
        compiler_params=pltpu.CompilerParams(
            collective_id=ident, has_side_effects=True, vmem_limit_bytes=VMEM_LIMIT
        ),
        name="fold_rows",
    )(table, final, grads, tokens)


def copy_slots(src, src_at, dst, dst_at, size):
    @pl.loop(0, size)
    def _(j):
        dst[dst_at + j] = src[src_at + j]


class WeightShare:
    def __init__(self, place, copies, w_refs, w_outs):
        self.place, self.copies, self.outs = place, copies, w_outs
        rows = w_refs[0].shape[0] // 2
        self.half = pl.ds(place.k * rows, rows)
        self.near, self.middle, self.gifts = [], [], []
        for w_ref, w_out in zip(w_refs, w_outs):
            for slot, step in ((2, 1), (0, -1)):
                src, dst = w_ref.at[self.half], w_out.at[slot, self.half]
                self.near.append(copies.start(src, dst, place.along_x(step)))

    def forward(self):
        for copy in self.near:
            copy.wait_recv()
        for w_out in self.outs:
            src = w_out.at[2 * self.place.k, self.half]
            dst = w_out.at[1, self.half]
            device = self.place.along_x(2 * self.place.k - 1)
            self.middle.append(self.copies.start(src, dst, device))
            for slot in (0, 2):
                self.give(w_out.at[slot, self.half])

    def give(self, part):
        self.gifts.append(self.copies.start(part, part, self.place.twin))

    def finish(self):
        for copy, w_out in zip(self.middle, self.outs):
            copy.wait_recv()
            self.give(w_out.at[1, self.half])

    def wait(self):
        for gift in self.gifts:
            gift.wait_recv()


def stream_cast_kernel(weights, table_ref, kv_ref, *refs):
    w_refs, refs = refs[:weights], refs[weights:]
    out_ref, w_outs, refs = refs[0], refs[1 : 1 + weights], refs[1 + weights :]
    kept, land, twin_land, leave, *sems = refs
    ring_copies, gifts, w_copies = (Copies(*sems[2 * i : 2 * i + 2]) for i in range(3))
    place = Place()
    count = kv_ref.shape[0]
    length = land.shape[0] // 2
    stages = length // STAGE
    home = 2 * count

    greet(place.along_z(1), place.along_z(-1), place.along_x(1), place.along_x(-1), place.twin)
    own_gift = gifts.start(kv_ref, kept.at[pl.ds(count, count)], place.twin)

    @pl.loop(0, count)
    def _(j):
        kept[j] = kv_ref[j]

    own_gift.wait_recv()
    sends, given = {}, {}
    share = None
    for i in range(stages + 4):
        for d in range(2):
            if 0 <= i - 2 < stages:
                at = d * length + (i - 2) * STAGE
                sends[d, i - 2].wait_recv()
                part = pl.ds(at, STAGE)
                given[d, i - 2] = gifts.start(land.at[part], twin_land.at[part], place.twin)
                copy_slots(land, at, kept, home + at, STAGE)
            if i < stages:
                at = d * length + i * STAGE

                @pl.loop(at, at + STAGE)
                def _(q):
                    leave[q] = kept[table_ref[q]]

            if 0 <= i - 4 < stages:
                at = d * length + (i - 4) * STAGE
                given[d, i - 4].wait_recv()
                copy_slots(twin_land, at, kept, home + 2 * length + at, STAGE)
        if i < stages:
            for d in range(2):
                part = pl.ds(d * length + i * STAGE, STAGE)
                sends[d, i] = ring_copies.start(
                    leave.at[part], land.at[part], place.along_z(1 - 2 * d)
                )
        if i == 1:
            share = WeightShare(place, w_copies, w_refs, w_outs)
        if i == 2 * stages // 3:
            share.forward()
    share.finish()

    @pl.loop(0, out_ref.shape[0])
    def _(r):
        out_ref[r] = kept[table_ref[2 * length + r]]

    share.wait()
    for group in (gifts, ring_copies, w_copies):
        group.wait_sends()


def stream_cast(ident, table, kv, weights):
    count, rows, cols = kv.shape
    stages = LENGTH // STAGE
    others = lax.axis_size("tp") - 1
    return pl.pallas_call(
        functools.partial(stream_cast_kernel, len(weights)),
        out_shape=[jax.ShapeDtypeStruct((table.shape[0] - 2 * LENGTH, rows, cols), kv.dtype)]
        + [jax.ShapeDtypeStruct((others, *w.shape), w.dtype) for w in weights],
        in_specs=[SMEM_SPEC, VMEM_SPEC] + [ANY_SPEC] * len(weights),
        out_specs=[VMEM_SPEC] + [ANY_SPEC] * len(weights),
        scratch_shapes=[
            pltpu.VMEM((2 * count + 4 * LENGTH, rows, cols), kv.dtype),
            pltpu.VMEM((2 * LENGTH, rows, cols), kv.dtype),
            pltpu.VMEM((2 * LENGTH, rows, cols), kv.dtype),
            pltpu.VMEM((2 * LENGTH, rows, cols), kv.dtype),
        ]
        + copy_sems(2 * stages)
        + copy_sems(2 * stages + 1)
        + copy_sems(6 * len(weights)),
        compiler_params=pltpu.CompilerParams(
            collective_id=ident, has_side_effects=True, vmem_limit_bytes=VMEM_LIMIT
        ),
        name="stream_cast",
    )(table, kv, *weights)


def stream_fold_kernel(
    table_ref, grads_ref, tokens_ref, out_ref, tokens_out, held, kept, land,
    leave, twin_land, load_sem, *sems
):
    ring_copies, gifts, exchange = (Copies(*sems[2 * i : 2 * i + 2]) for i in range(3))
    place = Place()
    count = out_ref.shape[0]
    length = land.shape[0] // 2
    stages = length // STAGE
    own = grads_ref.shape[0]
    readers = 2 * MOST
    zero = 2 * length
    onward_at = (count + 2 * length + 1) * readers
    final_at = onward_at + 2 * length
    peers = [place.along_x(rel) for rel in range(1, place.tp)]

    load = pltpu.make_async_copy(grads_ref, held.at[pl.ds(0, own)], load_sem)
    load.start()
    blank = jnp.zeros_like(held[0])
    held[2 * own] = blank
    kept[zero] = blank
    twin_land[2 * count] = blank
    greet(place.along_z(1), place.along_z(-1), place.twin, *peers)
    own_gift = gifts.start(grads_ref, held.at[pl.ds(own, own)], place.twin)
    block = tokens_out.shape[1]
    for rel, peer in enumerate(peers, 1):
        exchange.start(
            tokens_ref.at[pl.ds(peer[3] * block, block)],
            tokens_out.at[place.tp - 1 - rel],
            peer,
        )
    load.wait()
    own_gift.wait_recv()

    def readers_sum(slot):
        total = held[table_ref[slot * readers]].astype(F32)
        for q in range(1, readers):
            total += held[table_ref[slot * readers + q]].astype(F32)
        return total

    sends = {}

    def arrive(i):
        for d in range(2):
            at = d * length + i * STAGE
            sends[d, i].wait_recv()
            if i * STAGE < count:
                src = land.at[pl.ds(at, STAGE)]
                dst = twin_land.at[pl.ds(d * count + i * STAGE, STAGE)]
                gifts.start(src, dst, place.twin)
            copy_slots(land, at, kept, at, STAGE)

    for i in reversed(range(stages)):
        if i + 2 < stages:
            arrive(i + 2)
        for d in range(2):
            at = d * length + i * STAGE

            @pl.loop(at, at + STAGE)
            def _(q):
                total = readers_sum(count + q) + kept[table_ref[onward_at + q]].astype(F32)
                leave[q] = total.astype(leave.dtype)

        for d in range(2):
            part = pl.ds(d * length + i * STAGE, STAGE)
            sends[d, i] = ring_copies.start(
                leave.at[part], land.at[part], place.along_z(2 * d - 1)
            )
    arrive(1)
    arrive(0)
    for gift in gifts.all[1:]:
        gift.wait_recv()

    @pl.loop(0, count)
    def _(p):
        total = readers_sum(p)
        for d in range(2):
            total += kept[table_ref[final_at + d * count + p]].astype(F32)
            total += twin_land[table_ref[final_at + (2 + d) * count + p]].astype(F32)
        out_ref[p] = total.astype(out_ref.dtype)

    for copy in exchange.all:
        copy.wait_recv()
    for group in (gifts, ring_copies, exchange):
        group.wait_sends()


def stream_fold(ident, count, table, grads, tokens):
    own, rows, cols = grads.shape
    stages = LENGTH // STAGE
    tp = lax.axis_size("tp")
    return pl.pallas_call(
        stream_fold_kernel,
        out_shape=[
            jax.ShapeDtypeStruct((count, rows, cols), grads.dtype),
            jax.ShapeDtypeStruct((tp - 1, tokens.shape[0] // tp, tokens.shape[1]), tokens.dtype),
        ],
        in_specs=[SMEM_SPEC, ANY_SPEC, ANY_SPEC],
        out_specs=[VMEM_SPEC, ANY_SPEC],
        scratch_shapes=[
            pltpu.VMEM((2 * own + 1, rows, cols), grads.dtype),
            pltpu.VMEM((2 * LENGTH + 1, rows, cols), grads.dtype),
            pltpu.VMEM((2 * LENGTH, rows, cols), grads.dtype),
            pltpu.VMEM((2 * LENGTH, rows, cols), grads.dtype),
            pltpu.VMEM((2 * count + 1, rows, cols), grads.dtype),
            pltpu.SemaphoreType.DMA,
        ]
        + copy_sems(2 * stages)
        + copy_sems(1 + 2 * (-(-count // STAGE)))
        + copy_sems(tp - 1),
        compiler_params=pltpu.CompilerParams(
            collective_id=ident, has_side_effects=True, vmem_limit_bytes=VMEM_LIMIT
        ),
        name="stream_fold",
    )(table, grads, tokens)


def readers_table(slot, slots, requests):
    at_slot = slot[:, None] == jnp.arange(slots, dtype=jnp.int32)[None, :]
    turn = jnp.cumsum(at_slot.astype(jnp.int32), axis=0)
    number = jnp.arange(requests, dtype=jnp.int32)[:, None]
    columns = [
        jnp.min(jnp.where(at_slot & (turn == q + 1), number, requests), axis=0)
        for q in range(2 * MOST)
    ]
    return jnp.stack(columns, axis=1).reshape(-1).astype(jnp.int32)


def needs(ring, count, ids):
    devices = ids.shape[0]
    pair = 2 * count
    every = jnp.arange(devices * count, dtype=jnp.int32)
    owner = ids // count
    owner_z, owner_k = owner // 2, owner % 2
    reader_z = (jnp.arange(devices, dtype=jnp.int32) // 2)[:, None]
    away = jnp.mod(reader_z - owner_z, ring)
    up = (2 * away < ring) | ((2 * away == ring) & (owner_k == 0))
    steps = (jnp.where(up, away, 0), jnp.where(up, 0, ring - away))
    hot = ids.reshape(-1)[:, None] == every[None, :]
    place = jnp.arange(pair, dtype=jnp.int32)
    ranks, fars = [], []
    for d in range(2):
        far = jnp.max(jnp.where(hot, steps[d].reshape(-1)[:, None], 0), axis=0)
        far = far.reshape(ring, pair)
        before = (far[:, None, :] > far[:, :, None]) | (
            (far[:, None, :] == far[:, :, None]) & (place[None, None, :] < place[None, :, None])
        )
        ranks.append(jnp.sum(before.astype(jnp.int32), axis=2))
        fars.append(far)
    return owner_k, steps, fars, ranks


def own_chip(array):
    return lax.dynamic_slice_in_dim(array, lax.axis_index("st_0"), 1, axis=0)[0]


def chip_requests(array):
    return lax.dynamic_slice_in_dim(array, 2 * lax.axis_index("st_0"), 2, axis=0).reshape(-1)


def routes_kernel(count, requests, size_ref, info_ref, fits_ref, cast_ref, fold_ref, starts, start, size, used, sem):
    z, k = lax.axis_index("st_0"), lax.axis_index("st_1")
    ring = lax.axis_size("st_0")
    reach = ring // 2
    pair = 2 * count
    twin_at = 2 * LENGTH
    lane = lax.broadcasted_iota(jnp.int32, starts.shape, 1)
    lanes = starts.shape[1]
    spot = lane % ring
    up = lane < 2 * ring
    now = jnp.zeros(starts.shape, jnp.int32)
    most = jnp.zeros(starts.shape, jnp.int32)
    for t in range(reach):
        if t > 0:
            ends = now + jnp.broadcast_to(size_ref[t - 1 : t, :], starts.shape)
            after = jnp.where(
                spot == ring - 1, pltpu.roll(ends, ring - 1, 1), pltpu.roll(ends, lanes - 1, 1)
            )
            before = jnp.where(
                spot == 0, pltpu.roll(ends, lanes - ring + 1, 1), pltpu.roll(ends, 1, 1)
            )
            now = jnp.maximum(jnp.where(up, after, before), now + LAG)
        starts[t : t + 1, :] = now[0:1, :]
        here = now + jnp.broadcast_to(size_ref[t : t + 1, :], starts.shape)
        most = jnp.maximum(most, jnp.where(lane < 4 * ring, here, 0))
    fits_ref[0] = (jnp.max(most) <= LENGTH).astype(jnp.int32)
    for n, (src, dst) in enumerate(((starts, start), (size_ref, size))):
        copy = pltpu.make_async_copy(src, dst, sem.at[n])
        copy.start()
        copy.wait()

    slots = count + 2 * LENGTH
    readers = 2 * MOST
    onward_at, final_at = (slots + 1) * readers, (slots + 1) * readers + 2 * LENGTH

    @pl.loop(0, onward_at)
    def _(i):
        fold_ref[i] = 2 * requests

    @pl.loop(0, slots + 1)
    def _(i):
        used[i] = 0

    @pl.loop(0, 2 * LENGTH)
    def _(i):
        fold_ref[onward_at + i] = 2 * LENGTH
        cast_ref[i] = 0

    def info(row, i):
        return info_ref[row * 2 * requests + i]

    def column(d, core, step):
        source = lax.rem(z - (1 - 2 * d) * step + 2 * ring, ring)
        return (2 * d + core) * ring + source

    last = LENGTH - 1
    for d in range(2):

        @pl.loop(0, pair)
        def _(p):
            rank = info(5, d * pair + p)
            far = info(6, d * pair + p)
            core = lax.div(p, count)
            mine = rank % 2 == k
            home = p % count + jnp.where(core == k, 0, count)

            @pl.when(mine)
            def _():
                cast_ref[d * LENGTH + rank // 2] = home

            @pl.when(core == k)
            def _():
                i = p % count
                near = jnp.where((far > 0) & mine, d * LENGTH + rank // 2, 2 * LENGTH)
                aside = jnp.where((far > 0) & (rank % 2 != k), d * count + rank // 2, 2 * count)
                fold_ref[final_at + d * count + i] = near
                fold_ref[final_at + (2 + d) * count + i] = aside

        for t in range(1, reach):
            lane_of = column(d, k, t)
            at_out, at_in = start[t, lane_of], start[t - 1, lane_of]

            @pl.loop(0, size[t, lane_of])
            def _(r):
                out = d * LENGTH + jnp.minimum(at_out + r, last)
                come = d * LENGTH + jnp.minimum(at_in + r, last)
                cast_ref[out] = pair + come
                fold_ref[onward_at + come] = out

    @pl.loop(0, 2 * requests)
    def _(i):
        c = lax.rem(i + k * requests, 2 * requests)
        step, way, rank, within, owner = (info(row, c) for row in range(5))
        core = jnp.where(step > 0, rank % 2, owner)
        lane_of = column(way, core, step)
        at = start[jnp.maximum(step - 1, 0), lane_of] + lax.div(rank, 2)
        at = way * LENGTH + jnp.minimum(at, last)
        where = pair + at + jnp.where(core == k, 0, twin_at)
        where = jnp.where(step > 0, where, within + jnp.where(core == k, 0, count))
        slot = jnp.where(core == k, jnp.where(step > 0, count + at, within), slots)
        turn = jnp.where(slot == slots, 0, jnp.minimum(used[slot], readers - 1))
        used[slot] = turn + 1
        fold_ref[slot * readers + turn] = i

        @pl.when(i < requests)
        def _():
            cast_ref[2 * LENGTH + i] = where


def stream_routes(ring, count, ids):
    devices, requests = ids.shape
    pair = 2 * count
    reach = ring // 2
    owner_k, steps, fars, ranks = needs(ring, count, ids)
    dist = jnp.arange(1, reach + 1, dtype=jnp.int32)
    core = jnp.arange(2, dtype=jnp.int32)
    far = jnp.stack(fars)
    whole = jnp.sum((far[None] >= dist[:, None, None, None]).astype(jnp.int32), axis=3)
    size = (whole[:, :, None, :] + 1 - core[None, None, :, None]) // 2
    size = jnp.pad(size.reshape(reach, 4 * ring), ((0, 0), (0, 128 - 4 * ring)))
    chip_ids = chip_requests(ids)
    every = jnp.arange(devices * count, dtype=jnp.int32)
    chip_hot = chip_ids[:, None] == every[None, :]
    step = [chip_requests(s) for s in steps]
    way = (step[1] > 0).astype(jnp.int32)
    ranked = [jnp.sum(jnp.where(chip_hot, r.reshape(-1)[None, :], 0), axis=1) for r in ranks]
    info = jnp.concatenate(
        [
            step[0] + step[1],
            way,
            jnp.where(way == 0, ranked[0], ranked[1]),
            chip_ids % count,
            chip_requests(owner_k),
            own_chip(ranks[0]),
            own_chip(ranks[1]),
            own_chip(fars[0]),
            own_chip(fars[1]),
        ]
    ).astype(jnp.int32)
    slots = count + 2 * LENGTH
    fold_size = (slots + 1) * 2 * MOST + 2 * LENGTH + 4 * count
    return pl.pallas_call(
        functools.partial(routes_kernel, count, requests),
        out_shape=[
            jax.ShapeDtypeStruct((1,), jnp.int32),
            jax.ShapeDtypeStruct((2 * LENGTH + requests,), jnp.int32),
            jax.ShapeDtypeStruct((fold_size,), jnp.int32),
        ],
        in_specs=[VMEM_SPEC, SMEM_SPEC],
        out_specs=[SMEM_SPEC] * 3,
        scratch_shapes=[
            pltpu.VMEM((reach, 128), jnp.int32),
            pltpu.SMEM((reach, 128), jnp.int32),
            pltpu.SMEM((reach, 128), jnp.int32),
            pltpu.SMEM((slots + 1,), jnp.int32),
            pltpu.SemaphoreType.DMA((2,)),
        ],
        name="routes",
    )(size, info)


def project(rows_list, weight_list, out_ref, n, tile):
    cols = pl.ds(n * tile, tile)
    total = None
    for rows, weight in zip(rows_list, weight_list):
        term = lax.dot_general(
            rows[...], weight[cols, :], (((1,), (1,)), ((), ())), preferred_element_type=F32
        )
        total = term if total is None else total + term
    out_ref[:, cols] = total.astype(out_ref.dtype)


def tail_kernel(sums_ref, all_ref, tokens_ref, tokens_in, *refs):
    weights, refs = refs[:8], refs[8:]
    d_tokens_ref, d_store_ref, d_wkey_ref = refs[:3]
    wbuf_t, wbuf_s, own_t, in_t, own_s, in_s, refs = *refs[3:9], refs[9:]
    keys, keys_turned, all_buf, terms, twin_terms, sent, come, last, last_in, refs = *refs[:9], refs[9:]
    load_sem, *sems = refs
    exchange, gifts, ring_copies = (Copies(*sems[2 * i : 2 * i + 2]) for i in range(3))
    place = Place()
    tp, ring = place.tp, place.ring
    reach = ring // 2
    peers = [place.along_x(rel) for rel in range(1, tp)]
    loads = []

    def load(src, dst):
        copy = pltpu.make_async_copy(src, dst, load_sem.at[len(loads)])
        copy.start()
        loads.append(copy)

    load(sums_ref, keys)
    for n in range(tp):
        load(all_ref.at[n], all_buf.at[n])
    greet(place.twin, place.along_z(1), place.along_z(-1), *peers)
    share = sums_ref.shape[0] // tp
    for rel, peer in enumerate(peers, 1):
        exchange.start(
            sums_ref.at[pl.ds(peer[3] * share, share)], in_s.at[tp - 1 - rel], peer
        )
    block = own_t.shape[0]
    load(tokens_ref.at[pl.ds(place.x * block, block)], own_t)
    load(tokens_in, in_t)
    load(sums_ref.at[pl.ds(place.x * share, share)], own_s)
    for wbuf, (wa, wb, wa_far, wb_far) in ((wbuf_t, weights[:4]), (wbuf_s, weights[4:])):
        load(wa, wbuf.at[0])
        load(wb, wbuf.at[1])
        load(wa_far, wbuf.at[pl.ds(2, tp - 1)])
        load(wb_far, wbuf.at[pl.ds(2 + tp - 1, tp - 1)])
    count, pass_len, pair = sums_ref.shape
    rows, cols = count * pass_len, pair // 2
    depth = all_ref.shape[3]
    width = terms.shape[3]
    loads[0].wait()
    keys_turned[...] = keys[:, :, :cols].reshape(rows, cols).T
    for n in range(tp):
        loads[1 + n].wait()
        term = jnp.dot(
            keys_turned[...], all_buf[n].reshape(rows, depth), preferred_element_type=F32
        )
        for c in range(depth // width):
            for h in range(2):
                terms[h, n * (depth // width) + c] = term[
                    h * (cols // 2) : (h + 1) * (cols // 2), c * width : (c + 1) * width
                ]
    gift = gifts.start(terms.at[1 - place.k], twin_terms, place.twin)
    for copy in loads[1 + tp :]:
        copy.wait()

    def operands(own, far_rows, wbuf):
        n_cols = own.shape[-1] // 2
        rows_list, weight_list = [], []
        for c in range(2):
            rows_list.append(own.at[:, pl.ds(c * n_cols, n_cols)])
            weight_list.append(wbuf.at[c])
        for rel in range(tp - 1):
            for c in range(2):
                rows_list.append(far_rows.at[rel, :, pl.ds(c * n_cols, n_cols)])
                weight_list.append(wbuf.at[2 + c * (tp - 1) + rel])
        return rows_list, weight_list

    part_rows = share * pass_len
    tile = 512
    tiles = d_tokens_ref.shape[1] // tile
    for_tokens = operands(own_t, in_t, wbuf_t)
    for_store = operands(
        own_s.reshape(part_rows, pair), in_s.reshape(tp - 1, part_rows, pair), wbuf_s
    )
    gift.wait_recv()
    hops = {}

    def mine(dest):
        return terms[place.k, dest] + twin_terms[dest]

    done = 0
    for s in range(1, reach + 1):
        for d in range(2):
            to_go = reach - d + 1 - s
            if to_go < 1:
                continue
            turn = 1 - 2 * d
            total = mine(lax.rem(place.z + turn * to_go + ring, ring))
            n = d * reach + s - 1
            if s > 1:
                hops[d, s - 1].wait_recv()
                total += come[n - 1].astype(F32)
            sent[n] = total.astype(sent.dtype)
            hops[d, s] = ring_copies.start(sent.at[n], come.at[n], place.along_z(turn))
        if s == reach // 2:
            for copy in exchange.all:
                copy.wait_recv()
        if s <= reach // 2:
            for _ in range(-(-tiles // (reach // 2))):
                if done < tiles:
                    project(*for_tokens, d_tokens_ref, done, tile)
                    done += 1
        elif s < reach:
            for _ in range(-(-tiles // (reach // 2 - 1))):
                if done < 2 * tiles:
                    project(*for_store, d_store_ref, done - tiles, tile)
                    done += 1
    total = mine(place.z)
    for d in range(2):
        hops[d, reach - d].wait_recv()
        total += come[d * reach + reach - d - 1].astype(F32)
    turned = total.T
    out_rows = turned.shape[0] // 2
    for c in range(2):
        last[c] = turned[c * out_rows : (c + 1) * out_rows]
    end = gifts.start(last.at[1 - place.k], last_in, place.twin)
    half = cols // 2
    d_wkey_ref[:, pl.ds(pl.multiple_of(place.k * half, half), half)] = last[place.k]
    end.wait_recv()
    d_wkey_ref[:, pl.ds(pl.multiple_of((1 - place.k) * half, half), half)] = last_in[...]
    for group in (exchange, gifts, ring_copies):
        group.wait_sends()


def tail(ident, sums, all_rows, tokens, tokens_in, weights):
    tp, ring = lax.axis_size("tp"), lax.axis_size("st_0")
    model, head_cols = weights[0].shape
    count, pass_len, pair = sums.shape
    share = count // tp
    width = model // ring
    low = sums.dtype
    return pl.pallas_call(
        tail_kernel,
        out_shape=[
            jax.ShapeDtypeStruct((tokens.shape[0] // tp, model), low),
            jax.ShapeDtypeStruct((share * pass_len, model), low),
            jax.ShapeDtypeStruct((width // 2, head_cols), F32),
        ],
        in_specs=[ANY_SPEC] * (4 + len(weights)),
        out_specs=[VMEM_SPEC] * 3,
        scratch_shapes=[
            pltpu.VMEM((2 * tp, model, head_cols), low),
            pltpu.VMEM((2 * tp, model, head_cols), low),
            pltpu.VMEM((tokens.shape[0] // tp, tokens.shape[1]), low),
            pltpu.VMEM(tokens_in.shape, low),
            pltpu.VMEM((share, pass_len, pair), low),
            pltpu.VMEM((tp - 1, share, pass_len, pair), low),
            pltpu.VMEM(sums.shape, low),
            pltpu.VMEM((head_cols, count * pass_len), low),
            pltpu.VMEM(all_rows.shape, low),
            pltpu.VMEM((2, ring, head_cols // 2, width), F32),
            pltpu.VMEM((ring, head_cols // 2, width), F32),
            pltpu.VMEM((ring, head_cols // 2, width), low),
            pltpu.VMEM((ring, head_cols // 2, width), low),
            pltpu.VMEM((2, width // 2, head_cols // 2), F32),
            pltpu.VMEM((width // 2, head_cols // 2), F32),
            pltpu.SemaphoreType.DMA((4 + tp + len(weights),)),
        ]
        + copy_sems(tp - 1)
        + copy_sems(2)
        + copy_sems(ring - 1),
        compiler_params=pltpu.CompilerParams(
            collective_id=ident, has_side_effects=True, vmem_limit_bytes=VMEM_LIMIT
        ),
        name="tail",
    )(sums, all_rows, tokens, tokens_in, *weights)


def first_slot(plan, d, step):
    total = jnp.zeros_like(step)
    for t, at in plan.base[d].items():
        total = total + jnp.where(step == t, at, 0)
    return total


def routes(plan, ids):
    count, slots = plan.passages, plan.slots
    me_k = lax.axis_index("st_1")
    requests = ids.shape[1]
    every = jnp.arange(ids.shape[0] * count, dtype=jnp.int32)
    owner_k, steps, fars, ranks = needs(plan.ring, count, ids)
    place = jnp.arange(2 * count, dtype=jnp.int32)
    at_home = place % count + jnp.where(place // count == me_k, 0, count)
    want = 2 * jnp.arange(count, dtype=jnp.int32) + me_k
    order, final = [], []
    for d in range(2):
        rank, far = own_chip(ranks[d]), own_chip(fars[d])
        order.append(jnp.sum(jnp.where(rank[None, :] == want[:, None], at_home[None, :], 0), axis=1))
        twin_at = plan.slots - count
        near = plan.base[d][1] - count
        aside = twin_at + d * (plan.layout[1] // 2)
        index = jnp.where(rank % 2 == me_k, near, aside) + rank // 2
        index = jnp.where(far > 0, index, twin_at + plan.layout[1])
        final.append(lax.dynamic_slice_in_dim(index, me_k * count, count))
    chip_ids = chip_requests(ids)
    chip_hot = chip_ids[:, None] == every[None, :]
    slot, core = chip_ids % count, chip_requests(owner_k)
    for d in range(2):
        rank = jnp.sum(jnp.where(chip_hot, ranks[d].reshape(-1)[None, :], 0), axis=1)
        step = chip_requests(steps[d])
        slot = jnp.where(step > 0, first_slot(plan, d, step) + rank // 2, slot)
        core = jnp.where(step > 0, rank % 2, core)
    where = slot + jnp.where(core == me_k, 0, slots)
    where = lax.dynamic_slice_in_dim(where, me_k * requests, requests)
    mine = jnp.where(core == me_k, slot, -1).reshape(2, requests)
    mine = jnp.where(me_k == 0, mine, mine[::-1]).reshape(-1)
    table = readers_table(mine, slots, 2 * requests)
    tables = (jnp.concatenate(order), where, jnp.concatenate(final))
    order, where, final = (t.astype(jnp.int32) for t in tables)
    return order, where, table, final


def local(pass_ids, store, queries, gate_pre, w_query, w_gate, w_key, w_value, d_mem):
    tp_count = lax.axis_size("tp")
    ring = lax.axis_size("st_0")
    passages, pass_len, _ = store.shape
    model_width = w_key.shape[0]
    requests = pass_ids.size
    plan = Plan(ring, passages)
    ids = jnp.zeros((8, 128), jnp.int32).at[0, :requests].set(pass_ids.reshape(-1))
    ids, all_rows, kv = front(5, ids, store, w_key, w_value)
    ids = ids[:, :, 0, :requests].reshape(2 * ring, requests)
    fits, cast_table, fold_table = stream_routes(ring, passages, ids)
    fits = fits[0] > 0

    def cast_short(ids, table, kv, weights):
        return stream_cast(0, table, kv, weights)

    def cast_any(ids, table, kv, weights):
        order, where, _, _ = routes(plan, ids)
        return cast_rows(plan, 1, order, where, kv, weights)

    def fold_short(ids, table, grads, tokens):
        return stream_fold(2, passages, table, grads, tokens)

    def fold_any(ids, table, grads, tokens):
        _, _, table, final = routes(plan, ids)
        return fold_rows(plan, 3, table, final, grads, tokens)

    weights = (w_query, w_gate, w_key, w_value)
    request_kv, wq_far, wg_far, wk_far, wv_far = lax.cond(
        fits, cast_short, cast_any, ids, cast_table, kv, weights
    )
    request_grads, token_grads = attend(queries, gate_pre, d_mem, request_kv)
    sums, tokens_in = lax.cond(
        fits, fold_short, fold_any, ids, fold_table, request_grads, token_grads
    )
    d_tokens, d_store, d_wkey = tail(
        4,
        sums,
        all_rows,
        token_grads,
        tokens_in,
        (w_query, w_gate, wq_far, wg_far, w_key, w_value, wk_far, wv_far),
    )
    return d_tokens, d_store.reshape(passages // tp_count, pass_len, model_width), d_wkey


def solution(mesh):
    finer = Mesh(
        mesh.devices.reshape(mesh.shape["grp"], -1, 2, mesh.shape["tp"]),
        ("grp", "st_0", "st_1", "tp"),
    )
    in_specs = (
        P(GRP_ST, None),
        P(ST, None, "tp"),
        P(GRP_ST, "tp"),
        P(GRP_ST, "tp"),
        P(None, "tp"),
        P(None, "tp"),
        P(None, "tp"),
        P(None, "tp"),
        P(GRP_ST, "tp"),
    )
    out_specs = (P(GRP_ST_TP, None), P(GRP_ST_TP, None, None), P(GRP_ST, "tp"))
    return jax.shard_map(local, mesh=finer, in_specs=in_specs, out_specs=out_specs, check_vma=False)
```

```python
import functools

import jax
import jax.numpy as jnp
from jax import lax
from jax.experimental import pallas as pl
from jax.experimental.pallas import tpu as pltpu
from jax.sharding import Mesh
from jax.sharding import PartitionSpec as P

HD = 256
BLK = 128
PB = 4
MOST = 2
CHUNK = 4
LENGTH = 54
STAGE = 2
LAG = 2 * STAGE
VMEM_LIMIT = 62 * 1024 * 1024
ST = ("st_0", "st_1")
GRP_ST = ("grp", "st_0", "st_1")
GRP_ST_TP = ("grp", "st_0", "st_1", "tp")
MESH_ID = pl.DeviceIdType.MESH
VMEM_SPEC = pl.BlockSpec(memory_space=pltpu.VMEM)
SMEM_SPEC = pl.BlockSpec(memory_space=pltpu.SMEM)
ANY_SPEC = pl.BlockSpec(memory_space=pl.ANY)
F32 = jnp.float32


class Plan:
    def __init__(self, ring, passages):
        self.ring = ring
        self.passages = passages
        self.reach = ring // 2
        self.steps_of = range(1, self.reach + 1)
        per_owner = 2 * MOST
        self.layout = {
            t: min(passages, per_owner * (self.reach - t + 1))
            + min(passages, per_owner * (self.reach - t))
            for t in self.steps_of
        }
        self.sizes = self.layout
        self.base = [{}, {}]
        at = passages
        for d in range(2):
            for t in self.steps_of:
                self.base[d][t] = at
                at += -(-self.layout[t] // 2)
        self.slots = at

    def half(self, t):
        return -(-self.sizes[t] // 2) if t <= self.reach else 0

    def steps(self, down=False):
        for t in reversed(self.steps_of) if down else self.steps_of:
            for first in range(0, self.half(t), CHUNK):
                for d in range(2):
                    yield d, t, first, min(CHUNK, self.half(t) - first)


class Place:
    def __init__(self):
        self.g, self.z, self.k, self.x = (lax.axis_index(a) for a in GRP_ST_TP)
        self.ring = lax.axis_size("st_0")
        self.tp = lax.axis_size("tp")
        self.twin = (self.g, self.z, 1 - self.k, self.x)

    def along_z(self, step):
        return (self.g, lax.rem(self.z + step + self.ring, self.ring), self.k, self.x)

    def along_x(self, step):
        return (self.g, self.z, self.k, lax.rem(self.x + step + self.tp, self.tp))


def greet(*devices):
    barrier = pltpu.get_barrier_semaphore()
    for device in devices:
        pl.semaphore_signal(barrier, inc=1, device_id=device, device_id_type=MESH_ID)
    pl.semaphore_wait(barrier, len(devices))


class Copies:
    def __init__(self, send_sem, recv_sem):
        self.send_sem, self.recv_sem = send_sem, recv_sem
        self.all = []

    def start(self, src, dst, device):
        n = len(self.all)
        copy = pltpu.make_async_remote_copy(
            src_ref=src,
            dst_ref=dst,
            send_sem=self.send_sem.at[n],
            recv_sem=self.recv_sem.at[n],
            device_id=device,
            device_id_type=MESH_ID,
        )
        copy.start()
        self.all.append(copy)
        return copy

    def wait_sends(self):
        for copy in self.all:
            copy.wait_send()


def copy_sems(count):
    return [pltpu.SemaphoreType.DMA((count,)), pltpu.SemaphoreType.DMA((count,))]


def ids_kernel(ids_ref, ids_out, *sems):
    gifts, ring_copies = (Copies(*sems[2 * i : 2 * i + 2]) for i in range(2))
    place = Place()
    reach = place.ring // 2
    greet(place.along_z(1), place.along_z(-1), place.twin)
    gift = gifts.start(ids_ref, ids_out.at[place.z, place.k], place.twin)
    ids_out[place.z, place.k] = ids_ref[...]
    gift.wait_recv()
    hops = {}
    for t in range(1, reach + 1):
        for d in range(2):
            if t > reach - d:
                continue
            if t > 1:
                hops[d, t - 1].wait_recv()
            source = lax.rem(place.z + (t - 1) * (2 * d - 1) + place.ring, place.ring)
            part = ids_out.at[source]
            hops[d, t] = ring_copies.start(part, part, place.along_z(1 - 2 * d))
    for d in range(2):
        hops[d, reach - d].wait_recv()
    for group in (gifts, ring_copies):
        group.wait_sends()


def gather_ids(ident, ids):
    ring = lax.axis_size("st_0")
    return pl.pallas_call(
        ids_kernel,
        out_shape=jax.ShapeDtypeStruct((ring, 2, *ids.shape), ids.dtype),
        in_specs=[VMEM_SPEC],
        out_specs=VMEM_SPEC,
        scratch_shapes=copy_sems(1) + copy_sems(ring - 1),
        compiler_params=pltpu.CompilerParams(
            collective_id=ident, has_side_effects=True, vmem_limit_bytes=8 * 1024 * 1024
        ),
        cost_estimate=pl.CostEstimate(flops=9 * 10**9, bytes_accessed=10**6, transcendentals=0),
        name="gather_ids",
    )(ids)


def keys_values_kernel(own_ref, ahead_ref, behind_ref, low_ref, high_ref, wk_ref, wv_ref, kv_ref):
    x, tp = lax.axis_index("tp"), lax.axis_size("tp")
    count, pass_len, depth = own_ref.shape
    rows, cols = count * pass_len, wk_ref.shape[1]
    early = pl.program_id(0) < pl.num_programs(0) // 2
    opposite = jnp.where(early, low_ref[...], high_ref[...])
    parts = (own_ref[...], ahead_ref[...], opposite, behind_ref[...])
    for c, w_ref in enumerate((wk_ref, wv_ref)):
        total = None
        for rel, part in enumerate(parts):
            at = pl.multiple_of(lax.rem(x + rel, tp) * depth, depth)
            weight = w_ref[pl.ds(at, depth), :]
            term = jnp.dot(part.reshape(rows, depth), weight, preferred_element_type=F32)
            total = term if total is None else total + term
        at = slice(c * cols, (c + 1) * cols)
        kv_ref[:, :, at] = total.reshape(count, pass_len, cols).astype(kv_ref.dtype)


def keys_values(pieces, w_key, w_value):
    count, rows, depth = pieces[0].shape
    pair = 2 * w_key.shape[1]
    steps = 4
    block = (count // steps, rows, depth)
    whole = pl.BlockSpec(block, lambda i: (i, 0, 0))
    low = pl.BlockSpec(block, lambda i: (jnp.minimum(i, steps // 2 - 1), 0, 0))
    high = pl.BlockSpec(block, lambda i: (jnp.maximum(i - steps // 2, 0), 0, 0))
    weight = pl.BlockSpec(w_key.shape, lambda i: (0, 0))
    return pl.pallas_call(
        keys_values_kernel,
        grid=(steps,),
        out_shape=jax.ShapeDtypeStruct((count, rows, pair), pieces[0].dtype),
        in_specs=[whole, whole, whole, low, high, weight, weight],
        out_specs=pl.BlockSpec((count // steps, rows, pair), lambda i: (i, 0, 0)),
        name="keys_values",
    )(*pieces, w_key, w_value)


def gather_store(store):
    tp = lax.axis_size("tp")
    half = store.shape[0] // 2
    up = [(i, (i + 1) % tp) for i in range(tp)]
    down = [(i, (i - 1) % tp) for i in range(tp)]
    behind = lax.ppermute(store, "tp", up)
    ahead = lax.ppermute(store, "tp", down)
    low = lax.ppermute(behind[:half], "tp", up)
    high = lax.ppermute(ahead[half:], "tp", down)
    return store, ahead, behind, low, high


def attend_kernel(scale, q_ref, gate_ref, mem_ref, kv_ref, grads_ref, tokens_ref):
    blocks = q_ref.shape[0] // BLK
    cols = q_ref.shape[1]
    pass_len = kv_ref.shape[1]
    low = q_ref.dtype

    def dot(a, b, ca, cb):
        return lax.dot_general(a, b, (((ca,), (cb,)), ((), ())), preferred_element_type=F32)

    for b in range(blocks):
        toks = pl.ds(b * BLK, BLK)
        kv = kv_ref[pl.ds(b * PB, PB)].reshape(PB * pass_len, 2 * cols)
        for h in range(cols // HD):
            k_at = slice(h * HD, (h + 1) * HD)
            v_at = slice(cols + h * HD, cols + (h + 1) * HD)
            q, keys, values = q_ref[toks, k_at], kv[:, k_at], kv[:, v_at]
            scores = dot(q, keys, 1, 1) * scale
            shifted = jnp.exp(scores - jnp.max(scores, axis=-1, keepdims=True))
            probs = shifted / jnp.sum(shifted, axis=-1, keepdims=True)
            probs_low = probs.astype(low)
            attended = dot(probs_low, values, 1, 0)
            gate = gate_ref[toks, k_at].astype(F32)
            mem = mem_ref[toks, k_at].astype(F32)
            sig = jax.nn.sigmoid(gate)
            attended_grad = (gate * sig * mem).astype(low)
            gate_grad = mem * attended * sig * (1.0 + gate * (1.0 - sig))
            prob_grad = dot(attended_grad, values, 1, 1)
            inner = jnp.sum(probs * prob_grad, axis=-1, keepdims=True)
            score_grad = (scale * probs * (prob_grad - inner)).astype(low)
            tokens_ref[toks, k_at] = dot(score_grad, keys, 1, 0).astype(low)
            tokens_ref[toks, v_at] = gate_grad.astype(low)
            key_grad = dot(score_grad, q, 0, 0).astype(low)
            value_grad = dot(probs_low, attended_grad, 0, 0).astype(low)
            passes = pl.ds(b * PB, PB)
            grads_ref[passes, :, k_at] = key_grad.reshape(PB, pass_len, HD)
            grads_ref[passes, :, v_at] = value_grad.reshape(PB, pass_len, HD)


def attend(queries, gate_pre, d_mem, request_kv):
    toks, cols = queries.shape
    _, pass_len, pair = request_kv.shape
    step = 2
    grid = toks // BLK // step
    tok_spec = pl.BlockSpec((step * BLK, cols), lambda i: (i, 0))
    kv_spec = pl.BlockSpec((step * PB, pass_len, pair), lambda i: (i, 0, 0))
    return pl.pallas_call(
        functools.partial(attend_kernel, HD**-0.5),
        grid=(grid,),
        out_shape=[
            jax.ShapeDtypeStruct(request_kv.shape, request_kv.dtype),
            jax.ShapeDtypeStruct((toks, pair), queries.dtype),
        ],
        in_specs=[tok_spec, tok_spec, tok_spec, kv_spec],
        out_specs=[kv_spec, pl.BlockSpec((step * BLK, pair), lambda i: (i, 0))],
        name="attend",
    )(queries, gate_pre, d_mem, request_kv)


def cast_kernel(plan, weights, order_ref, where_ref, kv_ref, *refs):
    w_refs, refs = refs[:weights], refs[weights:]
    out_ref, w_outs, refs = refs[0], refs[1 : 1 + weights], refs[1 + weights :]
    buf, first_buf, home, *sems = refs
    ring_copies, gifts, w_copies = (Copies(*sems[2 * i : 2 * i + 2]) for i in range(3))
    place = Place()
    count, slots = plan.passages, plan.slots
    top = plan.half(1)

    greet(place.along_z(1), place.along_z(-1), place.along_x(1), place.along_x(-1), place.twin)
    own_gift = gifts.start(kv_ref, home.at[pl.ds(count, count)], place.twin)

    @pl.loop(0, count)
    def _(j):
        home[j] = kv_ref[j]
        buf[j] = kv_ref[j]

    own_gift.wait_recv()

    @pl.loop(0, top)
    def _(j):
        for d in range(2):
            first_buf[d * top + j] = home[order_ref[d * count + j]]

    copies = {}
    steps = list(plan.steps())
    extent = {(d, t, first): size for d, t, first, size in steps}

    def send(d, t, first):
        size = extent[d, t, first]
        if t == 1:
            src = first_buf.at[pl.ds(d * top + first, size)]
        else:
            src = buf.at[pl.ds(plan.base[d][t - 1] + first, size)]
        dst = buf.at[pl.ds(plan.base[d][t] + first, size)]
        copies[d, t, first] = ring_copies.start(src, dst, place.along_z(1 - 2 * d))

    for d, t, first, _ in steps:
        if t == 1:
            send(d, t, first)
    rows = w_refs[0].shape[0] // 2
    half = pl.ds(place.k * rows, rows)
    arrive = [[], []]
    for w_ref, w_out in zip(w_refs, w_outs):
        arrive[0].append(
            w_copies.start(w_ref.at[half], w_out.at[2, half], place.along_x(1))
        )
        arrive[1].append(
            w_copies.start(w_ref.at[half], w_out.at[0, half], place.along_x(-1))
        )
    w_gifts = []
    middle = []

    def forward_weights():
        for copy in arrive[0] + arrive[1]:
            copy.wait_recv()
        for w_out in w_outs:
            middle.append(
                w_copies.start(
                    w_out.at[2 * place.k, half],
                    w_out.at[1, half],
                    place.along_x(2 * place.k - 1),
                )
            )
            for rel in (0, 2):
                part = w_out.at[rel, half]
                w_gifts.append(w_copies.start(part, part, place.twin))

    last = None
    for d, t, first, size in steps:
        if t != last and t == plan.reach // 2 + 1:
            forward_weights()
        last = t
        copies[d, t, first].wait_recv()
        if (d, t + 1, first) in extent:
            send(d, t + 1, first)
        at = plan.base[d][t] + first
        gifts.start(buf.at[pl.ds(at, size)], buf.at[pl.ds(slots + at, size)], place.twin)
    for copy, w_out in zip(middle, w_outs):
        copy.wait_recv()
        part = w_out.at[1, half]
        w_gifts.append(w_copies.start(part, part, place.twin))
    for gift in gifts.all[1:]:
        gift.wait_recv()

    @pl.loop(0, count)
    def _(j):
        buf[slots + j] = home[count + j]

    @pl.loop(0, out_ref.shape[0])
    def _(r):
        out_ref[r] = buf[where_ref[r]]

    for gift in w_gifts:
        gift.wait_recv()
    for group in (gifts, ring_copies, w_copies):
        group.wait_sends()


def cast_rows(plan, ident, order, where, kv, weights):
    count, rows, cols = kv.shape
    steps = len(list(plan.steps()))
    others = lax.axis_size("tp") - 1
    return pl.pallas_call(
        functools.partial(cast_kernel, plan, len(weights)),
        out_shape=[jax.ShapeDtypeStruct((where.shape[0], rows, cols), kv.dtype)]
        + [jax.ShapeDtypeStruct((others, *w.shape), w.dtype) for w in weights],
        in_specs=[SMEM_SPEC, SMEM_SPEC, VMEM_SPEC] + [ANY_SPEC] * len(weights),
        out_specs=[VMEM_SPEC] + [ANY_SPEC] * len(weights),
        scratch_shapes=[
            pltpu.VMEM((2 * plan.slots, rows, cols), kv.dtype),
            pltpu.VMEM((2 * plan.half(1), rows, cols), kv.dtype),
            pltpu.VMEM((2 * count, rows, cols), kv.dtype),
        ]
        + copy_sems(steps)
        + copy_sems(steps + 1)
        + copy_sems(6 * len(weights)),
        compiler_params=pltpu.CompilerParams(
            collective_id=ident, has_side_effects=True, vmem_limit_bytes=VMEM_LIMIT
        ),
        name="cast_rows",
    )(order, where, kv, *weights)


def fold_kernel(
    plan,
    table_ref,
    final_ref,
    grads_ref,
    tokens_ref,
    out_ref,
    tokens_out,
    held,
    here,
    sums,
    load_sem,
    *sems,
):
    ring_copies, gifts, exchange = (Copies(*sems[2 * i : 2 * i + 2]) for i in range(3))
    place = Place()
    count, top = plan.passages, plan.half(1)
    own = grads_ref.shape[0]
    readers = 2 * MOST
    twin_at = plan.slots - count
    zero_at = twin_at + plan.layout[1]
    peers = [place.along_x(rel) for rel in range(1, place.tp)]

    load = pltpu.make_async_copy(grads_ref, held.at[pl.ds(0, own)], load_sem)
    load.start()
    held[2 * own] = jnp.zeros_like(held[2 * own])
    here[zero_at] = jnp.zeros_like(here[zero_at])
    greet(place.along_z(1), place.along_z(-1), place.twin, *peers)
    own_gift = gifts.start(grads_ref, held.at[pl.ds(own, own)], place.twin)
    block = tokens_out.shape[1]
    for rel, peer in enumerate(peers, 1):
        exchange.start(
            tokens_ref.at[pl.ds(peer[3] * block, block)],
            tokens_out.at[place.tp - 1 - rel],
            peer,
        )
    load.wait()
    own_gift.wait_recv()

    def readers_sum(slot):
        total = held[table_ref[slot * readers]].astype(F32)
        for q in range(1, readers):
            total += held[table_ref[slot * readers + q]].astype(F32)
        return total

    copies = {}
    steps = list(plan.steps(down=True))
    extent = {(d, t, first): size for d, t, first, size in steps}
    for d, t, first, size in steps:
        at = plan.base[d][t] + first
        begin = extent.get((d, t + 1, first), 0)
        if begin:
            copies[d, t + 1, first].wait_recv()
            far_at = plan.base[d][t + 1] + first

            @pl.loop(0, begin)
            def _(j):
                total = readers_sum(at + j) + here[far_at - count + j].astype(F32)
                sums[at - count + j] = total.astype(sums.dtype)

        if begin < size:

            @pl.loop(begin, size)
            def _(j):
                sums[at - count + j] = readers_sum(at + j).astype(sums.dtype)

        part = pl.ds(at - count, size)
        copies[d, t, first] = ring_copies.start(
            sums.at[part], here.at[part], place.along_z(2 * d - 1)
        )
    for d, t, first, size in steps:
        if t == 1:
            copies[d, t, first].wait_recv()
            src = here.at[pl.ds(plan.base[d][1] - count + first, size)]
            dst = here.at[pl.ds(twin_at + d * (plan.layout[1] // 2) + first, size)]
            gifts.start(src, dst, place.twin)
    for gift in gifts.all[1:]:
        gift.wait_recv()

    @pl.loop(0, count)
    def _(p):
        total = readers_sum(p)
        for d in range(2):
            total += here[final_ref[d * count + p]].astype(F32)
        out_ref[p] = total.astype(out_ref.dtype)

    for copy in exchange.all:
        copy.wait_recv()
    for group in (gifts, ring_copies, exchange):
        group.wait_sends()


def fold_rows(plan, ident, table, final, grads, tokens):
    own, rows, cols = grads.shape
    steps = list(plan.steps())
    ends = sum(1 for _, t, _, _ in steps if t == 1)
    count = plan.passages
    tp = lax.axis_size("tp")
    return pl.pallas_call(
        functools.partial(fold_kernel, plan),
        out_shape=[
            jax.ShapeDtypeStruct((count, rows, cols), grads.dtype),
            jax.ShapeDtypeStruct((tp - 1, tokens.shape[0] // tp, tokens.shape[1]), tokens.dtype),
        ],
        in_specs=[SMEM_SPEC, SMEM_SPEC, ANY_SPEC, ANY_SPEC],
        out_specs=[VMEM_SPEC, ANY_SPEC],
        scratch_shapes=[
            pltpu.VMEM((2 * own + 1, rows, cols), grads.dtype),
            pltpu.VMEM((plan.slots - count + plan.layout[1] + 1, rows, cols), grads.dtype),
            pltpu.VMEM((plan.slots - count, rows, cols), grads.dtype),
            pltpu.SemaphoreType.DMA,
        ]
        + copy_sems(len(steps))
        + copy_sems(1 + ends)
        + copy_sems(tp - 1),
        compiler_params=pltpu.CompilerParams(
            collective_id=ident, has_side_effects=True, vmem_limit_bytes=VMEM_LIMIT
        ),
        name="fold_rows",
    )(table, final, grads, tokens)


def copy_slots(src, src_at, dst, dst_at, size):
    @pl.loop(0, size)
    def _(j):
        dst[dst_at + j] = src[src_at + j]


class WeightShare:
    def __init__(self, place, copies, w_refs, w_outs):
        self.place, self.copies, self.outs = place, copies, w_outs
        rows = w_refs[0].shape[0] // 2
        self.half = pl.ds(place.k * rows, rows)
        self.near, self.middle, self.gifts = [], [], []
        for w_ref, w_out in zip(w_refs, w_outs):
            for slot, step in ((2, 1), (0, -1)):
                src, dst = w_ref.at[self.half], w_out.at[slot, self.half]
                self.near.append(copies.start(src, dst, place.along_x(step)))

    def forward(self, n):
        for copy in self.near[2 * n : 2 * n + 2]:
            copy.wait_recv()
        w_out = self.outs[n]
        src = w_out.at[2 * self.place.k, self.half]
        dst = w_out.at[1, self.half]
        device = self.place.along_x(2 * self.place.k - 1)
        self.middle.append(self.copies.start(src, dst, device))
        for slot in (0, 2):
            self.give(w_out.at[slot, self.half])

    def give(self, part):
        self.gifts.append(self.copies.start(part, part, self.place.twin))

    def finish(self):
        for copy, w_out in zip(self.middle, self.outs):
            copy.wait_recv()
            self.give(w_out.at[1, self.half])

    def wait(self):
        for gift in self.gifts:
            gift.wait_recv()


def stream_cast_kernel(weights, table_ref, kv_ref, *refs):
    w_refs, refs = refs[:weights], refs[weights:]
    out_ref, w_outs, refs = refs[0], refs[1 : 1 + weights], refs[1 + weights :]
    kept, land, twin_land, leave, *sems = refs
    ring_copies, gifts, w_copies = (Copies(*sems[2 * i : 2 * i + 2]) for i in range(3))
    place = Place()
    count = kv_ref.shape[0]
    length = land.shape[0] // 2
    stages = length // STAGE
    home = 2 * count

    greet(place.along_z(1), place.along_z(-1), place.along_x(1), place.along_x(-1), place.twin)
    own_gift = gifts.start(kv_ref, kept.at[pl.ds(count, count)], place.twin)

    @pl.loop(0, count)
    def _(j):
        kept[j] = kv_ref[j]

    own_gift.wait_recv()
    sends, given = {}, {}
    share = None
    for i in range(stages + 4):
        for d in range(2):
            if 0 <= i - 2 < stages:
                at = d * length + (i - 2) * STAGE
                sends[d, i - 2].wait_recv()
                part = pl.ds(at, STAGE)
                given[d, i - 2] = gifts.start(land.at[part], twin_land.at[part], place.twin)
                copy_slots(land, at, kept, home + at, STAGE)
            if i < stages:
                at = d * length + i * STAGE

                @pl.loop(at, at + STAGE)
                def _(q):
                    leave[q] = kept[table_ref[q]]

            if 0 <= i - 4 < stages:
                at = d * length + (i - 4) * STAGE
                given[d, i - 4].wait_recv()
                copy_slots(twin_land, at, kept, home + 2 * length + at, STAGE)
        if i < stages:
            for d in range(2):
                part = pl.ds(d * length + i * STAGE, STAGE)
                sends[d, i] = ring_copies.start(
                    leave.at[part], land.at[part], place.along_z(1 - 2 * d)
                )
        if i == 1:
            share = WeightShare(place, w_copies, w_refs, w_outs)
        if i in (6, 10, 14, 18):
            share.forward((i - 6) // 4)
    share.finish()

    @pl.loop(0, out_ref.shape[0])
    def _(r):
        out_ref[r] = kept[table_ref[2 * length + r]]

    share.wait()
    for group in (gifts, ring_copies, w_copies):
        group.wait_sends()


def stream_cast(ident, table, kv, weights):
    count, rows, cols = kv.shape
    stages = LENGTH // STAGE
    others = lax.axis_size("tp") - 1
    return pl.pallas_call(
        functools.partial(stream_cast_kernel, len(weights)),
        out_shape=[jax.ShapeDtypeStruct((table.shape[0] - 2 * LENGTH, rows, cols), kv.dtype)]
        + [jax.ShapeDtypeStruct((others, *w.shape), w.dtype) for w in weights],
        in_specs=[SMEM_SPEC, VMEM_SPEC] + [ANY_SPEC] * len(weights),
        out_specs=[VMEM_SPEC] + [ANY_SPEC] * len(weights),
        scratch_shapes=[
            pltpu.VMEM((2 * count + 4 * LENGTH, rows, cols), kv.dtype),
            pltpu.VMEM((2 * LENGTH, rows, cols), kv.dtype),
            pltpu.VMEM((2 * LENGTH, rows, cols), kv.dtype),
            pltpu.VMEM((2 * LENGTH, rows, cols), kv.dtype),
        ]
        + copy_sems(2 * stages)
        + copy_sems(2 * stages + 1)
        + copy_sems(6 * len(weights)),
        compiler_params=pltpu.CompilerParams(
            collective_id=ident, has_side_effects=True, vmem_limit_bytes=VMEM_LIMIT
        ),
        name="stream_cast",
    )(table, kv, *weights)


def stream_fold_kernel(
    table_ref, grads_ref, tokens_ref, out_ref, tokens_out, held, kept, land,
    leave, twin_land, load_sem, *sems
):
    ring_copies, gifts, exchange = (Copies(*sems[2 * i : 2 * i + 2]) for i in range(3))
    place = Place()
    count = out_ref.shape[0]
    length = land.shape[0] // 2
    stages = length // STAGE
    own = grads_ref.shape[0]
    readers = 2 * MOST
    zero = 2 * length
    onward_at = (count + 2 * length + 1) * readers
    final_at = onward_at + 2 * length
    peers = [place.along_x(rel) for rel in range(1, place.tp)]

    load = pltpu.make_async_copy(grads_ref, held.at[pl.ds(0, own)], load_sem)
    load.start()
    blank = jnp.zeros_like(held[0])
    held[2 * own] = blank
    kept[zero] = blank
    twin_land[2 * count] = blank
    greet(place.along_z(1), place.along_z(-1), place.twin, *peers)
    own_gift = gifts.start(grads_ref, held.at[pl.ds(own, own)], place.twin)
    block = tokens_out.shape[1]
    for rel, peer in enumerate(peers, 1):
        exchange.start(
            tokens_ref.at[pl.ds(peer[3] * block, block)],
            tokens_out.at[place.tp - 1 - rel],
            peer,
        )
    load.wait()
    own_gift.wait_recv()

    def readers_sum(slot):
        total = held[table_ref[slot * readers]].astype(F32)
        for q in range(1, readers):
            total += held[table_ref[slot * readers + q]].astype(F32)
        return total

    sends = {}

    def arrive(i):
        for d in range(2):
            at = d * length + i * STAGE
            sends[d, i].wait_recv()
            if i * STAGE < count:
                src = land.at[pl.ds(at, STAGE)]
                dst = twin_land.at[pl.ds(d * count + i * STAGE, STAGE)]
                gifts.start(src, dst, place.twin)
            copy_slots(land, at, kept, at, STAGE)

    for i in reversed(range(stages)):
        if i + 2 < stages:
            arrive(i + 2)
        for d in range(2):
            at = d * length + i * STAGE

            @pl.loop(at, at + STAGE)
            def _(q):
                total = readers_sum(count + q) + kept[table_ref[onward_at + q]].astype(F32)
                leave[q] = total.astype(leave.dtype)

        for d in range(2):
            part = pl.ds(d * length + i * STAGE, STAGE)
            sends[d, i] = ring_copies.start(
                leave.at[part], land.at[part], place.along_z(2 * d - 1)
            )
    arrive(1)
    arrive(0)
    for gift in gifts.all[1:]:
        gift.wait_recv()

    @pl.loop(0, count)
    def _(p):
        total = readers_sum(p)
        for d in range(2):
            total += kept[table_ref[final_at + d * count + p]].astype(F32)
            total += twin_land[table_ref[final_at + (2 + d) * count + p]].astype(F32)
        out_ref[p] = total.astype(out_ref.dtype)

    for copy in exchange.all:
        copy.wait_recv()
    for group in (gifts, ring_copies, exchange):
        group.wait_sends()


def stream_fold(ident, count, table, grads, tokens):
    own, rows, cols = grads.shape
    stages = LENGTH // STAGE
    tp = lax.axis_size("tp")
    return pl.pallas_call(
        stream_fold_kernel,
        out_shape=[
            jax.ShapeDtypeStruct((count, rows, cols), grads.dtype),
            jax.ShapeDtypeStruct((tp - 1, tokens.shape[0] // tp, tokens.shape[1]), tokens.dtype),
        ],
        in_specs=[SMEM_SPEC, ANY_SPEC, ANY_SPEC],
        out_specs=[VMEM_SPEC, ANY_SPEC],
        scratch_shapes=[
            pltpu.VMEM((2 * own + 1, rows, cols), grads.dtype),
            pltpu.VMEM((2 * LENGTH + 1, rows, cols), grads.dtype),
            pltpu.VMEM((2 * LENGTH, rows, cols), grads.dtype),
            pltpu.VMEM((2 * LENGTH, rows, cols), grads.dtype),
            pltpu.VMEM((2 * count + 1, rows, cols), grads.dtype),
            pltpu.SemaphoreType.DMA,
        ]
        + copy_sems(2 * stages)
        + copy_sems(1 + 2 * (-(-count // STAGE)))
        + copy_sems(tp - 1),
        compiler_params=pltpu.CompilerParams(
            collective_id=ident, has_side_effects=True, vmem_limit_bytes=VMEM_LIMIT
        ),
        name="stream_fold",
    )(table, grads, tokens)


def readers_table(slot, slots, requests):
    at_slot = slot[:, None] == jnp.arange(slots, dtype=jnp.int32)[None, :]
    turn = jnp.cumsum(at_slot.astype(jnp.int32), axis=0)
    number = jnp.arange(requests, dtype=jnp.int32)[:, None]
    columns = [
        jnp.min(jnp.where(at_slot & (turn == q + 1), number, requests), axis=0)
        for q in range(2 * MOST)
    ]
    return jnp.stack(columns, axis=1).reshape(-1).astype(jnp.int32)


def needs(ring, count, ids):
    devices = ids.shape[0]
    pair = 2 * count
    every = jnp.arange(devices * count, dtype=jnp.int32)
    owner = ids // count
    owner_z, owner_k = owner // 2, owner % 2
    reader_z = (jnp.arange(devices, dtype=jnp.int32) // 2)[:, None]
    away = jnp.mod(reader_z - owner_z, ring)
    up = (2 * away < ring) | ((2 * away == ring) & (owner_k == 0))
    steps = (jnp.where(up, away, 0), jnp.where(up, 0, ring - away))
    hot = ids.reshape(-1)[:, None] == every[None, :]
    place = jnp.arange(pair, dtype=jnp.int32)
    ranks, fars = [], []
    for d in range(2):
        far = jnp.max(jnp.where(hot, steps[d].reshape(-1)[:, None], 0), axis=0)
        far = far.reshape(ring, pair)
        before = (far[:, None, :] > far[:, :, None]) | (
            (far[:, None, :] == far[:, :, None]) & (place[None, None, :] < place[None, :, None])
        )
        ranks.append(jnp.sum(before.astype(jnp.int32), axis=2))
        fars.append(far)
    return owner_k, steps, fars, ranks


def own_chip(array):
    return lax.dynamic_slice_in_dim(array, lax.axis_index("st_0"), 1, axis=0)[0]


def chip_requests(array):
    return lax.dynamic_slice_in_dim(array, 2 * lax.axis_index("st_0"), 2, axis=0).reshape(-1)


def routes_kernel(count, requests, size_ref, info_ref, fits_ref, cast_ref, fold_ref, starts, start, size, used, sem):
    z, k = lax.axis_index("st_0"), lax.axis_index("st_1")
    ring = lax.axis_size("st_0")
    reach = ring // 2
    pair = 2 * count
    twin_at = 2 * LENGTH
    lane = lax.broadcasted_iota(jnp.int32, starts.shape, 1)
    lanes = starts.shape[1]
    spot = lane % ring
    up = lane < 2 * ring
    now = jnp.zeros(starts.shape, jnp.int32)
    most = jnp.zeros(starts.shape, jnp.int32)
    for t in range(reach):
        if t > 0:
            ends = now + jnp.broadcast_to(size_ref[t - 1 : t, :], starts.shape)
            after = jnp.where(
                spot == ring - 1, pltpu.roll(ends, ring - 1, 1), pltpu.roll(ends, lanes - 1, 1)
            )
            before = jnp.where(
                spot == 0, pltpu.roll(ends, lanes - ring + 1, 1), pltpu.roll(ends, 1, 1)
            )
            now = jnp.maximum(jnp.where(up, after, before), now + LAG)
        starts[t : t + 1, :] = now[0:1, :]
        here = now + jnp.broadcast_to(size_ref[t : t + 1, :], starts.shape)
        most = jnp.maximum(most, jnp.where(lane < 4 * ring, here, 0))
    fits_ref[0] = (jnp.max(most) <= LENGTH).astype(jnp.int32)
    for n, (src, dst) in enumerate(((starts, start), (size_ref, size))):
        copy = pltpu.make_async_copy(src, dst, sem.at[n])
        copy.start()
        copy.wait()

    slots = count + 2 * LENGTH
    readers = 2 * MOST
    onward_at, final_at = (slots + 1) * readers, (slots + 1) * readers + 2 * LENGTH

    @pl.loop(0, onward_at)
    def _(i):
        fold_ref[i] = 2 * requests

    @pl.loop(0, slots + 1)
    def _(i):
        used[i] = 0

    @pl.loop(0, 2 * LENGTH)
    def _(i):
        fold_ref[onward_at + i] = 2 * LENGTH
        cast_ref[i] = 0

    def info(row, i):
        return info_ref[row * 2 * requests + i]

    def column(d, core, step):
        source = lax.rem(z - (1 - 2 * d) * step + 2 * ring, ring)
        return (2 * d + core) * ring + source

    last = LENGTH - 1
    for d in range(2):

        @pl.loop(0, pair)
        def _(p):
            rank = info(5, d * pair + p)
            far = info(6, d * pair + p)
            core = lax.div(p, count)
            mine = rank % 2 == k
            home = p % count + jnp.where(core == k, 0, count)

            @pl.when(mine)
            def _():
                cast_ref[d * LENGTH + rank // 2] = home

            @pl.when(core == k)
            def _():
                i = p % count
                near = jnp.where((far > 0) & mine, d * LENGTH + rank // 2, 2 * LENGTH)
                aside = jnp.where((far > 0) & (rank % 2 != k), d * count + rank // 2, 2 * count)
                fold_ref[final_at + d * count + i] = near
                fold_ref[final_at + (2 + d) * count + i] = aside

        for t in range(1, reach):
            lane_of = column(d, k, t)
            at_out, at_in = start[t, lane_of], start[t - 1, lane_of]

            @pl.loop(0, size[t, lane_of])
            def _(r):
                out = d * LENGTH + jnp.minimum(at_out + r, last)
                come = d * LENGTH + jnp.minimum(at_in + r, last)
                cast_ref[out] = pair + come
                fold_ref[onward_at + come] = out

    @pl.loop(0, 2 * requests)
    def _(i):
        c = lax.rem(i + k * requests, 2 * requests)
        step, way, rank, within, owner = (info(row, c) for row in range(5))
        core = jnp.where(step > 0, rank % 2, owner)
        lane_of = column(way, core, step)
        at = start[jnp.maximum(step - 1, 0), lane_of] + lax.div(rank, 2)
        at = way * LENGTH + jnp.minimum(at, last)
        where = pair + at + jnp.where(core == k, 0, twin_at)
        where = jnp.where(step > 0, where, within + jnp.where(core == k, 0, count))
        slot = jnp.where(core == k, jnp.where(step > 0, count + at, within), slots)
        turn = jnp.where(slot == slots, 0, jnp.minimum(used[slot], readers - 1))
        used[slot] = turn + 1
        fold_ref[slot * readers + turn] = i

        @pl.when(i < requests)
        def _():
            cast_ref[2 * LENGTH + i] = where


def stream_routes(ring, count, ids):
    devices, requests = ids.shape
    pair = 2 * count
    reach = ring // 2
    owner_k, steps, fars, ranks = needs(ring, count, ids)
    dist = jnp.arange(1, reach + 1, dtype=jnp.int32)
    core = jnp.arange(2, dtype=jnp.int32)
    far = jnp.stack(fars)
    whole = jnp.sum((far[None] >= dist[:, None, None, None]).astype(jnp.int32), axis=3)
    size = (whole[:, :, None, :] + 1 - core[None, None, :, None]) // 2
    size = jnp.pad(size.reshape(reach, 4 * ring), ((0, 0), (0, 128 - 4 * ring)))
    chip_ids = chip_requests(ids)
    every = jnp.arange(devices * count, dtype=jnp.int32)
    chip_hot = chip_ids[:, None] == every[None, :]
    step = [chip_requests(s) for s in steps]
    way = (step[1] > 0).astype(jnp.int32)
    ranked = [jnp.sum(jnp.where(chip_hot, r.reshape(-1)[None, :], 0), axis=1) for r in ranks]
    info = jnp.concatenate(
        [
            step[0] + step[1],
            way,
            jnp.where(way == 0, ranked[0], ranked[1]),
            chip_ids % count,
            chip_requests(owner_k),
            own_chip(ranks[0]),
            own_chip(ranks[1]),
            own_chip(fars[0]),
            own_chip(fars[1]),
        ]
    ).astype(jnp.int32)
    slots = count + 2 * LENGTH
    fold_size = (slots + 1) * 2 * MOST + 2 * LENGTH + 4 * count
    return pl.pallas_call(
        functools.partial(routes_kernel, count, requests),
        out_shape=[
            jax.ShapeDtypeStruct((1,), jnp.int32),
            jax.ShapeDtypeStruct((2 * LENGTH + requests,), jnp.int32),
            jax.ShapeDtypeStruct((fold_size,), jnp.int32),
        ],
        in_specs=[VMEM_SPEC, SMEM_SPEC],
        out_specs=[SMEM_SPEC] * 3,
        scratch_shapes=[
            pltpu.VMEM((reach, 128), jnp.int32),
            pltpu.SMEM((reach, 128), jnp.int32),
            pltpu.SMEM((reach, 128), jnp.int32),
            pltpu.SMEM((slots + 1,), jnp.int32),
            pltpu.SemaphoreType.DMA((2,)),
        ],
        cost_estimate=pl.CostEstimate(flops=6 * 10**9, bytes_accessed=10**5, transcendentals=0),
        name="routes",
    )(size, info)


def project(rows_list, weight_list, out_ref, n, tile):
    cols = pl.ds(n * tile, tile)
    total = None
    for rows, weight in zip(rows_list, weight_list):
        term = lax.dot_general(
            rows[...], weight[cols, :], (((1,), (1,)), ((), ())), preferred_element_type=F32
        )
        total = term if total is None else total + term
    out_ref[:, cols] = total.astype(out_ref.dtype)


def tail_kernel(sums_ref, tokens_ref, tokens_in, *refs):
    pieces, refs = refs[:5], refs[5:]
    weights, refs = refs[:8], refs[8:]
    d_tokens_ref, d_store_ref, d_wkey_ref = refs[:3]
    wbuf_t, wbuf_s, own_t, in_t, own_s, in_s, refs = *refs[3:9], refs[9:]
    keys, keys_turned, all_buf, terms, twin_terms, sent, come, last, last_in, refs = *refs[:9], refs[9:]
    load_sem, *sems = refs
    exchange, gifts, ring_copies = (Copies(*sems[2 * i : 2 * i + 2]) for i in range(3))
    place = Place()
    tp, ring = place.tp, place.ring
    reach = ring // 2
    peers = [place.along_x(rel) for rel in range(1, tp)]
    loads = []

    def load(src, dst):
        copy = pltpu.make_async_copy(src, dst, load_sem.at[len(loads)])
        copy.start()
        loads.append(copy)

    load(sums_ref, keys)
    own_piece, ahead, behind, low, high = pieces
    part = low.shape[0]
    load(own_piece, all_buf.at[0])
    load(ahead, all_buf.at[1])
    load(behind, all_buf.at[tp - 1])
    load(low, all_buf.at[2, pl.ds(0, part)])
    load(high, all_buf.at[2, pl.ds(part, part)])
    greet(place.twin, place.along_z(1), place.along_z(-1), *peers)
    share = sums_ref.shape[0] // tp
    for rel, peer in enumerate(peers, 1):
        exchange.start(
            sums_ref.at[pl.ds(peer[3] * share, share)], in_s.at[tp - 1 - rel], peer
        )
    block = own_t.shape[0]
    load(tokens_ref.at[pl.ds(place.x * block, block)], own_t)
    load(tokens_in, in_t)
    load(sums_ref.at[pl.ds(place.x * share, share)], own_s)
    for wbuf, (wa, wb, wa_far, wb_far) in ((wbuf_t, weights[:4]), (wbuf_s, weights[4:])):
        load(wa, wbuf.at[0])
        load(wb, wbuf.at[1])
        load(wa_far, wbuf.at[pl.ds(2, tp - 1)])
        load(wb_far, wbuf.at[pl.ds(2 + tp - 1, tp - 1)])
    count, pass_len, pair = sums_ref.shape
    rows, cols = count * pass_len, pair // 2
    depth = own_piece.shape[2]
    width = terms.shape[3]
    loads[0].wait()
    keys_turned[...] = keys[:, :, :cols].reshape(rows, cols).T
    for copy in loads[1:6]:
        copy.wait()
    for rel in range(tp):
        n = lax.rem(place.x + rel, tp)
        term = jnp.dot(
            keys_turned[...], all_buf[rel].reshape(rows, depth), preferred_element_type=F32
        )
        for c in range(depth // width):
            for h in range(2):
                terms[h, n * (depth // width) + c] = term[
                    h * (cols // 2) : (h + 1) * (cols // 2), c * width : (c + 1) * width
                ]
    gift = gifts.start(terms.at[1 - place.k], twin_terms, place.twin)
    for copy in loads[6:]:
        copy.wait()

    def operands(own, far_rows, wbuf):
        n_cols = own.shape[-1] // 2
        rows_list, weight_list = [], []
        for c in range(2):
            rows_list.append(own.at[:, pl.ds(c * n_cols, n_cols)])
            weight_list.append(wbuf.at[c])
        for rel in range(tp - 1):
            for c in range(2):
                rows_list.append(far_rows.at[rel, :, pl.ds(c * n_cols, n_cols)])
                weight_list.append(wbuf.at[2 + c * (tp - 1) + rel])
        return rows_list, weight_list

    part_rows = share * pass_len
    tile = 512
    tiles = d_tokens_ref.shape[1] // tile
    for_tokens = operands(own_t, in_t, wbuf_t)
    for_store = operands(
        own_s.reshape(part_rows, pair), in_s.reshape(tp - 1, part_rows, pair), wbuf_s
    )
    gift.wait_recv()
    hops = {}

    def mine(dest):
        return terms[place.k, dest] + twin_terms[dest]

    done = 0
    for s in range(1, reach + 1):
        for d in range(2):
            to_go = reach - d + 1 - s
            if to_go < 1:
                continue
            turn = 1 - 2 * d
            total = mine(lax.rem(place.z + turn * to_go + ring, ring))
            n = d * reach + s - 1
            if s > 1:
                hops[d, s - 1].wait_recv()
                total += come[n - 1].astype(F32)
            sent[n] = total.astype(sent.dtype)
            hops[d, s] = ring_copies.start(sent.at[n], come.at[n], place.along_z(turn))
        if s == reach // 2:
            for copy in exchange.all:
                copy.wait_recv()
        if s <= reach // 2:
            for _ in range(-(-tiles // (reach // 2))):
                if done < tiles:
                    project(*for_tokens, d_tokens_ref, done, tile)
                    done += 1
        elif s < reach:
            for _ in range(-(-tiles // (reach // 2 - 1))):
                if done < 2 * tiles:
                    project(*for_store, d_store_ref, done - tiles, tile)
                    done += 1
    total = mine(place.z)
    for d in range(2):
        hops[d, reach - d].wait_recv()
        total += come[d * reach + reach - d - 1].astype(F32)
    turned = total.T
    out_rows = turned.shape[0] // 2
    for c in range(2):
        last[c] = turned[c * out_rows : (c + 1) * out_rows]
    end = gifts.start(last.at[1 - place.k], last_in, place.twin)
    half = cols // 2
    d_wkey_ref[:, pl.ds(pl.multiple_of(place.k * half, half), half)] = last[place.k]
    end.wait_recv()
    d_wkey_ref[:, pl.ds(pl.multiple_of((1 - place.k) * half, half), half)] = last_in[...]
    for group in (exchange, gifts, ring_copies):
        group.wait_sends()


def tail(ident, sums, tokens, tokens_in, pieces, weights):
    tp, ring = lax.axis_size("tp"), lax.axis_size("st_0")
    model, head_cols = weights[0].shape
    count, pass_len, pair = sums.shape
    share = count // tp
    width = model // ring
    low = sums.dtype
    return pl.pallas_call(
        tail_kernel,
        out_shape=[
            jax.ShapeDtypeStruct((tokens.shape[0] // tp, model), low),
            jax.ShapeDtypeStruct((share * pass_len, model), low),
            jax.ShapeDtypeStruct((width // 2, head_cols), F32),
        ],
        in_specs=[ANY_SPEC] * (3 + len(pieces) + len(weights)),
        out_specs=[VMEM_SPEC] * 3,
        scratch_shapes=[
            pltpu.VMEM((2 * tp, model, head_cols), low),
            pltpu.VMEM((2 * tp, model, head_cols), low),
            pltpu.VMEM((tokens.shape[0] // tp, tokens.shape[1]), low),
            pltpu.VMEM(tokens_in.shape, low),
            pltpu.VMEM((share, pass_len, pair), low),
            pltpu.VMEM((tp - 1, share, pass_len, pair), low),
            pltpu.VMEM(sums.shape, low),
            pltpu.VMEM((head_cols, count * pass_len), low),
            pltpu.VMEM((tp, *pieces[0].shape), low),
            pltpu.VMEM((2, ring, head_cols // 2, width), F32),
            pltpu.VMEM((ring, head_cols // 2, width), F32),
            pltpu.VMEM((ring, head_cols // 2, width), low),
            pltpu.VMEM((ring, head_cols // 2, width), low),
            pltpu.VMEM((2, width // 2, head_cols // 2), F32),
            pltpu.VMEM((width // 2, head_cols // 2), F32),
            pltpu.SemaphoreType.DMA((4 + len(pieces) + len(weights),)),
        ]
        + copy_sems(tp - 1)
        + copy_sems(2)
        + copy_sems(ring - 1),
        compiler_params=pltpu.CompilerParams(
            collective_id=ident, has_side_effects=True, vmem_limit_bytes=VMEM_LIMIT
        ),
        name="tail",
    )(sums, tokens, tokens_in, *pieces, *weights)


def first_slot(plan, d, step):
    total = jnp.zeros_like(step)
    for t, at in plan.base[d].items():
        total = total + jnp.where(step == t, at, 0)
    return total


def routes(plan, ids):
    count, slots = plan.passages, plan.slots
    me_k = lax.axis_index("st_1")
    requests = ids.shape[1]
    every = jnp.arange(ids.shape[0] * count, dtype=jnp.int32)
    owner_k, steps, fars, ranks = needs(plan.ring, count, ids)
    place = jnp.arange(2 * count, dtype=jnp.int32)
    at_home = place % count + jnp.where(place // count == me_k, 0, count)
    want = 2 * jnp.arange(count, dtype=jnp.int32) + me_k
    order, final = [], []
    for d in range(2):
        rank, far = own_chip(ranks[d]), own_chip(fars[d])
        order.append(jnp.sum(jnp.where(rank[None, :] == want[:, None], at_home[None, :], 0), axis=1))
        twin_at = plan.slots - count
        near = plan.base[d][1] - count
        aside = twin_at + d * (plan.layout[1] // 2)
        index = jnp.where(rank % 2 == me_k, near, aside) + rank // 2
        index = jnp.where(far > 0, index, twin_at + plan.layout[1])
        final.append(lax.dynamic_slice_in_dim(index, me_k * count, count))
    chip_ids = chip_requests(ids)
    chip_hot = chip_ids[:, None] == every[None, :]
    slot, core = chip_ids % count, chip_requests(owner_k)
    for d in range(2):
        rank = jnp.sum(jnp.where(chip_hot, ranks[d].reshape(-1)[None, :], 0), axis=1)
        step = chip_requests(steps[d])
        slot = jnp.where(step > 0, first_slot(plan, d, step) + rank // 2, slot)
        core = jnp.where(step > 0, rank % 2, core)
    where = slot + jnp.where(core == me_k, 0, slots)
    where = lax.dynamic_slice_in_dim(where, me_k * requests, requests)
    mine = jnp.where(core == me_k, slot, -1).reshape(2, requests)
    mine = jnp.where(me_k == 0, mine, mine[::-1]).reshape(-1)
    table = readers_table(mine, slots, 2 * requests)
    tables = (jnp.concatenate(order), where, jnp.concatenate(final))
    order, where, final = (t.astype(jnp.int32) for t in tables)
    return order, where, table, final


def local(pass_ids, store, queries, gate_pre, w_query, w_gate, w_key, w_value, d_mem):
    tp_count = lax.axis_size("tp")
    ring = lax.axis_size("st_0")
    passages, pass_len, _ = store.shape
    model_width = w_key.shape[0]
    requests = pass_ids.size
    plan = Plan(ring, passages)
    ids = jnp.zeros((8, 128), jnp.int32).at[0, :requests].set(pass_ids.reshape(-1))
    pieces = gather_store(store)
    ids = gather_ids(5, ids)
    ids = ids[:, :, 0, :requests].reshape(2 * ring, requests)
    fits, cast_table, fold_table = stream_routes(ring, passages, ids)
    fits = fits[0] > 0
    kv = keys_values(pieces, w_key, w_value)

    def cast_short(ids, table, kv, weights):
        return stream_cast(0, table, kv, weights)

    def cast_any(ids, table, kv, weights):
        order, where, _, _ = routes(plan, ids)
        return cast_rows(plan, 1, order, where, kv, weights)

    def fold_short(ids, table, grads, tokens):
        return stream_fold(2, passages, table, grads, tokens)

    def fold_any(ids, table, grads, tokens):
        _, _, table, final = routes(plan, ids)
        return fold_rows(plan, 3, table, final, grads, tokens)

    weights = (w_query, w_gate, w_key, w_value)
    request_kv, wq_far, wg_far, wk_far, wv_far = lax.cond(
        fits, cast_short, cast_any, ids, cast_table, kv, weights
    )
    request_grads, token_grads = attend(queries, gate_pre, d_mem, request_kv)
    sums, tokens_in = lax.cond(
        fits, fold_short, fold_any, ids, fold_table, request_grads, token_grads
    )
    d_tokens, d_store, d_wkey = tail(
        4,
        sums,
        token_grads,
        tokens_in,
        pieces,
        (w_query, w_gate, wq_far, wg_far, w_key, w_value, wk_far, wv_far),
    )
    return d_tokens, d_store.reshape(passages // tp_count, pass_len, model_width), d_wkey


def solution(mesh):
    finer = Mesh(
        mesh.devices.reshape(mesh.shape["grp"], -1, 2, mesh.shape["tp"]),
        ("grp", "st_0", "st_1", "tp"),
    )
    in_specs = (
        P(GRP_ST, None),
        P(ST, None, "tp"),
        P(GRP_ST, "tp"),
        P(GRP_ST, "tp"),
        P(None, "tp"),
        P(None, "tp"),
        P(None, "tp"),
        P(None, "tp"),
        P(GRP_ST, "tp"),
    )
    out_specs = (P(GRP_ST_TP, None), P(GRP_ST_TP, None, None), P(GRP_ST, "tp"))
    return jax.shard_map(local, mesh=finer, in_specs=in_specs, out_specs=out_specs, check_vma=False)
```

```python
import functools

import jax
import jax.numpy as jnp
from jax import lax
from jax.experimental import pallas as pl
from jax.experimental.pallas import tpu as pltpu
from jax.sharding import Mesh
from jax.sharding import PartitionSpec as P

HD = 256
BLK = 128
PB = 4
MOST = 2
CHUNK = 4
LENGTH = 54
STAGE = 2
LAG = 2 * STAGE
VMEM_LIMIT = 62 * 1024 * 1024
ST = ("st_0", "st_1")
GRP_ST = ("grp", "st_0", "st_1")
GRP_ST_TP = ("grp", "st_0", "st_1", "tp")
MESH_ID = pl.DeviceIdType.MESH
VMEM_SPEC = pl.BlockSpec(memory_space=pltpu.VMEM)
SMEM_SPEC = pl.BlockSpec(memory_space=pltpu.SMEM)
ANY_SPEC = pl.BlockSpec(memory_space=pl.ANY)
F32 = jnp.float32


class Plan:
    def __init__(self, ring, passages):
        self.ring = ring
        self.passages = passages
        self.reach = ring // 2
        self.steps_of = range(1, self.reach + 1)
        per_owner = 2 * MOST
        self.layout = {
            t: min(passages, per_owner * (self.reach - t + 1))
            + min(passages, per_owner * (self.reach - t))
            for t in self.steps_of
        }
        self.sizes = self.layout
        self.base = [{}, {}]
        at = passages
        for d in range(2):
            for t in self.steps_of:
                self.base[d][t] = at
                at += -(-self.layout[t] // 2)
        self.slots = at

    def half(self, t):
        return -(-self.sizes[t] // 2) if t <= self.reach else 0

    def steps(self, down=False):
        for t in reversed(self.steps_of) if down else self.steps_of:
            for first in range(0, self.half(t), CHUNK):
                for d in range(2):
                    yield d, t, first, min(CHUNK, self.half(t) - first)


class Place:
    def __init__(self):
        self.g, self.z, self.k, self.x = (lax.axis_index(a) for a in GRP_ST_TP)
        self.ring = lax.axis_size("st_0")
        self.tp = lax.axis_size("tp")
        self.twin = (self.g, self.z, 1 - self.k, self.x)

    def along_z(self, step):
        return (self.g, lax.rem(self.z + step + self.ring, self.ring), self.k, self.x)

    def along_x(self, step):
        return (self.g, self.z, self.k, lax.rem(self.x + step + self.tp, self.tp))


def greet(*devices):
    barrier = pltpu.get_barrier_semaphore()
    for device in devices:
        pl.semaphore_signal(barrier, inc=1, device_id=device, device_id_type=MESH_ID)
    pl.semaphore_wait(barrier, len(devices))


class Copies:
    def __init__(self, send_sem, recv_sem):
        self.send_sem, self.recv_sem = send_sem, recv_sem
        self.all = []

    def start(self, src, dst, device):
        n = len(self.all)
        copy = pltpu.make_async_remote_copy(
            src_ref=src,
            dst_ref=dst,
            send_sem=self.send_sem.at[n],
            recv_sem=self.recv_sem.at[n],
            device_id=device,
            device_id_type=MESH_ID,
        )
        copy.start()
        self.all.append(copy)
        return copy

    def wait_sends(self):
        for copy in self.all:
            copy.wait_send()


def copy_sems(count):
    return [pltpu.SemaphoreType.DMA((count,)), pltpu.SemaphoreType.DMA((count,))]


def ids_kernel(ids_ref, ids_out, twin_ids, *sems):
    gifts, sends = (Copies(*sems[2 * i : 2 * i + 2]) for i in range(2))
    place = Place()
    peers = [place.along_z(step) for step in range(1, place.ring)]
    greet(place.twin, *peers)
    gift = gifts.start(ids_ref, twin_ids, place.twin)
    row = lax.broadcasted_iota(jnp.int32, ids_ref.shape, 0)
    gift.wait_recv()
    ids_out[place.z] = jnp.where(row == place.k, ids_ref[...], twin_ids[...])
    part = ids_out.at[place.z]
    for peer in peers:
        sends.start(part, part, peer)
    for copy in sends.all:
        copy.wait_recv()
    for group in (gifts, sends):
        group.wait_sends()


def gather_ids(ident, ids):
    ring = lax.axis_size("st_0")
    return pl.pallas_call(
        ids_kernel,
        out_shape=jax.ShapeDtypeStruct((ring, *ids.shape), ids.dtype),
        in_specs=[VMEM_SPEC],
        out_specs=VMEM_SPEC,
        scratch_shapes=[pltpu.VMEM(ids.shape, ids.dtype)] + copy_sems(1) + copy_sems(ring - 1),
        compiler_params=pltpu.CompilerParams(
            collective_id=ident, has_side_effects=True, vmem_limit_bytes=8 * 1024 * 1024
        ),
        cost_estimate=pl.CostEstimate(flops=9 * 10**9, bytes_accessed=10**6, transcendentals=0),
        name="gather_ids",
    )(ids)


def keys_values_kernel(own_ref, ahead_ref, behind_ref, low_ref, high_ref, wk_ref, wv_ref, kv_ref):
    x, tp = lax.axis_index("tp"), lax.axis_size("tp")
    count, pass_len, depth = own_ref.shape
    rows, cols = count * pass_len, wk_ref.shape[1]
    early = pl.program_id(0) < pl.num_programs(0) // 2
    opposite = jnp.where(early, low_ref[...], high_ref[...])
    parts = (own_ref[...], ahead_ref[...], opposite, behind_ref[...])
    for c, w_ref in enumerate((wk_ref, wv_ref)):
        total = None
        for rel, part in enumerate(parts):
            at = pl.multiple_of(lax.rem(x + rel, tp) * depth, depth)
            weight = w_ref[pl.ds(at, depth), :]
            term = jnp.dot(part.reshape(rows, depth), weight, preferred_element_type=F32)
            total = term if total is None else total + term
        at = slice(c * cols, (c + 1) * cols)
        kv_ref[:, :, at] = total.reshape(count, pass_len, cols).astype(kv_ref.dtype)


def keys_values(pieces, w_key, w_value):
    count, rows, depth = pieces[0].shape
    pair = 2 * w_key.shape[1]
    steps = 4
    block = (count // steps, rows, depth)
    whole = pl.BlockSpec(block, lambda i: (i, 0, 0))
    low = pl.BlockSpec(block, lambda i: (jnp.minimum(i, steps // 2 - 1), 0, 0))
    high = pl.BlockSpec(block, lambda i: (jnp.maximum(i - steps // 2, 0), 0, 0))
    weight = pl.BlockSpec(w_key.shape, lambda i: (0, 0))
    return pl.pallas_call(
        keys_values_kernel,
        grid=(steps,),
        out_shape=jax.ShapeDtypeStruct((count, rows, pair), pieces[0].dtype),
        in_specs=[whole, whole, whole, low, high, weight, weight],
        out_specs=pl.BlockSpec((count // steps, rows, pair), lambda i: (i, 0, 0)),
        name="keys_values",
    )(*pieces, w_key, w_value)


def gather_store(store):
    tp = lax.axis_size("tp")
    half = store.shape[0] // 2
    up = [(i, (i + 1) % tp) for i in range(tp)]
    down = [(i, (i - 1) % tp) for i in range(tp)]
    behind = lax.ppermute(store, "tp", up)
    ahead = lax.ppermute(store, "tp", down)
    low = lax.ppermute(behind[:half], "tp", up)
    high = lax.ppermute(ahead[half:], "tp", down)
    return store, ahead, behind, low, high


def attend_kernel(scale, q_ref, gate_ref, mem_ref, kv_ref, grads_ref, tokens_ref):
    blocks = q_ref.shape[0] // BLK
    cols = q_ref.shape[1]
    pass_len = kv_ref.shape[1]
    low = q_ref.dtype

    def dot(a, b, ca, cb):
        return lax.dot_general(a, b, (((ca,), (cb,)), ((), ())), preferred_element_type=F32)

    for b in range(blocks):
        toks = pl.ds(b * BLK, BLK)
        kv = kv_ref[pl.ds(b * PB, PB)].reshape(PB * pass_len, 2 * cols)
        for h in range(cols // HD):
            k_at = slice(h * HD, (h + 1) * HD)
            v_at = slice(cols + h * HD, cols + (h + 1) * HD)
            q, keys, values = q_ref[toks, k_at], kv[:, k_at], kv[:, v_at]
            scores = dot(q, keys, 1, 1) * scale
            shifted = jnp.exp(scores - jnp.max(scores, axis=-1, keepdims=True))
            probs = shifted / jnp.sum(shifted, axis=-1, keepdims=True)
            probs_low = probs.astype(low)
            attended = dot(probs_low, values, 1, 0)
            gate = gate_ref[toks, k_at].astype(F32)
            mem = mem_ref[toks, k_at].astype(F32)
            sig = jax.nn.sigmoid(gate)
            attended_grad = (gate * sig * mem).astype(low)
            gate_grad = mem * attended * sig * (1.0 + gate * (1.0 - sig))
            prob_grad = dot(attended_grad, values, 1, 1)
            inner = jnp.sum(probs * prob_grad, axis=-1, keepdims=True)
            score_grad = (scale * probs * (prob_grad - inner)).astype(low)
            tokens_ref[toks, k_at] = dot(score_grad, keys, 1, 0).astype(low)
            tokens_ref[toks, v_at] = gate_grad.astype(low)
            key_grad = dot(score_grad, q, 0, 0).astype(low)
            value_grad = dot(probs_low, attended_grad, 0, 0).astype(low)
            passes = pl.ds(b * PB, PB)
            grads_ref[passes, :, k_at] = key_grad.reshape(PB, pass_len, HD)
            grads_ref[passes, :, v_at] = value_grad.reshape(PB, pass_len, HD)


def attend(queries, gate_pre, d_mem, request_kv):
    toks, cols = queries.shape
    _, pass_len, pair = request_kv.shape
    step = 2
    grid = toks // BLK // step
    tok_spec = pl.BlockSpec((step * BLK, cols), lambda i: (i, 0))
    kv_spec = pl.BlockSpec((step * PB, pass_len, pair), lambda i: (i, 0, 0))
    return pl.pallas_call(
        functools.partial(attend_kernel, HD**-0.5),
        grid=(grid,),
        out_shape=[
            jax.ShapeDtypeStruct(request_kv.shape, request_kv.dtype),
            jax.ShapeDtypeStruct((toks, pair), queries.dtype),
        ],
        in_specs=[tok_spec, tok_spec, tok_spec, kv_spec],
        out_specs=[kv_spec, pl.BlockSpec((step * BLK, pair), lambda i: (i, 0))],
        name="attend",
    )(queries, gate_pre, d_mem, request_kv)


def cast_kernel(plan, weights, order_ref, where_ref, kv_ref, *refs):
    w_refs, refs = refs[:weights], refs[weights:]
    out_ref, w_outs, refs = refs[0], refs[1 : 1 + weights], refs[1 + weights :]
    buf, first_buf, home, *sems = refs
    ring_copies, gifts, w_copies = (Copies(*sems[2 * i : 2 * i + 2]) for i in range(3))
    place = Place()
    count, slots = plan.passages, plan.slots
    top = plan.half(1)

    greet(place.along_z(1), place.along_z(-1), place.along_x(1), place.along_x(-1), place.twin)
    own_gift = gifts.start(kv_ref, home.at[pl.ds(count, count)], place.twin)

    @pl.loop(0, count)
    def _(j):
        home[j] = kv_ref[j]
        buf[j] = kv_ref[j]

    own_gift.wait_recv()

    @pl.loop(0, top)
    def _(j):
        for d in range(2):
            first_buf[d * top + j] = home[order_ref[d * count + j]]

    copies = {}
    steps = list(plan.steps())
    extent = {(d, t, first): size for d, t, first, size in steps}

    def send(d, t, first):
        size = extent[d, t, first]
        if t == 1:
            src = first_buf.at[pl.ds(d * top + first, size)]
        else:
            src = buf.at[pl.ds(plan.base[d][t - 1] + first, size)]
        dst = buf.at[pl.ds(plan.base[d][t] + first, size)]
        copies[d, t, first] = ring_copies.start(src, dst, place.along_z(1 - 2 * d))

    for d, t, first, _ in steps:
        if t == 1:
            send(d, t, first)
    rows = w_refs[0].shape[0] // 2
    half = pl.ds(place.k * rows, rows)
    arrive = [[], []]
    for w_ref, w_out in zip(w_refs, w_outs):
        arrive[0].append(
            w_copies.start(w_ref.at[half], w_out.at[2, half], place.along_x(1))
        )
        arrive[1].append(
            w_copies.start(w_ref.at[half], w_out.at[0, half], place.along_x(-1))
        )
    w_gifts = []
    middle = []

    def forward_weights():
        for copy in arrive[0] + arrive[1]:
            copy.wait_recv()
        for w_out in w_outs:
            middle.append(
                w_copies.start(
                    w_out.at[2 * place.k, half],
                    w_out.at[1, half],
                    place.along_x(2 * place.k - 1),
                )
            )
            for rel in (0, 2):
                part = w_out.at[rel, half]
                w_gifts.append(w_copies.start(part, part, place.twin))

    last = None
    for d, t, first, size in steps:
        if t != last and t == plan.reach // 2 + 1:
            forward_weights()
        last = t
        copies[d, t, first].wait_recv()
        if (d, t + 1, first) in extent:
            send(d, t + 1, first)
        at = plan.base[d][t] + first
        gifts.start(buf.at[pl.ds(at, size)], buf.at[pl.ds(slots + at, size)], place.twin)
    for copy, w_out in zip(middle, w_outs):
        copy.wait_recv()
        part = w_out.at[1, half]
        w_gifts.append(w_copies.start(part, part, place.twin))
    for gift in gifts.all[1:]:
        gift.wait_recv()

    @pl.loop(0, count)
    def _(j):
        buf[slots + j] = home[count + j]

    @pl.loop(0, out_ref.shape[0])
    def _(r):
        out_ref[r] = buf[where_ref[r]]

    for gift in w_gifts:
        gift.wait_recv()
    for group in (gifts, ring_copies, w_copies):
        group.wait_sends()


def cast_rows(plan, ident, order, where, kv, weights):
    count, rows, cols = kv.shape
    steps = len(list(plan.steps()))
    others = lax.axis_size("tp") - 1
    return pl.pallas_call(
        functools.partial(cast_kernel, plan, len(weights)),
        out_shape=[jax.ShapeDtypeStruct((where.shape[0], rows, cols), kv.dtype)]
        + [jax.ShapeDtypeStruct((others, *w.shape), w.dtype) for w in weights],
        in_specs=[SMEM_SPEC, SMEM_SPEC, VMEM_SPEC] + [ANY_SPEC] * len(weights),
        out_specs=[VMEM_SPEC] + [ANY_SPEC] * len(weights),
        scratch_shapes=[
            pltpu.VMEM((2 * plan.slots, rows, cols), kv.dtype),
            pltpu.VMEM((2 * plan.half(1), rows, cols), kv.dtype),
            pltpu.VMEM((2 * count, rows, cols), kv.dtype),
        ]
        + copy_sems(steps)
        + copy_sems(steps + 1)
        + copy_sems(6 * len(weights)),
        compiler_params=pltpu.CompilerParams(
            collective_id=ident, has_side_effects=True, vmem_limit_bytes=VMEM_LIMIT
        ),
        name="cast_rows",
    )(order, where, kv, *weights)


def fold_kernel(
    plan,
    table_ref,
    final_ref,
    grads_ref,
    tokens_ref,
    out_ref,
    tokens_out,
    held,
    here,
    sums,
    load_sem,
    *sems,
):
    ring_copies, gifts, exchange = (Copies(*sems[2 * i : 2 * i + 2]) for i in range(3))
    place = Place()
    count, top = plan.passages, plan.half(1)
    own = grads_ref.shape[0]
    readers = 2 * MOST
    twin_at = plan.slots - count
    zero_at = twin_at + plan.layout[1]
    peers = [place.along_x(rel) for rel in range(1, place.tp)]

    load = pltpu.make_async_copy(grads_ref, held.at[pl.ds(0, own)], load_sem)
    load.start()
    held[2 * own] = jnp.zeros_like(held[2 * own])
    here[zero_at] = jnp.zeros_like(here[zero_at])
    greet(place.along_z(1), place.along_z(-1), place.twin, *peers)
    own_gift = gifts.start(grads_ref, held.at[pl.ds(own, own)], place.twin)
    block = tokens_out.shape[1]
    for rel, peer in enumerate(peers, 1):
        exchange.start(
            tokens_ref.at[pl.ds(peer[3] * block, block)],
            tokens_out.at[place.tp - 1 - rel],
            peer,
        )
    load.wait()
    own_gift.wait_recv()

    def readers_sum(slot):
        total = held[table_ref[slot * readers]].astype(F32)
        for q in range(1, readers):
            total += held[table_ref[slot * readers + q]].astype(F32)
        return total

    copies = {}
    steps = list(plan.steps(down=True))
    extent = {(d, t, first): size for d, t, first, size in steps}
    for d, t, first, size in steps:
        at = plan.base[d][t] + first
        begin = extent.get((d, t + 1, first), 0)
        if begin:
            copies[d, t + 1, first].wait_recv()
            far_at = plan.base[d][t + 1] + first

            @pl.loop(0, begin)
            def _(j):
                total = readers_sum(at + j) + here[far_at - count + j].astype(F32)
                sums[at - count + j] = total.astype(sums.dtype)

        if begin < size:

            @pl.loop(begin, size)
            def _(j):
                sums[at - count + j] = readers_sum(at + j).astype(sums.dtype)

        part = pl.ds(at - count, size)
        copies[d, t, first] = ring_copies.start(
            sums.at[part], here.at[part], place.along_z(2 * d - 1)
        )
    for d, t, first, size in steps:
        if t == 1:
            copies[d, t, first].wait_recv()
            src = here.at[pl.ds(plan.base[d][1] - count + first, size)]
            dst = here.at[pl.ds(twin_at + d * (plan.layout[1] // 2) + first, size)]
            gifts.start(src, dst, place.twin)
    for gift in gifts.all[1:]:
        gift.wait_recv()

    @pl.loop(0, count)
    def _(p):
        total = readers_sum(p)
        for d in range(2):
            total += here[final_ref[d * count + p]].astype(F32)
        out_ref[p] = total.astype(out_ref.dtype)

    for copy in exchange.all:
        copy.wait_recv()
    for group in (gifts, ring_copies, exchange):
        group.wait_sends()


def fold_rows(plan, ident, table, final, grads, tokens):
    own, rows, cols = grads.shape
    steps = list(plan.steps())
    ends = sum(1 for _, t, _, _ in steps if t == 1)
    count = plan.passages
    tp = lax.axis_size("tp")
    return pl.pallas_call(
        functools.partial(fold_kernel, plan),
        out_shape=[
            jax.ShapeDtypeStruct((count, rows, cols), grads.dtype),
            jax.ShapeDtypeStruct((tp - 1, tokens.shape[0] // tp, tokens.shape[1]), tokens.dtype),
        ],
        in_specs=[SMEM_SPEC, SMEM_SPEC, ANY_SPEC, ANY_SPEC],
        out_specs=[VMEM_SPEC, ANY_SPEC],
        scratch_shapes=[
            pltpu.VMEM((2 * own + 1, rows, cols), grads.dtype),
            pltpu.VMEM((plan.slots - count + plan.layout[1] + 1, rows, cols), grads.dtype),
            pltpu.VMEM((plan.slots - count, rows, cols), grads.dtype),
            pltpu.SemaphoreType.DMA,
        ]
        + copy_sems(len(steps))
        + copy_sems(1 + ends)
        + copy_sems(tp - 1),
        compiler_params=pltpu.CompilerParams(
            collective_id=ident, has_side_effects=True, vmem_limit_bytes=VMEM_LIMIT
        ),
        name="fold_rows",
    )(table, final, grads, tokens)


def copy_slots(src, src_at, dst, dst_at, size):
    @pl.loop(0, size)
    def _(j):
        dst[dst_at + j] = src[src_at + j]


class WeightShare:
    def __init__(self, place, copies, w_refs, w_outs):
        self.place, self.copies, self.outs = place, copies, w_outs
        rows = w_refs[0].shape[0] // 2
        self.half = pl.ds(place.k * rows, rows)
        self.near, self.middle, self.gifts = [], [], []
        for w_ref, w_out in zip(w_refs, w_outs):
            for slot, step in ((2, 1), (0, -1)):
                src, dst = w_ref.at[self.half], w_out.at[slot, self.half]
                self.near.append(copies.start(src, dst, place.along_x(step)))

    def forward(self, n):
        for copy in self.near[2 * n : 2 * n + 2]:
            copy.wait_recv()
        w_out = self.outs[n]
        src = w_out.at[2 * self.place.k, self.half]
        dst = w_out.at[1, self.half]
        device = self.place.along_x(2 * self.place.k - 1)
        self.middle.append(self.copies.start(src, dst, device))
        for slot in (0, 2):
            self.give(w_out.at[slot, self.half])

    def give(self, part):
        self.gifts.append(self.copies.start(part, part, self.place.twin))

    def finish(self):
        for copy, w_out in zip(self.middle, self.outs):
            copy.wait_recv()
            self.give(w_out.at[1, self.half])

    def wait(self):
        for gift in self.gifts:
            gift.wait_recv()


def stream_cast_kernel(weights, table_ref, kv_ref, *refs):
    w_refs, refs = refs[:weights], refs[weights:]
    out_ref, w_outs, refs = refs[0], refs[1 : 1 + weights], refs[1 + weights :]
    kept, land, twin_land, leave, *sems = refs
    ring_copies, gifts, w_copies = (Copies(*sems[2 * i : 2 * i + 2]) for i in range(3))
    place = Place()
    count = kv_ref.shape[0]
    length = land.shape[0] // 2
    stages = length // STAGE
    home = 2 * count

    greet(place.along_z(1), place.along_z(-1), place.along_x(1), place.along_x(-1), place.twin)
    own_gift = gifts.start(kv_ref, kept.at[pl.ds(count, count)], place.twin)

    @pl.loop(0, count)
    def _(j):
        kept[j] = kv_ref[j]

    own_gift.wait_recv()
    sends, given = {}, {}
    share = None
    for i in range(stages + 4):
        for d in range(2):
            if 0 <= i - 2 < stages:
                at = d * length + (i - 2) * STAGE
                sends[d, i - 2].wait_recv()
                part = pl.ds(at, STAGE)
                given[d, i - 2] = gifts.start(land.at[part], twin_land.at[part], place.twin)
                copy_slots(land, at, kept, home + at, STAGE)
            if i < stages:
                at = d * length + i * STAGE

                @pl.loop(at, at + STAGE)
                def _(q):
                    leave[q] = kept[table_ref[q]]

            if 0 <= i - 4 < stages:
                at = d * length + (i - 4) * STAGE
                given[d, i - 4].wait_recv()
                copy_slots(twin_land, at, kept, home + 2 * length + at, STAGE)
        if i < stages:
            for d in range(2):
                part = pl.ds(d * length + i * STAGE, STAGE)
                sends[d, i] = ring_copies.start(
                    leave.at[part], land.at[part], place.along_z(1 - 2 * d)
                )
        if i == 1:
            share = WeightShare(place, w_copies, w_refs, w_outs)
        if i in (6, 10, 14, 18):
            share.forward((i - 6) // 4)
    share.finish()

    @pl.loop(0, out_ref.shape[0])
    def _(r):
        out_ref[r] = kept[table_ref[2 * length + r]]

    share.wait()
    for group in (gifts, ring_copies, w_copies):
        group.wait_sends()


def stream_cast(ident, table, kv, weights):
    count, rows, cols = kv.shape
    stages = LENGTH // STAGE
    others = lax.axis_size("tp") - 1
    return pl.pallas_call(
        functools.partial(stream_cast_kernel, len(weights)),
        out_shape=[jax.ShapeDtypeStruct((table.shape[0] - 2 * LENGTH, rows, cols), kv.dtype)]
        + [jax.ShapeDtypeStruct((others, *w.shape), w.dtype) for w in weights],
        in_specs=[SMEM_SPEC, VMEM_SPEC] + [ANY_SPEC] * len(weights),
        out_specs=[VMEM_SPEC] + [ANY_SPEC] * len(weights),
        scratch_shapes=[
            pltpu.VMEM((2 * count + 4 * LENGTH, rows, cols), kv.dtype),
            pltpu.VMEM((2 * LENGTH, rows, cols), kv.dtype),
            pltpu.VMEM((2 * LENGTH, rows, cols), kv.dtype),
            pltpu.VMEM((2 * LENGTH, rows, cols), kv.dtype),
        ]
        + copy_sems(2 * stages)
        + copy_sems(2 * stages + 1)
        + copy_sems(6 * len(weights)),
        compiler_params=pltpu.CompilerParams(
            collective_id=ident, has_side_effects=True, vmem_limit_bytes=VMEM_LIMIT
        ),
        name="stream_cast",
    )(table, kv, *weights)


def stream_fold_kernel(
    table_ref, grads_ref, tokens_ref, out_ref, tokens_out, held, kept, land,
    leave, twin_land, load_sem, *sems
):
    ring_copies, gifts, exchange = (Copies(*sems[2 * i : 2 * i + 2]) for i in range(3))
    place = Place()
    count = out_ref.shape[0]
    length = land.shape[0] // 2
    stages = length // STAGE
    own = grads_ref.shape[0]
    readers = 2 * MOST
    zero = 2 * length
    onward_at = (count + 2 * length + 1) * readers
    final_at = onward_at + 2 * length
    peers = [place.along_x(rel) for rel in range(1, place.tp)]

    load = pltpu.make_async_copy(grads_ref, held.at[pl.ds(0, own)], load_sem)
    load.start()
    blank = jnp.zeros_like(held[0])
    held[2 * own] = blank
    kept[zero] = blank
    twin_land[2 * count] = blank
    greet(place.along_z(1), place.along_z(-1), place.twin, *peers)
    own_gift = gifts.start(grads_ref, held.at[pl.ds(own, own)], place.twin)
    block = tokens_out.shape[1]
    for rel, peer in enumerate(peers, 1):
        exchange.start(
            tokens_ref.at[pl.ds(peer[3] * block, block)],
            tokens_out.at[place.tp - 1 - rel],
            peer,
        )
    load.wait()
    own_gift.wait_recv()

    def readers_sum(slot):
        total = held[table_ref[slot * readers]].astype(F32)
        for q in range(1, readers):
            total += held[table_ref[slot * readers + q]].astype(F32)
        return total

    sends = {}

    def arrive(i):
        for d in range(2):
            at = d * length + i * STAGE
            sends[d, i].wait_recv()
            if i * STAGE < count:
                src = land.at[pl.ds(at, STAGE)]
                dst = twin_land.at[pl.ds(d * count + i * STAGE, STAGE)]
                gifts.start(src, dst, place.twin)
            copy_slots(land, at, kept, at, STAGE)

    for i in reversed(range(stages)):
        if i + 2 < stages:
            arrive(i + 2)
        for d in range(2):
            at = d * length + i * STAGE

            @pl.loop(at, at + STAGE)
            def _(q):
                total = readers_sum(count + q) + kept[table_ref[onward_at + q]].astype(F32)
                leave[q] = total.astype(leave.dtype)

        for d in range(2):
            part = pl.ds(d * length + i * STAGE, STAGE)
            sends[d, i] = ring_copies.start(
                leave.at[part], land.at[part], place.along_z(2 * d - 1)
            )
    arrive(1)
    arrive(0)
    for gift in gifts.all[1:]:
        gift.wait_recv()

    @pl.loop(0, count)
    def _(p):
        total = readers_sum(p)
        for d in range(2):
            total += kept[table_ref[final_at + d * count + p]].astype(F32)
            total += twin_land[table_ref[final_at + (2 + d) * count + p]].astype(F32)
        out_ref[p] = total.astype(out_ref.dtype)

    for copy in exchange.all:
        copy.wait_recv()
    for group in (gifts, ring_copies, exchange):
        group.wait_sends()


def stream_fold(ident, count, table, grads, tokens):
    own, rows, cols = grads.shape
    stages = LENGTH // STAGE
    tp = lax.axis_size("tp")
    return pl.pallas_call(
        stream_fold_kernel,
        out_shape=[
            jax.ShapeDtypeStruct((count, rows, cols), grads.dtype),
            jax.ShapeDtypeStruct((tp - 1, tokens.shape[0] // tp, tokens.shape[1]), tokens.dtype),
        ],
        in_specs=[SMEM_SPEC, ANY_SPEC, ANY_SPEC],
        out_specs=[VMEM_SPEC, ANY_SPEC],
        scratch_shapes=[
            pltpu.VMEM((2 * own + 1, rows, cols), grads.dtype),
            pltpu.VMEM((2 * LENGTH + 1, rows, cols), grads.dtype),
            pltpu.VMEM((2 * LENGTH, rows, cols), grads.dtype),
            pltpu.VMEM((2 * LENGTH, rows, cols), grads.dtype),
            pltpu.VMEM((2 * count + 1, rows, cols), grads.dtype),
            pltpu.SemaphoreType.DMA,
        ]
        + copy_sems(2 * stages)
        + copy_sems(1 + 2 * (-(-count // STAGE)))
        + copy_sems(tp - 1),
        compiler_params=pltpu.CompilerParams(
            collective_id=ident, has_side_effects=True, vmem_limit_bytes=VMEM_LIMIT
        ),
        name="stream_fold",
    )(table, grads, tokens)


def readers_table(slot, slots, requests):
    at_slot = slot[:, None] == jnp.arange(slots, dtype=jnp.int32)[None, :]
    turn = jnp.cumsum(at_slot.astype(jnp.int32), axis=0)
    number = jnp.arange(requests, dtype=jnp.int32)[:, None]
    columns = [
        jnp.min(jnp.where(at_slot & (turn == q + 1), number, requests), axis=0)
        for q in range(2 * MOST)
    ]
    return jnp.stack(columns, axis=1).reshape(-1).astype(jnp.int32)


def needs(ring, count, ids):
    devices = ids.shape[0]
    pair = 2 * count
    every = jnp.arange(devices * count, dtype=jnp.int32)
    owner = ids // count
    owner_z, owner_k = owner // 2, owner % 2
    reader_z = (jnp.arange(devices, dtype=jnp.int32) // 2)[:, None]
    away = jnp.mod(reader_z - owner_z, ring)
    up = (2 * away < ring) | ((2 * away == ring) & (owner_k == 0))
    steps = (jnp.where(up, away, 0), jnp.where(up, 0, ring - away))
    hot = ids.reshape(-1)[:, None] == every[None, :]
    place = jnp.arange(pair, dtype=jnp.int32)
    ranks, fars = [], []
    for d in range(2):
        far = jnp.max(jnp.where(hot, steps[d].reshape(-1)[:, None], 0), axis=0)
        far = far.reshape(ring, pair)
        before = (far[:, None, :] > far[:, :, None]) | (
            (far[:, None, :] == far[:, :, None]) & (place[None, None, :] < place[None, :, None])
        )
        ranks.append(jnp.sum(before.astype(jnp.int32), axis=2))
        fars.append(far)
    return owner_k, steps, fars, ranks


def own_chip(array):
    return lax.dynamic_slice_in_dim(array, lax.axis_index("st_0"), 1, axis=0)[0]


def chip_requests(array):
    return lax.dynamic_slice_in_dim(array, 2 * lax.axis_index("st_0"), 2, axis=0).reshape(-1)


def routes_kernel(count, requests, size_ref, info_ref, fits_ref, cast_ref, fold_ref, starts, start, size, used, sem):
    z, k = lax.axis_index("st_0"), lax.axis_index("st_1")
    ring = lax.axis_size("st_0")
    reach = ring // 2
    pair = 2 * count
    twin_at = 2 * LENGTH
    lane = lax.broadcasted_iota(jnp.int32, starts.shape, 1)
    lanes = starts.shape[1]
    spot = lane % ring
    up = lane < 2 * ring
    now = jnp.zeros(starts.shape, jnp.int32)
    most = jnp.zeros(starts.shape, jnp.int32)
    for t in range(reach):
        if t > 0:
            ends = now + jnp.broadcast_to(size_ref[t - 1 : t, :], starts.shape)
            after = jnp.where(
                spot == ring - 1, pltpu.roll(ends, ring - 1, 1), pltpu.roll(ends, lanes - 1, 1)
            )
            before = jnp.where(
                spot == 0, pltpu.roll(ends, lanes - ring + 1, 1), pltpu.roll(ends, 1, 1)
            )
            now = jnp.maximum(jnp.where(up, after, before), now + LAG)
        starts[t : t + 1, :] = now[0:1, :]
        here = now + jnp.broadcast_to(size_ref[t : t + 1, :], starts.shape)
        most = jnp.maximum(most, jnp.where(lane < 4 * ring, here, 0))
    fits_ref[0] = (jnp.max(most) <= LENGTH).astype(jnp.int32)
    for n, (src, dst) in enumerate(((starts, start), (size_ref, size))):
        copy = pltpu.make_async_copy(src, dst, sem.at[n])
        copy.start()
        copy.wait()

    slots = count + 2 * LENGTH
    readers = 2 * MOST
    onward_at, final_at = (slots + 1) * readers, (slots + 1) * readers + 2 * LENGTH

    @pl.loop(0, slots + 1)
    def _(i):
        used[i] = 0
        for q in range(readers):
            fold_ref[i * readers + q] = 2 * requests

    @pl.loop(0, LENGTH)
    def _(i):
        for q in range(2):
            fold_ref[onward_at + 2 * i + q] = 2 * LENGTH
            cast_ref[2 * i + q] = 0

    def info(row, i):
        return info_ref[row * 2 * requests + i]

    def column(d, core, step):
        source = lax.rem(z - (1 - 2 * d) * step + 2 * ring, ring)
        return (2 * d + core) * ring + source

    last = LENGTH - 1
    for d in range(2):

        @pl.loop(0, pair)
        def _(p):
            rank = info(5, d * pair + p)
            far = info(6, d * pair + p)
            core = lax.div(p, count)
            mine = rank % 2 == k
            home = p % count + jnp.where(core == k, 0, count)

            @pl.when(mine)
            def _():
                cast_ref[d * LENGTH + rank // 2] = home

            @pl.when(core == k)
            def _():
                i = p % count
                near = jnp.where((far > 0) & mine, d * LENGTH + rank // 2, 2 * LENGTH)
                aside = jnp.where((far > 0) & (rank % 2 != k), d * count + rank // 2, 2 * count)
                fold_ref[final_at + d * count + i] = near
                fold_ref[final_at + (2 + d) * count + i] = aside

        for t in range(1, reach):
            lane_of = column(d, k, t)
            at_out, at_in = start[t, lane_of], start[t - 1, lane_of]

            @pl.loop(0, size[t, lane_of])
            def _(r):
                out = d * LENGTH + jnp.minimum(at_out + r, last)
                come = d * LENGTH + jnp.minimum(at_in + r, last)
                cast_ref[out] = pair + come
                fold_ref[onward_at + come] = out

    @pl.loop(0, 2 * requests)
    def _(i):
        c = lax.rem(i + k * requests, 2 * requests)
        step, way, rank, within, owner = (info(row, c) for row in range(5))
        core = jnp.where(step > 0, rank % 2, owner)
        lane_of = column(way, core, step)
        at = start[jnp.maximum(step - 1, 0), lane_of] + lax.div(rank, 2)
        at = way * LENGTH + jnp.minimum(at, last)
        where = pair + at + jnp.where(core == k, 0, twin_at)
        where = jnp.where(step > 0, where, within + jnp.where(core == k, 0, count))
        slot = jnp.where(core == k, jnp.where(step > 0, count + at, within), slots)
        turn = jnp.where(slot == slots, 0, jnp.minimum(used[slot], readers - 1))
        used[slot] = turn + 1
        fold_ref[slot * readers + turn] = i

        @pl.when(i < requests)
        def _():
            cast_ref[2 * LENGTH + i] = where


def stream_routes(ring, count, ids):
    devices, requests = ids.shape
    pair = 2 * count
    reach = ring // 2
    owner_k, steps, fars, ranks = needs(ring, count, ids)
    dist = jnp.arange(1, reach + 1, dtype=jnp.int32)
    core = jnp.arange(2, dtype=jnp.int32)
    far = jnp.stack(fars)
    whole = jnp.sum((far[None] >= dist[:, None, None, None]).astype(jnp.int32), axis=3)
    size = (whole[:, :, None, :] + 1 - core[None, None, :, None]) // 2
    size = jnp.pad(size.reshape(reach, 4 * ring), ((0, 0), (0, 128 - 4 * ring)))
    chip_ids = chip_requests(ids)
    every = jnp.arange(devices * count, dtype=jnp.int32)
    chip_hot = chip_ids[:, None] == every[None, :]
    step = [chip_requests(s) for s in steps]
    way = (step[1] > 0).astype(jnp.int32)
    ranked = [jnp.sum(jnp.where(chip_hot, r.reshape(-1)[None, :], 0), axis=1) for r in ranks]
    info = jnp.concatenate(
        [
            step[0] + step[1],
            way,
            jnp.where(way == 0, ranked[0], ranked[1]),
            chip_ids % count,
            chip_requests(owner_k),
            own_chip(ranks[0]),
            own_chip(ranks[1]),
            own_chip(fars[0]),
            own_chip(fars[1]),
        ]
    ).astype(jnp.int32)
    slots = count + 2 * LENGTH
    fold_size = (slots + 1) * 2 * MOST + 2 * LENGTH + 4 * count
    return pl.pallas_call(
        functools.partial(routes_kernel, count, requests),
        out_shape=[
            jax.ShapeDtypeStruct((1,), jnp.int32),
            jax.ShapeDtypeStruct((2 * LENGTH + requests,), jnp.int32),
            jax.ShapeDtypeStruct((fold_size,), jnp.int32),
        ],
        in_specs=[VMEM_SPEC, SMEM_SPEC],
        out_specs=[SMEM_SPEC] * 3,
        scratch_shapes=[
            pltpu.VMEM((reach, 128), jnp.int32),
            pltpu.SMEM((reach, 128), jnp.int32),
            pltpu.SMEM((reach, 128), jnp.int32),
            pltpu.SMEM((slots + 1,), jnp.int32),
            pltpu.SemaphoreType.DMA((2,)),
        ],
        cost_estimate=pl.CostEstimate(flops=6 * 10**9, bytes_accessed=10**5, transcendentals=0),
        name="routes",
    )(size, info)


def project(rows_list, weight_list, out_ref, n, tile):
    cols = pl.ds(n * tile, tile)
    total = None
    for rows, weight in zip(rows_list, weight_list):
        term = lax.dot_general(
            rows[...], weight[cols, :], (((1,), (1,)), ((), ())), preferred_element_type=F32
        )
        total = term if total is None else total + term
    out_ref[:, cols] = total.astype(out_ref.dtype)


def tail_kernel(sums_ref, tokens_ref, tokens_in, *refs):
    pieces, refs = refs[:5], refs[5:]
    weights, refs = refs[:8], refs[8:]
    d_tokens_ref, d_store_ref, d_wkey_ref = refs[:3]
    wbuf_t, wbuf_s, own_t, in_t, own_s, in_s, refs = *refs[3:9], refs[9:]
    keys, keys_turned, all_buf, terms, twin_terms, sent, come, last, last_in, refs = *refs[:9], refs[9:]
    load_sem, *sems = refs
    exchange, gifts, ring_copies = (Copies(*sems[2 * i : 2 * i + 2]) for i in range(3))
    place = Place()
    tp, ring = place.tp, place.ring
    reach = ring // 2
    peers = [place.along_x(rel) for rel in range(1, tp)]
    loads = []

    def load(src, dst):
        copy = pltpu.make_async_copy(src, dst, load_sem.at[len(loads)])
        copy.start()
        loads.append(copy)

    load(sums_ref, keys)
    own_piece, ahead, behind, low, high = pieces
    part = low.shape[0]
    load(own_piece, all_buf.at[0])
    load(ahead, all_buf.at[1])
    load(behind, all_buf.at[tp - 1])
    load(low, all_buf.at[2, pl.ds(0, part)])
    load(high, all_buf.at[2, pl.ds(part, part)])
    greet(place.twin, place.along_z(1), place.along_z(-1), *peers)
    share = sums_ref.shape[0] // tp
    for rel, peer in enumerate(peers, 1):
        exchange.start(
            sums_ref.at[pl.ds(peer[3] * share, share)], in_s.at[tp - 1 - rel], peer
        )
    block = own_t.shape[0]
    load(tokens_ref.at[pl.ds(place.x * block, block)], own_t)
    load(tokens_in, in_t)
    load(sums_ref.at[pl.ds(place.x * share, share)], own_s)
    for wbuf, (wa, wb, wa_far, wb_far) in ((wbuf_t, weights[:4]), (wbuf_s, weights[4:])):
        load(wa, wbuf.at[0])
        load(wb, wbuf.at[1])
        load(wa_far, wbuf.at[pl.ds(2, tp - 1)])
        load(wb_far, wbuf.at[pl.ds(2 + tp - 1, tp - 1)])
    count, pass_len, pair = sums_ref.shape
    rows, cols = count * pass_len, pair // 2
    depth = own_piece.shape[2]
    width = terms.shape[3]
    loads[0].wait()
    keys_turned[...] = keys[:, :, :cols].reshape(rows, cols).T
    chips = depth // width
    for rel in range(tp):
        for copy in [loads[1:2], loads[2:3], loads[4:6], loads[3:4]][rel]:
            copy.wait()
        n = lax.rem(place.x + rel, tp)
        term = jnp.dot(
            keys_turned[...], all_buf[rel].reshape(rows, depth), preferred_element_type=F32
        )
        for c in range(chips):
            for h in range(2):
                terms[h, n * chips + c] = term[
                    h * (cols // 2) : (h + 1) * (cols // 2), c * width : (c + 1) * width
                ]
        part = pl.ds(n * chips, chips)
        gifts.start(terms.at[1 - place.k, part], twin_terms.at[part], place.twin)

    def operands(own, far_rows, wbuf):
        n_cols = own.shape[-1] // 2
        rows_list, weight_list = [], []
        for c in range(2):
            rows_list.append(own.at[:, pl.ds(c * n_cols, n_cols)])
            weight_list.append(wbuf.at[c])
        for rel in range(tp - 1):
            for c in range(2):
                rows_list.append(far_rows.at[rel, :, pl.ds(c * n_cols, n_cols)])
                weight_list.append(wbuf.at[2 + c * (tp - 1) + rel])
        return rows_list, weight_list

    part_rows = share * pass_len
    tile = 512
    tiles = d_tokens_ref.shape[1] // tile
    for_tokens = operands(own_t, in_t, wbuf_t)
    for_store = operands(
        own_s.reshape(part_rows, pair), in_s.reshape(tp - 1, part_rows, pair), wbuf_s
    )
    for gift in gifts.all:
        gift.wait_recv()
    hops = {}

    def mine(dest):
        return terms[place.k, dest] + twin_terms[dest]

    done = 0
    for s in range(1, reach + 1):
        for d in range(2):
            to_go = reach - d + 1 - s
            if to_go < 1:
                continue
            turn = 1 - 2 * d
            total = mine(lax.rem(place.z + turn * to_go + ring, ring))
            n = d * reach + s - 1
            if s > 1:
                hops[d, s - 1].wait_recv()
                total += come[n - 1].astype(F32)
            sent[n] = total.astype(sent.dtype)
            hops[d, s] = ring_copies.start(sent.at[n], come.at[n], place.along_z(turn))
        if s == 1:
            for copy in loads[6:]:
                copy.wait()
        if s == reach // 2:
            for copy in exchange.all:
                copy.wait_recv()
        if s <= reach // 2:
            for _ in range(-(-tiles // (reach // 2))):
                if done < tiles:
                    project(*for_tokens, d_tokens_ref, done, tile)
                    done += 1
        elif s < reach:
            for _ in range(-(-tiles // (reach // 2 - 1))):
                if done < 2 * tiles:
                    project(*for_store, d_store_ref, done - tiles, tile)
                    done += 1
    total = mine(place.z)
    for d in range(2):
        hops[d, reach - d].wait_recv()
        total += come[d * reach + reach - d - 1].astype(F32)
    turned = total.T
    out_rows = turned.shape[0] // 2
    for c in range(2):
        last[c] = turned[c * out_rows : (c + 1) * out_rows]
    end = gifts.start(last.at[1 - place.k], last_in, place.twin)
    half = cols // 2
    d_wkey_ref[:, pl.ds(pl.multiple_of(place.k * half, half), half)] = last[place.k]
    end.wait_recv()
    d_wkey_ref[:, pl.ds(pl.multiple_of((1 - place.k) * half, half), half)] = last_in[...]
    for group in (exchange, gifts, ring_copies):
        group.wait_sends()


def tail(ident, sums, tokens, tokens_in, pieces, weights):
    tp, ring = lax.axis_size("tp"), lax.axis_size("st_0")
    model, head_cols = weights[0].shape
    count, pass_len, pair = sums.shape
    share = count // tp
    width = model // ring
    low = sums.dtype
    return pl.pallas_call(
        tail_kernel,
        out_shape=[
            jax.ShapeDtypeStruct((tokens.shape[0] // tp, model), low),
            jax.ShapeDtypeStruct((share * pass_len, model), low),
            jax.ShapeDtypeStruct((width // 2, head_cols), F32),
        ],
        in_specs=[ANY_SPEC] * (3 + len(pieces) + len(weights)),
        out_specs=[VMEM_SPEC] * 3,
        scratch_shapes=[
            pltpu.VMEM((2 * tp, model, head_cols), low),
            pltpu.VMEM((2 * tp, model, head_cols), low),
            pltpu.VMEM((tokens.shape[0] // tp, tokens.shape[1]), low),
            pltpu.VMEM(tokens_in.shape, low),
            pltpu.VMEM((share, pass_len, pair), low),
            pltpu.VMEM((tp - 1, share, pass_len, pair), low),
            pltpu.VMEM(sums.shape, low),
            pltpu.VMEM((head_cols, count * pass_len), low),
            pltpu.VMEM((tp, *pieces[0].shape), low),
            pltpu.VMEM((2, ring, head_cols // 2, width), F32),
            pltpu.VMEM((ring, head_cols // 2, width), F32),
            pltpu.VMEM((ring, head_cols // 2, width), low),
            pltpu.VMEM((ring, head_cols // 2, width), low),
            pltpu.VMEM((2, width // 2, head_cols // 2), F32),
            pltpu.VMEM((width // 2, head_cols // 2), F32),
            pltpu.SemaphoreType.DMA((4 + len(pieces) + len(weights),)),
        ]
        + copy_sems(tp - 1)
        + copy_sems(tp + 1)
        + copy_sems(ring - 1),
        compiler_params=pltpu.CompilerParams(
            collective_id=ident, has_side_effects=True, vmem_limit_bytes=VMEM_LIMIT
        ),
        name="tail",
    )(sums, tokens, tokens_in, *pieces, *weights)


def first_slot(plan, d, step):
    total = jnp.zeros_like(step)
    for t, at in plan.base[d].items():
        total = total + jnp.where(step == t, at, 0)
    return total


def routes(plan, ids):
    count, slots = plan.passages, plan.slots
    me_k = lax.axis_index("st_1")
    requests = ids.shape[1]
    every = jnp.arange(ids.shape[0] * count, dtype=jnp.int32)
    owner_k, steps, fars, ranks = needs(plan.ring, count, ids)
    place = jnp.arange(2 * count, dtype=jnp.int32)
    at_home = place % count + jnp.where(place // count == me_k, 0, count)
    want = 2 * jnp.arange(count, dtype=jnp.int32) + me_k
    order, final = [], []
    for d in range(2):
        rank, far = own_chip(ranks[d]), own_chip(fars[d])
        order.append(jnp.sum(jnp.where(rank[None, :] == want[:, None], at_home[None, :], 0), axis=1))
        twin_at = plan.slots - count
        near = plan.base[d][1] - count
        aside = twin_at + d * (plan.layout[1] // 2)
        index = jnp.where(rank % 2 == me_k, near, aside) + rank // 2
        index = jnp.where(far > 0, index, twin_at + plan.layout[1])
        final.append(lax.dynamic_slice_in_dim(index, me_k * count, count))
    chip_ids = chip_requests(ids)
    chip_hot = chip_ids[:, None] == every[None, :]
    slot, core = chip_ids % count, chip_requests(owner_k)
    for d in range(2):
        rank = jnp.sum(jnp.where(chip_hot, ranks[d].reshape(-1)[None, :], 0), axis=1)
        step = chip_requests(steps[d])
        slot = jnp.where(step > 0, first_slot(plan, d, step) + rank // 2, slot)
        core = jnp.where(step > 0, rank % 2, core)
    where = slot + jnp.where(core == me_k, 0, slots)
    where = lax.dynamic_slice_in_dim(where, me_k * requests, requests)
    mine = jnp.where(core == me_k, slot, -1).reshape(2, requests)
    mine = jnp.where(me_k == 0, mine, mine[::-1]).reshape(-1)
    table = readers_table(mine, slots, 2 * requests)
    tables = (jnp.concatenate(order), where, jnp.concatenate(final))
    order, where, final = (t.astype(jnp.int32) for t in tables)
    return order, where, table, final


def local(pass_ids, store, queries, gate_pre, w_query, w_gate, w_key, w_value, d_mem):
    tp_count = lax.axis_size("tp")
    ring = lax.axis_size("st_0")
    passages, pass_len, _ = store.shape
    model_width = w_key.shape[0]
    requests = pass_ids.size
    plan = Plan(ring, passages)
    ids = jnp.zeros((8, 128), jnp.int32).at[:2, :requests].set(pass_ids.reshape(1, -1))
    pieces = gather_store(store)
    ids = gather_ids(5, ids)
    ids = ids[:, :2, :requests].reshape(2 * ring, requests)
    fits, cast_table, fold_table = stream_routes(ring, passages, ids)
    fits = fits[0] > 0
    kv = keys_values(pieces, w_key, w_value)

    def cast_short(ids, table, kv, weights):
        return stream_cast(0, table, kv, weights)

    def cast_any(ids, table, kv, weights):
        order, where, _, _ = routes(plan, ids)
        return cast_rows(plan, 1, order, where, kv, weights)

    def fold_short(ids, table, grads, tokens):
        return stream_fold(2, passages, table, grads, tokens)

    def fold_any(ids, table, grads, tokens):
        _, _, table, final = routes(plan, ids)
        return fold_rows(plan, 3, table, final, grads, tokens)

    weights = (w_query, w_gate, w_key, w_value)
    request_kv, wq_far, wg_far, wk_far, wv_far = lax.cond(
        fits, cast_short, cast_any, ids, cast_table, kv, weights
    )
    request_grads, token_grads = attend(queries, gate_pre, d_mem, request_kv)
    sums, tokens_in = lax.cond(
        fits, fold_short, fold_any, ids, fold_table, request_grads, token_grads
    )
    d_tokens, d_store, d_wkey = tail(
        4,
        sums,
        token_grads,
        tokens_in,
        pieces,
        (w_query, w_gate, wq_far, wg_far, w_key, w_value, wk_far, wv_far),
    )
    return d_tokens, d_store.reshape(passages // tp_count, pass_len, model_width), d_wkey


def solution(mesh):
    finer = Mesh(
        mesh.devices.reshape(mesh.shape["grp"], -1, 2, mesh.shape["tp"]),
        ("grp", "st_0", "st_1", "tp"),
    )
    in_specs = (
        P(GRP_ST, None),
        P(ST, None, "tp"),
        P(GRP_ST, "tp"),
        P(GRP_ST, "tp"),
        P(None, "tp"),
        P(None, "tp"),
        P(None, "tp"),
        P(None, "tp"),
        P(GRP_ST, "tp"),
    )
    out_specs = (P(GRP_ST_TP, None), P(GRP_ST_TP, None, None), P(GRP_ST, "tp"))
    return jax.shard_map(local, mesh=finer, in_specs=in_specs, out_specs=out_specs, check_vma=False)
```

```python
import functools

import jax
import jax.numpy as jnp
from jax import lax
from jax.experimental import pallas as pl
from jax.experimental.pallas import tpu as pltpu
from jax.sharding import Mesh
from jax.sharding import PartitionSpec as P

HD = 256
BLK = 128
PB = 4
MOST = 2
CHUNK = 16
LENGTH = 54
SHORT = 50
STAGE = 2
LAG = 2 * STAGE
VMEM_LIMIT = 62 * 1024 * 1024
ST = ("st_0", "st_1")
GRP_ST = ("grp", "st_0", "st_1")
GRP_ST_TP = ("grp", "st_0", "st_1", "tp")
MESH_ID = pl.DeviceIdType.MESH
VMEM_SPEC = pl.BlockSpec(memory_space=pltpu.VMEM)
SMEM_SPEC = pl.BlockSpec(memory_space=pltpu.SMEM)
ANY_SPEC = pl.BlockSpec(memory_space=pl.ANY)
F32 = jnp.float32


class Plan:
    def __init__(self, ring, passages):
        self.ring = ring
        self.passages = passages
        self.reach = ring // 2
        self.steps_of = range(1, self.reach + 1)
        per_owner = 2 * MOST
        self.layout = {
            t: min(passages, per_owner * (self.reach - t + 1))
            + min(passages, per_owner * (self.reach - t))
            for t in self.steps_of
        }
        self.sizes = self.layout
        self.base = [{}, {}]
        at = passages
        for d in range(2):
            for t in self.steps_of:
                self.base[d][t] = at
                at += -(-self.layout[t] // 2)
        self.slots = at

    def half(self, t):
        return -(-self.sizes[t] // 2) if t <= self.reach else 0

    def steps(self, down=False):
        for t in reversed(self.steps_of) if down else self.steps_of:
            for first in range(0, self.half(t), CHUNK):
                for d in range(2):
                    yield d, t, first, min(CHUNK, self.half(t) - first)


class Place:
    def __init__(self):
        self.g, self.z, self.k, self.x = (lax.axis_index(a) for a in GRP_ST_TP)
        self.ring = lax.axis_size("st_0")
        self.tp = lax.axis_size("tp")
        self.twin = (self.g, self.z, 1 - self.k, self.x)

    def along_z(self, step):
        return (self.g, lax.rem(self.z + step + self.ring, self.ring), self.k, self.x)

    def along_x(self, step):
        return (self.g, self.z, self.k, lax.rem(self.x + step + self.tp, self.tp))


def greet(*devices):
    barrier = pltpu.get_barrier_semaphore()
    for device in devices:
        pl.semaphore_signal(barrier, inc=1, device_id=device, device_id_type=MESH_ID)
    pl.semaphore_wait(barrier, len(devices))


class Copies:
    def __init__(self, send_sem, recv_sem):
        self.send_sem, self.recv_sem = send_sem, recv_sem
        self.all = []

    def start(self, src, dst, device):
        n = len(self.all)
        copy = pltpu.make_async_remote_copy(
            src_ref=src,
            dst_ref=dst,
            send_sem=self.send_sem.at[n],
            recv_sem=self.recv_sem.at[n],
            device_id=device,
            device_id_type=MESH_ID,
        )
        copy.start()
        self.all.append(copy)
        return copy

    def wait_sends(self):
        for copy in self.all:
            copy.wait_send()


def copy_sems(count):
    return [pltpu.SemaphoreType.DMA((count,)), pltpu.SemaphoreType.DMA((count,))]


def ids_kernel(ids_ref, ids_out, twin_ids, *sems):
    gifts, sends = (Copies(*sems[2 * i : 2 * i + 2]) for i in range(2))
    place = Place()
    peers = [place.along_z(step) for step in range(1, place.ring)]
    greet(place.twin, *peers)
    gift = gifts.start(ids_ref, twin_ids, place.twin)
    row = lax.broadcasted_iota(jnp.int32, ids_ref.shape, 0)
    gift.wait_recv()
    ids_out[place.z] = jnp.where(row == place.k, ids_ref[...], twin_ids[...])
    part = ids_out.at[place.z]
    for peer in peers:
        sends.start(part, part, peer)
    for copy in sends.all:
        copy.wait_recv()
    for group in (gifts, sends):
        group.wait_sends()


def gather_ids(ident, ids):
    ring = lax.axis_size("st_0")
    return pl.pallas_call(
        ids_kernel,
        out_shape=jax.ShapeDtypeStruct((ring, *ids.shape), ids.dtype),
        in_specs=[VMEM_SPEC],
        out_specs=VMEM_SPEC,
        scratch_shapes=[pltpu.VMEM(ids.shape, ids.dtype)] + copy_sems(1) + copy_sems(ring - 1),
        compiler_params=pltpu.CompilerParams(
            collective_id=ident, has_side_effects=True, vmem_limit_bytes=8 * 1024 * 1024
        ),
        cost_estimate=pl.CostEstimate(flops=9 * 10**9, bytes_accessed=10**6, transcendentals=0),
        name="gather_ids",
    )(ids)


def keys_values_kernel(own_ref, ahead_ref, behind_ref, low_ref, high_ref, wk_ref, wv_ref, kv_ref):
    x, tp = lax.axis_index("tp"), lax.axis_size("tp")
    count, pass_len, depth = own_ref.shape
    rows, cols = count * pass_len, wk_ref.shape[1]
    early = pl.program_id(0) < pl.num_programs(0) // 2
    opposite = jnp.where(early, low_ref[...], high_ref[...])
    parts = (own_ref[...], ahead_ref[...], opposite, behind_ref[...])
    for c, w_ref in enumerate((wk_ref, wv_ref)):
        total = None
        for rel, part in enumerate(parts):
            at = pl.multiple_of(lax.rem(x + rel, tp) * depth, depth)
            weight = w_ref[pl.ds(at, depth), :]
            term = jnp.dot(part.reshape(rows, depth), weight, preferred_element_type=F32)
            total = term if total is None else total + term
        at = slice(c * cols, (c + 1) * cols)
        kv_ref[:, :, at] = total.reshape(count, pass_len, cols).astype(kv_ref.dtype)


def keys_values(pieces, w_key, w_value):
    count, rows, depth = pieces[0].shape
    pair = 2 * w_key.shape[1]
    steps = 4
    block = (count // steps, rows, depth)
    whole = pl.BlockSpec(block, lambda i: (i, 0, 0))
    low = pl.BlockSpec(block, lambda i: (jnp.minimum(i, steps // 2 - 1), 0, 0))
    high = pl.BlockSpec(block, lambda i: (jnp.maximum(i - steps // 2, 0), 0, 0))
    weight = pl.BlockSpec(w_key.shape, lambda i: (0, 0))
    return pl.pallas_call(
        keys_values_kernel,
        grid=(steps,),
        out_shape=jax.ShapeDtypeStruct((count, rows, pair), pieces[0].dtype),
        in_specs=[whole, whole, whole, low, high, weight, weight],
        out_specs=pl.BlockSpec((count // steps, rows, pair), lambda i: (i, 0, 0)),
        name="keys_values",
    )(*pieces, w_key, w_value)


def gather_store(store):
    tp = lax.axis_size("tp")
    half = store.shape[0] // 2
    up = [(i, (i + 1) % tp) for i in range(tp)]
    down = [(i, (i - 1) % tp) for i in range(tp)]
    behind = lax.ppermute(store, "tp", up)
    ahead = lax.ppermute(store, "tp", down)
    low = lax.ppermute(behind[:half], "tp", up)
    high = lax.ppermute(ahead[half:], "tp", down)
    return store, ahead, behind, low, high


def attend_kernel(scale, q_ref, gate_ref, mem_ref, kv_ref, grads_ref, tokens_ref):
    blocks = q_ref.shape[0] // BLK
    cols = q_ref.shape[1]
    pass_len = kv_ref.shape[1]
    low = q_ref.dtype

    def dot(a, b, ca, cb):
        return lax.dot_general(a, b, (((ca,), (cb,)), ((), ())), preferred_element_type=F32)

    for b in range(blocks):
        toks = pl.ds(b * BLK, BLK)
        kv = kv_ref[pl.ds(b * PB, PB)].reshape(PB * pass_len, 2 * cols)
        for h in range(cols // HD):
            k_at = slice(h * HD, (h + 1) * HD)
            v_at = slice(cols + h * HD, cols + (h + 1) * HD)
            q, keys, values = q_ref[toks, k_at], kv[:, k_at], kv[:, v_at]
            scores = dot(q, keys, 1, 1) * scale
            shifted = jnp.exp(scores - jnp.max(scores, axis=-1, keepdims=True))
            probs = shifted / jnp.sum(shifted, axis=-1, keepdims=True)
            probs_low = probs.astype(low)
            attended = dot(probs_low, values, 1, 0)
            gate = gate_ref[toks, k_at].astype(F32)
            mem = mem_ref[toks, k_at].astype(F32)
            sig = jax.nn.sigmoid(gate)
            attended_grad = (gate * sig * mem).astype(low)
            gate_grad = mem * attended * sig * (1.0 + gate * (1.0 - sig))
            prob_grad = dot(attended_grad, values, 1, 1)
            inner = jnp.sum(probs * prob_grad, axis=-1, keepdims=True)
            score_grad = (scale * probs * (prob_grad - inner)).astype(low)
            tokens_ref[toks, k_at] = dot(score_grad, keys, 1, 0).astype(low)
            tokens_ref[toks, v_at] = gate_grad.astype(low)
            key_grad = dot(score_grad, q, 0, 0).astype(low)
            value_grad = dot(probs_low, attended_grad, 0, 0).astype(low)
            passes = pl.ds(b * PB, PB)
            grads_ref[passes, :, k_at] = key_grad.reshape(PB, pass_len, HD)
            grads_ref[passes, :, v_at] = value_grad.reshape(PB, pass_len, HD)


def attend(queries, gate_pre, d_mem, request_kv):
    toks, cols = queries.shape
    _, pass_len, pair = request_kv.shape
    step = 2
    grid = toks // BLK // step
    tok_spec = pl.BlockSpec((step * BLK, cols), lambda i: (i, 0))
    kv_spec = pl.BlockSpec((step * PB, pass_len, pair), lambda i: (i, 0, 0))
    return pl.pallas_call(
        functools.partial(attend_kernel, HD**-0.5),
        grid=(grid,),
        out_shape=[
            jax.ShapeDtypeStruct(request_kv.shape, request_kv.dtype),
            jax.ShapeDtypeStruct((toks, pair), queries.dtype),
        ],
        in_specs=[tok_spec, tok_spec, tok_spec, kv_spec],
        out_specs=[kv_spec, pl.BlockSpec((step * BLK, pair), lambda i: (i, 0))],
        name="attend",
    )(queries, gate_pre, d_mem, request_kv)


def cast_kernel(plan, weights, order_ref, where_ref, kv_ref, *refs):
    w_refs, refs = refs[:weights], refs[weights:]
    out_ref, w_outs, refs = refs[0], refs[1 : 1 + weights], refs[1 + weights :]
    buf, first_buf, home, *sems = refs
    ring_copies, gifts, w_copies = (Copies(*sems[2 * i : 2 * i + 2]) for i in range(3))
    place = Place()
    count, slots = plan.passages, plan.slots
    top = plan.half(1)

    greet(place.along_z(1), place.along_z(-1), place.along_x(1), place.along_x(-1), place.twin)
    own_gift = gifts.start(kv_ref, home.at[pl.ds(count, count)], place.twin)

    @pl.loop(0, count)
    def _(j):
        home[j] = kv_ref[j]
        buf[j] = kv_ref[j]

    own_gift.wait_recv()

    @pl.loop(0, top)
    def _(j):
        for d in range(2):
            first_buf[d * top + j] = home[order_ref[d * count + j]]

    copies = {}
    steps = list(plan.steps())
    extent = {(d, t, first): size for d, t, first, size in steps}

    def send(d, t, first):
        size = extent[d, t, first]
        if t == 1:
            src = first_buf.at[pl.ds(d * top + first, size)]
        else:
            src = buf.at[pl.ds(plan.base[d][t - 1] + first, size)]
        dst = buf.at[pl.ds(plan.base[d][t] + first, size)]
        copies[d, t, first] = ring_copies.start(src, dst, place.along_z(1 - 2 * d))

    for d, t, first, _ in steps:
        if t == 1:
            send(d, t, first)
    rows = w_refs[0].shape[0] // 2
    half = pl.ds(place.k * rows, rows)
    arrive = [[], []]
    for w_ref, w_out in zip(w_refs, w_outs):
        arrive[0].append(
            w_copies.start(w_ref.at[half], w_out.at[2, half], place.along_x(1))
        )
        arrive[1].append(
            w_copies.start(w_ref.at[half], w_out.at[0, half], place.along_x(-1))
        )
    w_gifts = []
    middle = []

    def forward_weights():
        for copy in arrive[0] + arrive[1]:
            copy.wait_recv()
        for w_out in w_outs:
            middle.append(
                w_copies.start(
                    w_out.at[2 * place.k, half],
                    w_out.at[1, half],
                    place.along_x(2 * place.k - 1),
                )
            )
            for rel in (0, 2):
                part = w_out.at[rel, half]
                w_gifts.append(w_copies.start(part, part, place.twin))

    last = None
    for d, t, first, size in steps:
        if t != last and t == plan.reach // 2 + 1:
            forward_weights()
        last = t
        copies[d, t, first].wait_recv()
        if (d, t + 1, first) in extent:
            send(d, t + 1, first)
        at = plan.base[d][t] + first
        gifts.start(buf.at[pl.ds(at, size)], buf.at[pl.ds(slots + at, size)], place.twin)
    for copy, w_out in zip(middle, w_outs):
        copy.wait_recv()
        part = w_out.at[1, half]
        w_gifts.append(w_copies.start(part, part, place.twin))
    for gift in gifts.all[1:]:
        gift.wait_recv()

    @pl.loop(0, count)
    def _(j):
        buf[slots + j] = home[count + j]

    @pl.loop(0, out_ref.shape[0])
    def _(r):
        out_ref[r] = buf[where_ref[r]]

    for gift in w_gifts:
        gift.wait_recv()
    for group in (gifts, ring_copies, w_copies):
        group.wait_sends()


def cast_rows(plan, ident, order, where, kv, weights):
    count, rows, cols = kv.shape
    steps = len(list(plan.steps()))
    others = lax.axis_size("tp") - 1
    return pl.pallas_call(
        functools.partial(cast_kernel, plan, len(weights)),
        out_shape=[jax.ShapeDtypeStruct((where.shape[0], rows, cols), kv.dtype)]
        + [jax.ShapeDtypeStruct((others, *w.shape), w.dtype) for w in weights],
        in_specs=[SMEM_SPEC, SMEM_SPEC, VMEM_SPEC] + [ANY_SPEC] * len(weights),
        out_specs=[VMEM_SPEC] + [ANY_SPEC] * len(weights),
        scratch_shapes=[
            pltpu.VMEM((2 * plan.slots, rows, cols), kv.dtype),
            pltpu.VMEM((2 * plan.half(1), rows, cols), kv.dtype),
            pltpu.VMEM((2 * count, rows, cols), kv.dtype),
        ]
        + copy_sems(steps)
        + copy_sems(steps + 1)
        + copy_sems(6 * len(weights)),
        compiler_params=pltpu.CompilerParams(
            collective_id=ident, has_side_effects=True, vmem_limit_bytes=VMEM_LIMIT
        ),
        name="cast_rows",
    )(order, where, kv, *weights)


def fold_kernel(
    plan,
    table_ref,
    final_ref,
    grads_ref,
    tokens_ref,
    out_ref,
    tokens_out,
    held,
    here,
    sums,
    load_sem,
    *sems,
):
    ring_copies, gifts, exchange = (Copies(*sems[2 * i : 2 * i + 2]) for i in range(3))
    place = Place()
    count, top = plan.passages, plan.half(1)
    own = grads_ref.shape[0]
    readers = 2 * MOST
    twin_at = plan.slots - count
    zero_at = twin_at + plan.layout[1]
    peers = [place.along_x(rel) for rel in range(1, place.tp)]

    load = pltpu.make_async_copy(grads_ref, held.at[pl.ds(0, own)], load_sem)
    load.start()
    held[2 * own] = jnp.zeros_like(held[2 * own])
    here[zero_at] = jnp.zeros_like(here[zero_at])
    greet(place.along_z(1), place.along_z(-1), place.twin, *peers)
    own_gift = gifts.start(grads_ref, held.at[pl.ds(own, own)], place.twin)
    block = tokens_out.shape[1]
    for rel, peer in enumerate(peers, 1):
        exchange.start(
            tokens_ref.at[pl.ds(peer[3] * block, block)],
            tokens_out.at[place.tp - 1 - rel],
            peer,
        )
    load.wait()
    own_gift.wait_recv()

    def readers_sum(slot):
        total = held[table_ref[slot * readers]].astype(F32)
        for q in range(1, readers):
            total += held[table_ref[slot * readers + q]].astype(F32)
        return total

    copies = {}
    steps = list(plan.steps(down=True))
    extent = {(d, t, first): size for d, t, first, size in steps}
    for d, t, first, size in steps:
        at = plan.base[d][t] + first
        begin = extent.get((d, t + 1, first), 0)
        if begin:
            copies[d, t + 1, first].wait_recv()
            far_at = plan.base[d][t + 1] + first

            @pl.loop(0, begin)
            def _(j):
                total = readers_sum(at + j) + here[far_at - count + j].astype(F32)
                sums[at - count + j] = total.astype(sums.dtype)

        if begin < size:

            @pl.loop(begin, size)
            def _(j):
                sums[at - count + j] = readers_sum(at + j).astype(sums.dtype)

        part = pl.ds(at - count, size)
        copies[d, t, first] = ring_copies.start(
            sums.at[part], here.at[part], place.along_z(2 * d - 1)
        )
    for d, t, first, size in steps:
        if t == 1:
            copies[d, t, first].wait_recv()
            src = here.at[pl.ds(plan.base[d][1] - count + first, size)]
            dst = here.at[pl.ds(twin_at + d * (plan.layout[1] // 2) + first, size)]
            gifts.start(src, dst, place.twin)
    for gift in gifts.all[1:]:
        gift.wait_recv()

    @pl.loop(0, count)
    def _(p):
        total = readers_sum(p)
        for d in range(2):
            total += here[final_ref[d * count + p]].astype(F32)
        out_ref[p] = total.astype(out_ref.dtype)

    for copy in exchange.all:
        copy.wait_recv()
    for group in (gifts, ring_copies, exchange):
        group.wait_sends()


def fold_rows(plan, ident, table, final, grads, tokens):
    own, rows, cols = grads.shape
    steps = list(plan.steps())
    ends = sum(1 for _, t, _, _ in steps if t == 1)
    count = plan.passages
    tp = lax.axis_size("tp")
    return pl.pallas_call(
        functools.partial(fold_kernel, plan),
        out_shape=[
            jax.ShapeDtypeStruct((count, rows, cols), grads.dtype),
            jax.ShapeDtypeStruct((tp - 1, tokens.shape[0] // tp, tokens.shape[1]), tokens.dtype),
        ],
        in_specs=[SMEM_SPEC, SMEM_SPEC, ANY_SPEC, ANY_SPEC],
        out_specs=[VMEM_SPEC, ANY_SPEC],
        scratch_shapes=[
            pltpu.VMEM((2 * own + 1, rows, cols), grads.dtype),
            pltpu.VMEM((plan.slots - count + plan.layout[1] + 1, rows, cols), grads.dtype),
            pltpu.VMEM((plan.slots - count, rows, cols), grads.dtype),
            pltpu.SemaphoreType.DMA,
        ]
        + copy_sems(len(steps))
        + copy_sems(1 + ends)
        + copy_sems(tp - 1),
        compiler_params=pltpu.CompilerParams(
            collective_id=ident, has_side_effects=True, vmem_limit_bytes=VMEM_LIMIT
        ),
        name="fold_rows",
    )(table, final, grads, tokens)


def copy_slots(src, src_at, dst, dst_at, size):
    @pl.loop(0, size)
    def _(j):
        dst[dst_at + j] = src[src_at + j]


class WeightShare:
    def __init__(self, place, copies, w_refs, w_outs):
        self.place, self.copies, self.outs = place, copies, w_outs
        rows = w_refs[0].shape[0] // 2
        self.half = pl.ds(place.k * rows, rows)
        self.near, self.middle, self.gifts = [], [], []
        for w_ref, w_out in zip(w_refs, w_outs):
            for slot, step in ((2, 1), (0, -1)):
                src, dst = w_ref.at[self.half], w_out.at[slot, self.half]
                self.near.append(copies.start(src, dst, place.along_x(step)))

    def forward(self, n):
        for copy in self.near[2 * n : 2 * n + 2]:
            copy.wait_recv()
        w_out = self.outs[n]
        src = w_out.at[2 * self.place.k, self.half]
        dst = w_out.at[1, self.half]
        device = self.place.along_x(2 * self.place.k - 1)
        self.middle.append(self.copies.start(src, dst, device))
        for slot in (0, 2):
            self.give(w_out.at[slot, self.half])

    def give(self, part):
        self.gifts.append(self.copies.start(part, part, self.place.twin))

    def finish(self):
        for copy, w_out in zip(self.middle, self.outs):
            copy.wait_recv()
            self.give(w_out.at[1, self.half])

    def wait(self):
        for gift in self.gifts:
            gift.wait_recv()


def stream_cast_kernel(weights, stages, table_ref, kv_ref, *refs):
    w_refs, refs = refs[:weights], refs[weights:]
    out_ref, w_outs, refs = refs[0], refs[1 : 1 + weights], refs[1 + weights :]
    kept, land, twin_land, leave, *sems = refs
    ring_copies, gifts, w_copies = (Copies(*sems[2 * i : 2 * i + 2]) for i in range(3))
    place = Place()
    count = kv_ref.shape[0]
    length = land.shape[0] // 2
    home = 2 * count

    greet(place.along_z(1), place.along_z(-1), place.along_x(1), place.along_x(-1), place.twin)
    own_gift = gifts.start(kv_ref, kept.at[pl.ds(count, count)], place.twin)

    @pl.loop(0, count)
    def _(j):
        kept[j] = kv_ref[j]

    own_gift.wait_recv()
    sends, given = {}, {}
    share = None
    for i in range(stages + 4):
        for d in range(2):
            if 0 <= i - 2 < stages:
                at = d * length + (i - 2) * STAGE
                sends[d, i - 2].wait_recv()
                part = pl.ds(at, STAGE)
                given[d, i - 2] = gifts.start(land.at[part], twin_land.at[part], place.twin)
                copy_slots(land, at, kept, home + at, STAGE)
            if i < stages:
                at = d * length + i * STAGE

                @pl.loop(at, at + STAGE)
                def _(q):
                    leave[q] = kept[table_ref[q]]

            if 0 <= i - 4 < stages:
                at = d * length + (i - 4) * STAGE
                given[d, i - 4].wait_recv()
                copy_slots(twin_land, at, kept, home + 2 * length + at, STAGE)
        if i < stages:
            for d in range(2):
                part = pl.ds(d * length + i * STAGE, STAGE)
                sends[d, i] = ring_copies.start(
                    leave.at[part], land.at[part], place.along_z(1 - 2 * d)
                )
        if i == 1:
            share = WeightShare(place, w_copies, w_refs, w_outs)
        if i in (6, 10, 14, 18):
            share.forward((i - 6) // 4)
    share.finish()

    @pl.loop(0, out_ref.shape[0])
    def _(r):
        out_ref[r] = kept[table_ref[2 * length + r]]

    share.wait()
    for group in (gifts, ring_copies, w_copies):
        group.wait_sends()


def stream_cast(ident, sent, table, kv, weights):
    count, rows, cols = kv.shape
    stages = sent // STAGE
    others = lax.axis_size("tp") - 1
    return pl.pallas_call(
        functools.partial(stream_cast_kernel, len(weights), stages),
        out_shape=[jax.ShapeDtypeStruct((table.shape[0] - 2 * LENGTH, rows, cols), kv.dtype)]
        + [jax.ShapeDtypeStruct((others, *w.shape), w.dtype) for w in weights],
        in_specs=[SMEM_SPEC, VMEM_SPEC] + [ANY_SPEC] * len(weights),
        out_specs=[VMEM_SPEC] + [ANY_SPEC] * len(weights),
        scratch_shapes=[
            pltpu.VMEM((2 * count + 4 * LENGTH, rows, cols), kv.dtype),
            pltpu.VMEM((2 * LENGTH, rows, cols), kv.dtype),
            pltpu.VMEM((2 * LENGTH, rows, cols), kv.dtype),
            pltpu.VMEM((2 * LENGTH, rows, cols), kv.dtype),
        ]
        + copy_sems(2 * stages)
        + copy_sems(2 * stages + 1)
        + copy_sems(6 * len(weights)),
        compiler_params=pltpu.CompilerParams(
            collective_id=ident, has_side_effects=True, vmem_limit_bytes=VMEM_LIMIT
        ),
        name="stream_cast",
    )(table, kv, *weights)


def stream_fold_kernel(
    stages, table_ref, grads_ref, tokens_ref, out_ref, tokens_out, held, kept, land,
    leave, twin_land, load_sem, *sems
):
    ring_copies, gifts, exchange = (Copies(*sems[2 * i : 2 * i + 2]) for i in range(3))
    place = Place()
    count = out_ref.shape[0]
    length = land.shape[0] // 2
    own = grads_ref.shape[0]
    readers = 2 * MOST
    zero = 2 * length
    onward_at = (count + 2 * length + 1) * readers
    final_at = onward_at + 2 * length
    peers = [place.along_x(rel) for rel in range(1, place.tp)]

    load = pltpu.make_async_copy(grads_ref, held.at[pl.ds(0, own)], load_sem)
    load.start()
    blank = jnp.zeros_like(held[0])
    held[2 * own] = blank
    kept[zero] = blank
    twin_land[2 * count] = blank
    greet(place.along_z(1), place.along_z(-1), place.twin, *peers)
    own_gift = gifts.start(grads_ref, held.at[pl.ds(own, own)], place.twin)
    block = tokens_out.shape[1]
    for rel, peer in enumerate(peers, 1):
        exchange.start(
            tokens_ref.at[pl.ds(peer[3] * block, block)],
            tokens_out.at[place.tp - 1 - rel],
            peer,
        )
    load.wait()
    own_gift.wait_recv()

    def readers_sum(slot):
        total = held[table_ref[slot * readers]].astype(F32)
        for q in range(1, readers):
            total += held[table_ref[slot * readers + q]].astype(F32)
        return total

    sends = {}

    def arrive(i):
        for d in range(2):
            at = d * length + i * STAGE
            sends[d, i].wait_recv()
            if i * STAGE < count:
                src = land.at[pl.ds(at, STAGE)]
                dst = twin_land.at[pl.ds(d * count + i * STAGE, STAGE)]
                gifts.start(src, dst, place.twin)
            copy_slots(land, at, kept, at, STAGE)

    for i in reversed(range(stages)):
        if i + 2 < stages:
            arrive(i + 2)

        @pl.loop(0, 2 * STAGE)
        def _(n):
            q = lax.div(n, STAGE) * length + i * STAGE + lax.rem(n, STAGE)
            total = readers_sum(count + q) + kept[table_ref[onward_at + q]].astype(F32)
            leave[q] = total.astype(leave.dtype)

        for d in range(2):
            part = pl.ds(d * length + i * STAGE, STAGE)
            sends[d, i] = ring_copies.start(
                leave.at[part], land.at[part], place.along_z(2 * d - 1)
            )
    arrive(1)
    arrive(0)
    for gift in gifts.all[1:]:
        gift.wait_recv()

    @pl.loop(0, count)
    def _(p):
        total = readers_sum(p)
        for d in range(2):
            total += kept[table_ref[final_at + d * count + p]].astype(F32)
            total += twin_land[table_ref[final_at + (2 + d) * count + p]].astype(F32)
        out_ref[p] = total.astype(out_ref.dtype)

    for copy in exchange.all:
        copy.wait_recv()
    for group in (gifts, ring_copies, exchange):
        group.wait_sends()


def stream_fold(ident, sent, count, table, grads, tokens):
    own, rows, cols = grads.shape
    stages = sent // STAGE
    tp = lax.axis_size("tp")
    return pl.pallas_call(
        functools.partial(stream_fold_kernel, stages),
        out_shape=[
            jax.ShapeDtypeStruct((count, rows, cols), grads.dtype),
            jax.ShapeDtypeStruct((tp - 1, tokens.shape[0] // tp, tokens.shape[1]), tokens.dtype),
        ],
        in_specs=[SMEM_SPEC, ANY_SPEC, ANY_SPEC],
        out_specs=[VMEM_SPEC, ANY_SPEC],
        scratch_shapes=[
            pltpu.VMEM((2 * own + 1, rows, cols), grads.dtype),
            pltpu.VMEM((2 * LENGTH + 1, rows, cols), grads.dtype),
            pltpu.VMEM((2 * LENGTH, rows, cols), grads.dtype),
            pltpu.VMEM((2 * LENGTH, rows, cols), grads.dtype),
            pltpu.VMEM((2 * count + 1, rows, cols), grads.dtype),
            pltpu.SemaphoreType.DMA,
        ]
        + copy_sems(2 * stages)
        + copy_sems(1 + 2 * (-(-count // STAGE)))
        + copy_sems(tp - 1),
        compiler_params=pltpu.CompilerParams(
            collective_id=ident, has_side_effects=True, vmem_limit_bytes=VMEM_LIMIT
        ),
        name="stream_fold",
    )(table, grads, tokens)


def readers_table(slot, slots, requests):
    at_slot = slot[:, None] == jnp.arange(slots, dtype=jnp.int32)[None, :]
    turn = jnp.cumsum(at_slot.astype(jnp.int32), axis=0)
    number = jnp.arange(requests, dtype=jnp.int32)[:, None]
    columns = [
        jnp.min(jnp.where(at_slot & (turn == q + 1), number, requests), axis=0)
        for q in range(2 * MOST)
    ]
    return jnp.stack(columns, axis=1).reshape(-1).astype(jnp.int32)


def needs(ring, count, ids):
    devices = ids.shape[0]
    pair = 2 * count
    every = jnp.arange(devices * count, dtype=jnp.int32)
    owner = ids // count
    owner_z, owner_k = owner // 2, owner % 2
    reader_z = (jnp.arange(devices, dtype=jnp.int32) // 2)[:, None]
    away = jnp.mod(reader_z - owner_z, ring)
    up = (2 * away < ring) | ((2 * away == ring) & (owner_k == 0))
    steps = (jnp.where(up, away, 0), jnp.where(up, 0, ring - away))
    hot = ids.reshape(-1)[:, None] == every[None, :]
    place = jnp.arange(pair, dtype=jnp.int32)
    ranks, fars = [], []
    for d in range(2):
        far = jnp.max(jnp.where(hot, steps[d].reshape(-1)[:, None], 0), axis=0)
        far = far.reshape(ring, pair)
        before = (far[:, None, :] > far[:, :, None]) | (
            (far[:, None, :] == far[:, :, None]) & (place[None, None, :] < place[None, :, None])
        )
        ranks.append(jnp.sum(before.astype(jnp.int32), axis=2))
        fars.append(far)
    return owner_k, steps, fars, ranks


def own_chip(array):
    return lax.dynamic_slice_in_dim(array, lax.axis_index("st_0"), 1, axis=0)[0]


def chip_requests(array):
    return lax.dynamic_slice_in_dim(array, 2 * lax.axis_index("st_0"), 2, axis=0).reshape(-1)


def routes_kernel(count, requests, size_ref, info_ref, fits_ref, cast_ref, fold_ref, starts, start, size, used, sem):
    z, k = lax.axis_index("st_0"), lax.axis_index("st_1")
    ring = lax.axis_size("st_0")
    reach = ring // 2
    pair = 2 * count
    twin_at = 2 * LENGTH
    lane = lax.broadcasted_iota(jnp.int32, starts.shape, 1)
    lanes = starts.shape[1]
    spot = lane % ring
    up = lane < 2 * ring
    now = jnp.zeros(starts.shape, jnp.int32)
    most = jnp.zeros(starts.shape, jnp.int32)
    for t in range(reach):
        if t > 0:
            ends = now + jnp.broadcast_to(size_ref[t - 1 : t, :], starts.shape)
            after = jnp.where(
                spot == ring - 1, pltpu.roll(ends, ring - 1, 1), pltpu.roll(ends, lanes - 1, 1)
            )
            before = jnp.where(
                spot == 0, pltpu.roll(ends, lanes - ring + 1, 1), pltpu.roll(ends, 1, 1)
            )
            now = jnp.maximum(jnp.where(up, after, before), now + LAG)
        starts[t : t + 1, :] = now[0:1, :]
        here = now + jnp.broadcast_to(size_ref[t : t + 1, :], starts.shape)
        most = jnp.maximum(most, jnp.where(lane < 4 * ring, here, 0))
    top = jnp.max(most)
    fits_ref[0] = (top <= LENGTH).astype(jnp.int32) + (top <= SHORT).astype(jnp.int32)
    for n, (src, dst) in enumerate(((starts, start), (size_ref, size))):
        copy = pltpu.make_async_copy(src, dst, sem.at[n])
        copy.start()
        copy.wait()

    slots = count + 2 * LENGTH
    readers = 2 * MOST
    onward_at, final_at = (slots + 1) * readers, (slots + 1) * readers + 2 * LENGTH

    @pl.loop(0, slots + 1)
    def _(i):
        used[i] = 0
        for q in range(readers):
            fold_ref[i * readers + q] = 2 * requests

    @pl.loop(0, LENGTH)
    def _(i):
        for q in range(2):
            fold_ref[onward_at + 2 * i + q] = 2 * LENGTH
            cast_ref[2 * i + q] = 0

    def info(row, i):
        return info_ref[row * 2 * requests + i]

    def column(d, core, step):
        source = lax.rem(z - (1 - 2 * d) * step + 2 * ring, ring)
        return (2 * d + core) * ring + source

    last = LENGTH - 1
    for d in range(2):

        @pl.loop(0, pair)
        def _(p):
            rank = info(5, d * pair + p)
            far = info(6, d * pair + p)
            core = lax.div(p, count)
            mine = rank % 2 == k
            home = p % count + jnp.where(core == k, 0, count)

            @pl.when(mine)
            def _():
                cast_ref[d * LENGTH + rank // 2] = home

            @pl.when(core == k)
            def _():
                i = p % count
                near = jnp.where((far > 0) & mine, d * LENGTH + rank // 2, 2 * LENGTH)
                aside = jnp.where((far > 0) & (rank % 2 != k), d * count + rank // 2, 2 * count)
                fold_ref[final_at + d * count + i] = near
                fold_ref[final_at + (2 + d) * count + i] = aside

        for t in range(1, reach):
            lane_of = column(d, k, t)
            at_out, at_in = start[t, lane_of], start[t - 1, lane_of]

            @pl.loop(0, size[t, lane_of])
            def _(r):
                out = d * LENGTH + jnp.minimum(at_out + r, last)
                come = d * LENGTH + jnp.minimum(at_in + r, last)
                cast_ref[out] = pair + come
                fold_ref[onward_at + come] = out

    @pl.loop(0, 2 * requests)
    def _(i):
        c = lax.rem(i + k * requests, 2 * requests)
        step, way, rank, within, owner = (info(row, c) for row in range(5))
        core = jnp.where(step > 0, rank % 2, owner)
        lane_of = column(way, core, step)
        at = start[jnp.maximum(step - 1, 0), lane_of] + lax.div(rank, 2)
        at = way * LENGTH + jnp.minimum(at, last)
        where = pair + at + jnp.where(core == k, 0, twin_at)
        where = jnp.where(step > 0, where, within + jnp.where(core == k, 0, count))
        slot = jnp.where(core == k, jnp.where(step > 0, count + at, within), slots)
        turn = jnp.where(slot == slots, 0, jnp.minimum(used[slot], readers - 1))
        used[slot] = turn + 1
        fold_ref[slot * readers + turn] = i

        @pl.when(i < requests)
        def _():
            cast_ref[2 * LENGTH + i] = where


def stream_routes(ring, count, ids):
    devices, requests = ids.shape
    pair = 2 * count
    reach = ring // 2
    owner_k, steps, fars, ranks = needs(ring, count, ids)
    dist = jnp.arange(1, reach + 1, dtype=jnp.int32)
    core = jnp.arange(2, dtype=jnp.int32)
    far = jnp.stack(fars)
    whole = jnp.sum((far[None] >= dist[:, None, None, None]).astype(jnp.int32), axis=3)
    size = (whole[:, :, None, :] + 1 - core[None, None, :, None]) // 2
    size = jnp.pad(size.reshape(reach, 4 * ring), ((0, 0), (0, 128 - 4 * ring)))
    chip_ids = chip_requests(ids)
    every = jnp.arange(devices * count, dtype=jnp.int32)
    chip_hot = chip_ids[:, None] == every[None, :]
    step = [chip_requests(s) for s in steps]
    way = (step[1] > 0).astype(jnp.int32)
    ranked = [jnp.sum(jnp.where(chip_hot, r.reshape(-1)[None, :], 0), axis=1) for r in ranks]
    info = jnp.concatenate(
        [
            step[0] + step[1],
            way,
            jnp.where(way == 0, ranked[0], ranked[1]),
            chip_ids % count,
            chip_requests(owner_k),
            own_chip(ranks[0]),
            own_chip(ranks[1]),
            own_chip(fars[0]),
            own_chip(fars[1]),
        ]
    ).astype(jnp.int32)
    slots = count + 2 * LENGTH
    fold_size = (slots + 1) * 2 * MOST + 2 * LENGTH + 4 * count
    return pl.pallas_call(
        functools.partial(routes_kernel, count, requests),
        out_shape=[
            jax.ShapeDtypeStruct((1,), jnp.int32),
            jax.ShapeDtypeStruct((2 * LENGTH + requests,), jnp.int32),
            jax.ShapeDtypeStruct((fold_size,), jnp.int32),
        ],
        in_specs=[VMEM_SPEC, SMEM_SPEC],
        out_specs=[SMEM_SPEC] * 3,
        scratch_shapes=[
            pltpu.VMEM((reach, 128), jnp.int32),
            pltpu.SMEM((reach, 128), jnp.int32),
            pltpu.SMEM((reach, 128), jnp.int32),
            pltpu.SMEM((slots + 1,), jnp.int32),
            pltpu.SemaphoreType.DMA((2,)),
        ],
        cost_estimate=pl.CostEstimate(flops=6 * 10**9, bytes_accessed=10**5, transcendentals=0),
        name="routes",
    )(size, info)


def project(rows_list, weight_list, out_ref, n, tile):
    cols = pl.ds(n * tile, tile)
    total = None
    for rows, weight in zip(rows_list, weight_list):
        term = lax.dot_general(
            rows[...], weight[cols, :], (((1,), (1,)), ((), ())), preferred_element_type=F32
        )
        total = term if total is None else total + term
    out_ref[:, cols] = total.astype(out_ref.dtype)


def tail_kernel(sums_ref, tokens_ref, tokens_in, *refs):
    pieces, refs = refs[:5], refs[5:]
    weights, refs = refs[:8], refs[8:]
    d_tokens_ref, d_store_ref, d_wkey_ref = refs[:3]
    wbuf_t, wbuf_s, own_t, in_t, own_s, in_s, refs = *refs[3:9], refs[9:]
    keys, keys_turned, all_buf, terms, twin_terms, sent, come, last, last_in, refs = *refs[:9], refs[9:]
    load_sem, *sems = refs
    exchange, gifts, ring_copies = (Copies(*sems[2 * i : 2 * i + 2]) for i in range(3))
    place = Place()
    tp, ring = place.tp, place.ring
    reach = ring // 2
    peers = [place.along_x(rel) for rel in range(1, tp)]
    loads = []

    def load(src, dst):
        copy = pltpu.make_async_copy(src, dst, load_sem.at[len(loads)])
        copy.start()
        loads.append(copy)

    load(sums_ref, keys)
    own_piece, ahead, behind, low, high = pieces
    part = low.shape[0]
    load(own_piece, all_buf.at[0])
    load(ahead, all_buf.at[1])
    load(behind, all_buf.at[tp - 1])
    load(low, all_buf.at[2, pl.ds(0, part)])
    load(high, all_buf.at[2, pl.ds(part, part)])
    greet(place.twin, place.along_z(1), place.along_z(-1), *peers)
    share = sums_ref.shape[0] // tp
    for rel, peer in enumerate(peers, 1):
        exchange.start(
            sums_ref.at[pl.ds(peer[3] * share, share)], in_s.at[tp - 1 - rel], peer
        )
    block = own_t.shape[0]
    load(tokens_ref.at[pl.ds(place.x * block, block)], own_t)
    load(tokens_in, in_t)
    load(sums_ref.at[pl.ds(place.x * share, share)], own_s)
    for wbuf, (wa, wb, wa_far, wb_far) in ((wbuf_t, weights[:4]), (wbuf_s, weights[4:])):
        load(wa, wbuf.at[0])
        load(wb, wbuf.at[1])
        load(wa_far, wbuf.at[pl.ds(2, tp - 1)])
        load(wb_far, wbuf.at[pl.ds(2 + tp - 1, tp - 1)])
    count, pass_len, pair = sums_ref.shape
    rows, cols = count * pass_len, pair // 2
    depth = own_piece.shape[2]
    width = terms.shape[3]
    loads[0].wait()
    keys_turned[...] = keys[:, :, :cols].reshape(rows, cols).T
    chips = depth // width
    for rel in range(tp):
        for copy in [loads[1:2], loads[2:3], loads[4:6], loads[3:4]][rel]:
            copy.wait()
        n = lax.rem(place.x + rel, tp)
        term = jnp.dot(
            keys_turned[...], all_buf[rel].reshape(rows, depth), preferred_element_type=F32
        )
        for c in range(chips):
            for h in range(2):
                terms[h, n * chips + c] = term[
                    h * (cols // 2) : (h + 1) * (cols // 2), c * width : (c + 1) * width
                ]
        part = pl.ds(n * chips, chips)
        gifts.start(terms.at[1 - place.k, part], twin_terms.at[part], place.twin)

    def operands(own, far_rows, wbuf):
        n_cols = own.shape[-1] // 2
        rows_list, weight_list = [], []
        for c in range(2):
            rows_list.append(own.at[:, pl.ds(c * n_cols, n_cols)])
            weight_list.append(wbuf.at[c])
        for rel in range(tp - 1):
            for c in range(2):
                rows_list.append(far_rows.at[rel, :, pl.ds(c * n_cols, n_cols)])
                weight_list.append(wbuf.at[2 + c * (tp - 1) + rel])
        return rows_list, weight_list

    part_rows = share * pass_len
    tile = 512
    tiles = d_tokens_ref.shape[1] // tile
    for_tokens = operands(own_t, in_t, wbuf_t)
    for_store = operands(
        own_s.reshape(part_rows, pair), in_s.reshape(tp - 1, part_rows, pair), wbuf_s
    )
    for gift in gifts.all:
        gift.wait_recv()
    hops = {}

    def mine(dest):
        return terms[place.k, dest] + twin_terms[dest]

    done = 0
    for s in range(1, reach + 1):
        for d in range(2):
            to_go = reach - d + 1 - s
            if to_go < 1:
                continue
            turn = 1 - 2 * d
            total = mine(lax.rem(place.z + turn * to_go + ring, ring))
            n = d * reach + s - 1
            if s > 1:
                hops[d, s - 1].wait_recv()
                total += come[n - 1].astype(F32)
            sent[n] = total.astype(sent.dtype)
            hops[d, s] = ring_copies.start(sent.at[n], come.at[n], place.along_z(turn))
        if s == 1:
            for copy in loads[6:]:
                copy.wait()
        if s == reach // 2:
            for copy in exchange.all:
                copy.wait_recv()
        if s <= reach // 2:
            for _ in range(-(-tiles // (reach // 2))):
                if done < tiles:
                    project(*for_tokens, d_tokens_ref, done, tile)
                    done += 1
        elif s < reach:
            for _ in range(-(-tiles // (reach // 2 - 1))):
                if done < 2 * tiles:
                    project(*for_store, d_store_ref, done - tiles, tile)
                    done += 1
    total = mine(place.z)
    for d in range(2):
        hops[d, reach - d].wait_recv()
        total += come[d * reach + reach - d - 1].astype(F32)
    turned = total.T
    out_rows = turned.shape[0] // 2
    for c in range(2):
        last[c] = turned[c * out_rows : (c + 1) * out_rows]
    end = gifts.start(last.at[1 - place.k], last_in, place.twin)
    half = cols // 2
    d_wkey_ref[:, pl.ds(pl.multiple_of(place.k * half, half), half)] = last[place.k]
    end.wait_recv()
    d_wkey_ref[:, pl.ds(pl.multiple_of((1 - place.k) * half, half), half)] = last_in[...]
    for group in (exchange, gifts, ring_copies):
        group.wait_sends()


def tail(ident, sums, tokens, tokens_in, pieces, weights):
    tp, ring = lax.axis_size("tp"), lax.axis_size("st_0")
    model, head_cols = weights[0].shape
    count, pass_len, pair = sums.shape
    share = count // tp
    width = model // ring
    low = sums.dtype
    return pl.pallas_call(
        tail_kernel,
        out_shape=[
            jax.ShapeDtypeStruct((tokens.shape[0] // tp, model), low),
            jax.ShapeDtypeStruct((share * pass_len, model), low),
            jax.ShapeDtypeStruct((width // 2, head_cols), F32),
        ],
        in_specs=[ANY_SPEC] * (3 + len(pieces) + len(weights)),
        out_specs=[VMEM_SPEC] * 3,
        scratch_shapes=[
            pltpu.VMEM((2 * tp, model, head_cols), low),
            pltpu.VMEM((2 * tp, model, head_cols), low),
            pltpu.VMEM((tokens.shape[0] // tp, tokens.shape[1]), low),
            pltpu.VMEM(tokens_in.shape, low),
            pltpu.VMEM((share, pass_len, pair), low),
            pltpu.VMEM((tp - 1, share, pass_len, pair), low),
            pltpu.VMEM(sums.shape, low),
            pltpu.VMEM((head_cols, count * pass_len), low),
            pltpu.VMEM((tp, *pieces[0].shape), low),
            pltpu.VMEM((2, ring, head_cols // 2, width), F32),
            pltpu.VMEM((ring, head_cols // 2, width), F32),
            pltpu.VMEM((ring, head_cols // 2, width), low),
            pltpu.VMEM((ring, head_cols // 2, width), low),
            pltpu.VMEM((2, width // 2, head_cols // 2), F32),
            pltpu.VMEM((width // 2, head_cols // 2), F32),
            pltpu.SemaphoreType.DMA((4 + len(pieces) + len(weights),)),
        ]
        + copy_sems(tp - 1)
        + copy_sems(tp + 1)
        + copy_sems(ring - 1),
        compiler_params=pltpu.CompilerParams(
            collective_id=ident, has_side_effects=True, vmem_limit_bytes=VMEM_LIMIT
        ),
        name="tail",
    )(sums, tokens, tokens_in, *pieces, *weights)


def first_slot(plan, d, step):
    total = jnp.zeros_like(step)
    for t, at in plan.base[d].items():
        total = total + jnp.where(step == t, at, 0)
    return total


def routes(plan, ids):
    count, slots = plan.passages, plan.slots
    me_k = lax.axis_index("st_1")
    requests = ids.shape[1]
    every = jnp.arange(ids.shape[0] * count, dtype=jnp.int32)
    owner_k, steps, fars, ranks = needs(plan.ring, count, ids)
    place = jnp.arange(2 * count, dtype=jnp.int32)
    at_home = place % count + jnp.where(place // count == me_k, 0, count)
    want = 2 * jnp.arange(count, dtype=jnp.int32) + me_k
    order, final = [], []
    for d in range(2):
        rank, far = own_chip(ranks[d]), own_chip(fars[d])
        order.append(jnp.sum(jnp.where(rank[None, :] == want[:, None], at_home[None, :], 0), axis=1))
        twin_at = plan.slots - count
        near = plan.base[d][1] - count
        aside = twin_at + d * (plan.layout[1] // 2)
        index = jnp.where(rank % 2 == me_k, near, aside) + rank // 2
        index = jnp.where(far > 0, index, twin_at + plan.layout[1])
        final.append(lax.dynamic_slice_in_dim(index, me_k * count, count))
    chip_ids = chip_requests(ids)
    chip_hot = chip_ids[:, None] == every[None, :]
    slot, core = chip_ids % count, chip_requests(owner_k)
    for d in range(2):
        rank = jnp.sum(jnp.where(chip_hot, ranks[d].reshape(-1)[None, :], 0), axis=1)
        step = chip_requests(steps[d])
        slot = jnp.where(step > 0, first_slot(plan, d, step) + rank // 2, slot)
        core = jnp.where(step > 0, rank % 2, core)
    where = slot + jnp.where(core == me_k, 0, slots)
    where = lax.dynamic_slice_in_dim(where, me_k * requests, requests)
    mine = jnp.where(core == me_k, slot, -1).reshape(2, requests)
    mine = jnp.where(me_k == 0, mine, mine[::-1]).reshape(-1)
    table = readers_table(mine, slots, 2 * requests)
    tables = (jnp.concatenate(order), where, jnp.concatenate(final))
    order, where, final = (t.astype(jnp.int32) for t in tables)
    return order, where, table, final


def local(pass_ids, store, queries, gate_pre, w_query, w_gate, w_key, w_value, d_mem):
    tp_count = lax.axis_size("tp")
    ring = lax.axis_size("st_0")
    passages, pass_len, _ = store.shape
    model_width = w_key.shape[0]
    requests = pass_ids.size
    plan = Plan(ring, passages)
    ids = jnp.zeros((8, 128), jnp.int32).at[:2, :requests].set(pass_ids.reshape(1, -1))
    pieces = gather_store(store)
    ids = gather_ids(5, ids)
    ids = ids[:, :2, :requests].reshape(2 * ring, requests)
    fits, cast_table, fold_table = stream_routes(ring, passages, ids)
    fits = fits[0]
    kv = keys_values(pieces, w_key, w_value)

    def cast_any(ids, table, kv, weights):
        order, where, _, _ = routes(plan, ids)
        return cast_rows(plan, 1, order, where, kv, weights)

    def cast_stream(ident, sent):
        return lambda ids, table, kv, weights: stream_cast(ident, sent, table, kv, weights)

    def fold_any(ids, table, grads, tokens):
        _, _, table, final = routes(plan, ids)
        return fold_rows(plan, 3, table, final, grads, tokens)

    def fold_stream(ident, sent):
        return lambda ids, table, grads, tokens: stream_fold(
            ident, sent, passages, table, grads, tokens
        )

    weights = (w_query, w_gate, w_key, w_value)
    request_kv, wq_far, wg_far, wk_far, wv_far = lax.switch(
        fits,
        (cast_any, cast_stream(0, LENGTH), cast_stream(6, SHORT)),
        ids,
        cast_table,
        kv,
        weights,
    )
    request_grads, token_grads = attend(queries, gate_pre, d_mem, request_kv)
    sums, tokens_in = lax.switch(
        fits,
        (fold_any, fold_stream(2, LENGTH), fold_stream(7, SHORT)),
        ids,
        fold_table,
        request_grads,
        token_grads,
    )
    d_tokens, d_store, d_wkey = tail(
        4,
        sums,
        token_grads,
        tokens_in,
        pieces,
        (w_query, w_gate, wq_far, wg_far, w_key, w_value, wk_far, wv_far),
    )
    return d_tokens, d_store.reshape(passages // tp_count, pass_len, model_width), d_wkey


def solution(mesh):
    finer = Mesh(
        mesh.devices.reshape(mesh.shape["grp"], -1, 2, mesh.shape["tp"]),
        ("grp", "st_0", "st_1", "tp"),
    )
    in_specs = (
        P(GRP_ST, None),
        P(ST, None, "tp"),
        P(GRP_ST, "tp"),
        P(GRP_ST, "tp"),
        P(None, "tp"),
        P(None, "tp"),
        P(None, "tp"),
        P(None, "tp"),
        P(GRP_ST, "tp"),
    )
    out_specs = (P(GRP_ST_TP, None), P(GRP_ST_TP, None, None), P(GRP_ST, "tp"))
    return jax.shard_map(local, mesh=finer, in_specs=in_specs, out_specs=out_specs, check_vma=False)
```
